512 devices in a mesh: ep: 128 (over z, y, core), tp: 4 (over x).
Axes of the slice: x: 4, y: 8, z: 8, core: 2. Of those that a mesh axis runs over, the one named last changes fastest.
Arguments:
- tokens: bfloat16 [2048, 1024], P('ep'), may hold values from -6 to 6
- attn_gain: float32 [1024], replicated, may hold values from 0.1 to 1.9
- q_down: bfloat16 [1024, 512], P(None, 'tp'), may hold values from -0.1875 to 0.1875
- kv_down: bfloat16 [1024, 512], P(None, 'tp'), may hold values from -0.1875 to 0.1875
- rope_down: bfloat16 [1024, 32], replicated, may hold values from -0.1875 to 0.1875
- q_latent_gain: float32 [512], replicated, may hold values from 0.1 to 1.9
- kv_latent_gain: float32 [512], replicated, may hold values from 0.1 to 1.9
- q_up: bfloat16 [512, 768], P(None, 'tp'), may hold values from -0.25 to 0.25
- query_gain: float32 [8, 96], P('tp'), may hold values from 0.4 to 48
- key_up: bfloat16 [512, 512], P(None, 'tp'), may hold values from -0.25 to 0.25
- value_up: bfloat16 [512, 512], P(None, 'tp'), may hold values from -0.25 to 0.25
- attn_out: bfloat16 [512, 1024], P('tp'), may hold values from -0.25 to 0.25
- cache_latent: bfloat16 [2048, 512, 512], P(('ep', 'tp')), may hold values from -6 to 6
- cache_rope: bfloat16 [2048, 32, 512], P(('ep', 'tp')), may hold values from -6 to 6
- lengths: int32 [2048], P('ep'), may hold values from 1 to 512, as said below
- moe_gain: float32 [1024], replicated, may hold values from 0.1 to 1.9
- route: int32 [2048, 6], P('ep'), may hold values from 0 to 127, as said below
- route_weight: float32 [2048, 6], P('ep'), may hold values from 0.1 to 1
- expert_gate: bfloat16 [128, 1024, 512], P('ep', None, 'tp'), may hold values from -0.1875 to 0.1875
- expert_up: bfloat16 [128, 1024, 512], P('ep', None, 'tp'), may hold values from -0.1875 to 0.1875
- expert_down: bfloat16 [128, 512, 1024], P('ep', 'tp'), may hold values from -0.25 to 0.25
Outputs:
- mixed_out: bfloat16 [2048, 1024], P('ep', 'tp')
- new_latent: bfloat16 [2048, 512], P('ep', 'tp')
- new_rope: bfloat16 [2048, 32], P('ep')
The draws below stay inside these ranges and needn't reach their ends.
Inputs may be any that keep to these rules, and one draw needn't show every extreme that they name: `route`: each row names 6 different experts that lie in one group of 8 consecutive expert numbers. Among the rows of the 16 sequences of one index of ep no expert is named more than 2 times, and some expert is named exactly 2 times by the rows of every index of ep. `lengths`: some sequence has exactly 512 cached positions.
All inputs are finite; a program needn't handle non-finite values.
Results may differ from the reference program's by a relative error of at most 0.02.
Values may be sent and summed in bfloat16 or wider, within the bound.
No kernel may reach another device: no remote copies, remote signals or barrier semaphores. Data moves between devices by JAX's collectives and lax.ppermute only.
A program may use at most 64 MiB of HBM per device.

```python
import math
import jax
import jax.numpy as jnp
from jax import lax

D = 1024
HEADS = 8
NOPE = 64
ROPE = 32
VDIM = 64
QK = 96
Q_RANK = 512
KV_RANK = 512
FF = 512
EXPERTS = 128
EPG = 8
GROUPS = 16
TOPK = 6
SEQ_DEV = 16
CACHE_LEN = 512
SEQS = 2048
NG_CAP = 2
CAP = 2
N_EP = 128
N_TP = 4


def draw_lengths(key, part):
    base_len = jax.random.randint(jax.random.fold_in(key, 11), (SEQS,), 1, CACHE_LEN + 1)
    longest = jax.random.randint(jax.random.fold_in(key, 12), (), 0, SEQS)
    return jnp.where(jnp.arange(SEQS) == longest, CACHE_LEN, base_len).astype(jnp.int32)


def draw_query_gain(key, part):
    noise = jax.random.truncated_normal(jax.random.fold_in(key, 23), -3.0, 3.0, (HEADS, QK), jnp.float32)
    return (1.0 + 0.18 * noise).astype(jnp.float32)


def draw_route(key, part):
    blocks_count = SEQS // SEQ_DEV
    slot_count = GROUPS * NG_CAP
    forced = jax.random.randint(jax.random.fold_in(key, 31), (), 0, GROUPS)
    forced_perm = jax.random.permutation(jax.random.fold_in(key, 32), EPG)
    slot_ids = jnp.arange(slot_count, dtype=jnp.int32)
    slot_group = slot_ids // NG_CAP
    noise = jax.random.randint(jax.random.fold_in(key, 33), (blocks_count, slot_count), 0, 1 << 16) * slot_count + slot_ids
    priority = jnp.where(slot_group[None, :] == forced, slot_ids[None, :] - slot_count, noise)
    chosen = jnp.argsort(priority, axis=1)[:, :SEQ_DEV]
    shuffle_keys = jax.random.randint(jax.random.fold_in(key, 34), (blocks_count, SEQ_DEV), 0, 1 << 16) * SEQ_DEV + jnp.arange(SEQ_DEV)
    taken = jnp.take_along_axis(chosen, jnp.argsort(shuffle_keys, axis=1), axis=1)
    groups_of = taken // NG_CAP
    ranks_of = taken % NG_CAP
    perm_keys = jax.random.randint(jax.random.fold_in(key, 35), (blocks_count, GROUPS, EPG), 0, 1 << 16) * EPG + jnp.arange(EPG)
    group_perm = jnp.argsort(perm_keys, axis=2)
    group_perm = jnp.where((jnp.arange(GROUPS) == forced)[None, :, None], forced_perm[None, None, :], group_perm)
    token_perm = group_perm[jnp.arange(blocks_count)[:, None], groups_of]
    offsets = (ranks_of[:, :, None] * TOPK + jnp.arange(TOPK)[None, None, :]) % EPG
    local_ids = jnp.take_along_axis(token_perm, offsets, axis=2)
    return (groups_of[:, :, None] * EPG + local_ids).reshape(SEQS, TOPK).astype(jnp.int32)


def block_levels(own_key, shape, shards, smallest, top_value):
    level, own = 1.0, jax.random.fold_in(own_key, 6)
    for dim, parts in shards:
        draws = jnp.exp(jax.random.uniform(jax.random.fold_in(own, dim), (parts,), jnp.float32, smallest / len(shards), top_value / len(shards)))
        level = level * jnp.repeat(draws, shape[dim] // parts).reshape([-1 if axis == dim else 1 for axis in range(len(shape))])
    return level


def normal_values(stream_key, shape, deviation, bound, cuts=(), kind=jnp.bfloat16):
    array = jax.random.normal(stream_key, shape, jnp.float32) * deviation
    if len(cuts) > 0:
        array = block_levels(stream_key, shape, cuts, -0.22, 0.18) * array
    return jnp.clip(array, min=-bound, max=bound).astype(kind)


def setup_inputs(seed: int = 0) -> dict:
    streams_of = jax.random.split(jax.random.key(seed), 22)
    tokens = normal_values(streams_of[0], (SEQS, D), 1.0, 6.0, ((0, 128),))
    attn_gain = jnp.clip(1.0 + 0.18 * jax.random.normal(streams_of[1], (D,), jnp.float32), 0.1, 1.9)
    q_down = normal_values(streams_of[2], (D, Q_RANK), D ** -0.5, 0.1875, ((1, 4),))
    kv_down = normal_values(streams_of[3], (D, KV_RANK), D ** -0.5, 0.1875, ((1, 4),))
    rope_down = normal_values(streams_of[4], (D, ROPE), D ** -0.5, 0.1875)
    q_latent_gain = jnp.clip(1.0 + 0.18 * jax.random.normal(streams_of[5], (Q_RANK,), jnp.float32), 0.1, 1.9)
    kv_latent_gain = jnp.clip(1.0 + 0.18 * jax.random.normal(streams_of[6], (KV_RANK,), jnp.float32), 0.1, 1.9)
    q_up = normal_values(streams_of[7], (Q_RANK, HEADS * QK), Q_RANK ** -0.5, 0.25, ((1, 4),))
    query_gain = draw_query_gain(jax.random.fold_in(streams_of[21], 71), 0)
    key_up = normal_values(streams_of[9], (KV_RANK, HEADS * NOPE), KV_RANK ** -0.5, 0.25, ((1, 4),))
    value_up = normal_values(streams_of[10], (KV_RANK, HEADS * VDIM), KV_RANK ** -0.5, 0.25, ((1, 4),))
    attn_out = normal_values(streams_of[11], (HEADS * VDIM, D), (HEADS * VDIM) ** -0.5, 0.25, ((0, 4),))
    cache_latent = normal_values(streams_of[12], (SEQS, CACHE_LEN, KV_RANK), 1.0, 6.0, ((0, 512),))
    cache_rope = normal_values(streams_of[13], (SEQS, ROPE, CACHE_LEN), 1.0, 6.0, ((0, 512),))
    lengths = draw_lengths(jax.random.fold_in(streams_of[21], 71), 0)
    moe_gain = jnp.clip(1.0 + 0.18 * jax.random.normal(streams_of[15], (D,), jnp.float32), 0.1, 1.9)
    route = draw_route(jax.random.fold_in(streams_of[21], 71), 0)
    route_weight = jnp.clip(jnp.exp(math.log(1.0) - 2.3025851 * jax.random.uniform(streams_of[17], (SEQS, TOPK), jnp.float32) ** block_levels(streams_of[17], (SEQS, TOPK), ((0, 128),), -0.2, 0.2)), 0.1, 1.0)
    expert_gate = normal_values(streams_of[18], (EXPERTS, D, FF), D ** -0.5, 0.1875, ((0, 128), (2, 4)))
    expert_up = normal_values(streams_of[19], (EXPERTS, D, FF), D ** -0.5, 0.1875, ((0, 128), (2, 4)))
    expert_down = normal_values(streams_of[20], (EXPERTS, FF, D), FF ** -0.5, 0.25, ((0, 128), (1, 4)))
    return {"tokens": tokens, "attn_gain": attn_gain, "q_down": q_down, "kv_down": kv_down, "rope_down": rope_down, "q_latent_gain": q_latent_gain, "kv_latent_gain": kv_latent_gain, "q_up": q_up, "query_gain": query_gain, "key_up": key_up, "value_up": value_up, "attn_out": attn_out, "cache_latent": cache_latent, "cache_rope": cache_rope, "lengths": lengths, "moe_gain": moe_gain, "route": route, "route_weight": route_weight, "expert_gate": expert_gate, "expert_up": expert_up, "expert_down": expert_down}


EPS = 1e-06
ROPE_BASE = 10000.0

def rms_scaled(values_in, gain_vec):
    values_in = values_in.astype(jnp.float32)
    return values_in * lax.rsqrt(lax.optimization_barrier(jnp.mean(values_in * values_in, axis=-1, keepdims=True)) + EPS) * gain_vec

def rotate_last(values_in, positions):
    half_dim = values_in.shape[-1] // 2
    inverse = ROPE_BASE ** (-jnp.arange(half_dim, dtype=jnp.float32) / half_dim)
    angles = positions.astype(jnp.float32)[..., None] * inverse
    lower_half = values_in[..., :half_dim]
    upper_half = values_in[..., half_dim:]
    return jnp.concatenate([lower_half * jnp.cos(angles) - upper_half * jnp.sin(angles), upper_half * jnp.cos(angles) + lower_half * jnp.sin(angles)], -1)

def rotate_rows(values_in, positions):
    half_dim = values_in.shape[1] // 2
    inverse = ROPE_BASE ** (-jnp.arange(half_dim, dtype=jnp.float32) / half_dim)
    angles = inverse[:, None] * positions.astype(jnp.float32)[None, :]
    lower_half = values_in[:, :half_dim]
    upper_half = values_in[:, half_dim:]
    return jnp.concatenate([lower_half * jnp.cos(angles) - upper_half * jnp.sin(angles), upper_half * jnp.cos(angles) + lower_half * jnp.sin(angles)], 1)

def reference(tokens, attn_gain, q_down, kv_down, rope_down, q_latent_gain, kv_latent_gain, q_up, query_gain, key_up, value_up, attn_out, cache_latent, cache_rope, lengths, moe_gain, route, route_weight, expert_gate, expert_up, expert_down):
    score_scale = QK ** (-0.5)
    normed = rms_scaled(tokens, attn_gain).astype(jnp.bfloat16)
    q_raw = jnp.dot(normed, q_down, preferred_element_type=jnp.float32).astype(jnp.bfloat16)
    kv_raw = jnp.dot(normed, kv_down, preferred_element_type=jnp.float32).astype(jnp.bfloat16)
    new_rope = jnp.dot(normed, rope_down, preferred_element_type=jnp.float32).astype(jnp.bfloat16)
    q_lat = rms_scaled(q_raw, q_latent_gain).astype(jnp.bfloat16)
    new_latent = rms_scaled(kv_raw, kv_latent_gain).astype(jnp.bfloat16)
    query_head = rms_scaled(jnp.dot(q_lat, q_up, preferred_element_type=jnp.float32).reshape(SEQS, HEADS, QK), query_gain)
    query_head = jnp.concatenate([query_head[..., :NOPE], rotate_last(query_head[..., NOPE:], lengths[:, None])], -1).astype(jnp.bfloat16)
    absorbed = jnp.einsum('shn,rhn->shr', query_head[..., :NOPE].astype(jnp.float32), key_up.reshape(KV_RANK, HEADS, NOPE).astype(jnp.float32)).astype(jnp.bfloat16)
    rot_query = query_head[..., NOPE:]
    key_new = rotate_last(new_rope.astype(jnp.float32), lengths).astype(jnp.bfloat16)
    self_score = (jnp.einsum('shr,sr->sh', absorbed.astype(jnp.float32), new_latent.astype(jnp.float32)) + jnp.einsum('shp,sp->sh', rot_query.astype(jnp.float32), key_new.astype(jnp.float32))) * score_scale

    def attend(block_data):
        absorbed_b, rot_b, cache_b, rope_b, len_b, self_b, latent_b = block_data
        positions = jnp.arange(CACHE_LEN, dtype=jnp.int32)
        rotated_keys = rotate_rows(rope_b.astype(jnp.float32), positions).astype(jnp.bfloat16)
        scores = (jnp.einsum('shr,sjr->shj', absorbed_b.astype(jnp.float32), cache_b.astype(jnp.float32)) + jnp.einsum('shp,spj->shj', rot_b.astype(jnp.float32), rotated_keys.astype(jnp.float32))) * score_scale
        valid_keys = positions[None, :] < len_b[:, None]
        masked = jnp.where(valid_keys[:, None, :], scores, -jnp.inf)
        row_max = jnp.maximum(lax.optimization_barrier(jnp.max(masked, axis=-1)), self_b)
        weights = jnp.exp(masked - row_max[..., None])
        self_weight = jnp.exp(self_b - row_max)
        total_weight = lax.optimization_barrier(jnp.sum(weights, axis=-1)) + self_weight
        latent_sum = jnp.einsum('shj,sjr->shr', weights.astype(jnp.bfloat16).astype(jnp.float32), cache_b.astype(jnp.float32))
        latent_sum = latent_sum + self_weight.astype(jnp.bfloat16).astype(jnp.float32)[..., None] * latent_b.astype(jnp.float32)[:, None, :]
        return (latent_sum / total_weight[..., None]).astype(jnp.bfloat16)

    def split_seqs(array_in):
        return array_in.reshape((SEQS // SEQ_DEV, SEQ_DEV) + array_in.shape[1:])
    attended = lax.map(attend, tuple((split_seqs(a) for a in (absorbed, rot_query, cache_latent, cache_rope, lengths, self_score, new_latent))))
    attended = attended.reshape(SEQS, HEADS, KV_RANK)
    head_values = jnp.einsum('shr,rhv->shv', attended.astype(jnp.float32), value_up.reshape(KV_RANK, HEADS, VDIM).astype(jnp.float32)).astype(jnp.bfloat16)
    group_cols = HEADS * VDIM // N_TP
    partials = jnp.einsum('sgk,gkd->gsd', head_values.reshape(SEQS, N_TP, group_cols).astype(jnp.float32), attn_out.reshape(N_TP, group_cols, D).astype(jnp.float32))
    head_sum = lax.optimization_barrier(jnp.sum(partials.astype(jnp.bfloat16).astype(jnp.float32), axis=0))
    attn_resid = (tokens.astype(jnp.float32) + head_sum).astype(jnp.bfloat16)
    moe_input = rms_scaled(attn_resid, moe_gain).astype(jnp.bfloat16)
    rows_dev = SEQ_DEV * TOPK
    route_blocks = route.reshape(N_EP, rows_dev)
    same_expert = route_blocks[:, :, None] == route_blocks[:, None, :]
    earlier = jnp.arange(rows_dev)[None, :] < jnp.arange(rows_dev)[:, None]
    slot_rank = lax.optimization_barrier(jnp.sum(same_expert & earlier[None], axis=-1)).astype(jnp.int32)
    slot_index = (jnp.arange(N_EP, dtype=jnp.int32)[:, None] * CAP + slot_rank).reshape(-1)
    flat_route = route.reshape(-1)
    buffer = jnp.zeros((EXPERTS, N_EP * CAP, D), jnp.bfloat16).at[flat_route, slot_index].set(jnp.repeat(moe_input, TOPK, axis=0))

    def expert(block_data):
        row_data, gate_weight, up_weight, down_weight = block_data
        gate_pre = jnp.dot(row_data, gate_weight, preferred_element_type=jnp.float32)
        up_pre = jnp.dot(row_data, up_weight, preferred_element_type=jnp.float32)
        hidden = (jax.nn.silu(gate_pre) * up_pre).astype(jnp.bfloat16)
        ff_part = FF // N_TP
        partial_value = jnp.einsum('rgf,gfd->grd', hidden.reshape(-1, N_TP, ff_part).astype(jnp.float32), down_weight.reshape(N_TP, ff_part, D).astype(jnp.float32))
        return lax.optimization_barrier(jnp.sum(partial_value.astype(jnp.bfloat16).astype(jnp.float32), axis=0)).astype(jnp.bfloat16)
    outputs = lax.map(expert, (buffer, expert_gate, expert_up, expert_down))
    picked = outputs[flat_route, slot_index].astype(jnp.float32).reshape(SEQS, TOPK, D)
    mixed_out = (attn_resid.astype(jnp.float32) + lax.optimization_barrier(jnp.sum(picked * route_weight[..., None], axis=1))).astype(jnp.bfloat16)
    return (mixed_out, new_latent, new_rope)
```

```python
import jax
import jax.numpy as jnp
from jax import lax
from jax.sharding import Mesh
from jax.sharding import PartitionSpec as P

NOPE = 64
VDIM = 64
QK = 96
EPG = 8
EP = ("ep_0", "ep_1", "ep_2")
CHIPS = ("ep_0", "ep_1")
CORE = "ep_2"
GROUP_CAP = 2
EXTRA = 128
EP_TP = ("ep_0", "ep_1", "ep_2", "tp")


EPS = 1e-06
ROPE_BASE = 10000.0


def sent_together(arrays, axis, split_dim, concat_dim, along):
    ends, at = ([], 0)
    for a in arrays[:-1]:
        at += a.shape[along]
        ends.append(at)
    both = jnp.concatenate(arrays, axis=along)
    return tuple(
        jnp.split(
            lax.all_to_all(both, axis, split_axis=split_dim, concat_axis=concat_dim, tiled=True),
            ends,
            axis=along,
        )
    )


def sent_to_all(shard, axis):
    size = lax.axis_size(axis)
    return lax.all_to_all(
        jnp.broadcast_to(shard[None], (size, *shard.shape)), axis, 0, 0, tiled=True
    )


def of_everyone(shard, axis):
    return sent_to_all(shard, axis).astype(jnp.float32).sum(axis=0)


def in_order(parts, dim):
    shape = list(parts.shape[1:])
    shape[dim] *= parts.shape[0]
    return jnp.moveaxis(parts, 0, dim).reshape(shape)


def gathered_copies(shard, axis, dim):
    parts = sent_to_all(shard, axis)
    return in_order(parts, dim)


def in_blocks(shard, dim, size):
    before, after = (shard.shape[:dim], shard.shape[dim + 1 :])
    return jnp.moveaxis(shard.reshape(*before, size, -1, *after), dim, 0)


def sent_and_summed(shard, axis, dim):
    parts = in_blocks(shard, dim, lax.axis_size(axis))
    arrived = lax.all_to_all(parts, axis, split_axis=0, concat_axis=0, tiled=True)
    return arrived.astype(jnp.float32).sum(axis=0)


def rms_scaled(values_in, gain_vec):
    values_in = values_in.astype(jnp.float32)
    return (
        values_in
        * lax.rsqrt(jnp.mean(values_in * values_in, axis=-1, keepdims=True) + EPS)
        * gain_vec
    )


def rotate_last(values_in, positions):
    half_dim = values_in.shape[-1] // 2
    inverse = ROPE_BASE ** (-jnp.arange(half_dim, dtype=jnp.float32) / half_dim)
    angles = positions.astype(jnp.float32)[..., None] * inverse
    lower_half = values_in[..., :half_dim]
    upper_half = values_in[..., half_dim:]
    return jnp.concatenate(
        [
            lower_half * jnp.cos(angles) - upper_half * jnp.sin(angles),
            upper_half * jnp.cos(angles) + lower_half * jnp.sin(angles),
        ],
        -1,
    )


def rotate_rows(values_in, positions):
    half_dim = values_in.shape[1] // 2
    inverse = ROPE_BASE ** (-jnp.arange(half_dim, dtype=jnp.float32) / half_dim)
    angles = inverse[:, None] * positions.astype(jnp.float32)[None, :]
    lower_half = values_in[:, :half_dim]
    upper_half = values_in[:, half_dim:]
    return jnp.concatenate(
        [
            lower_half * jnp.cos(angles) - upper_half * jnp.sin(angles),
            upper_half * jnp.cos(angles) + lower_half * jnp.sin(angles),
        ],
        1,
    )


def shards(
    tokens,
    attn_gain,
    q_down,
    kv_down,
    rope_down,
    q_latent_gain,
    kv_latent_gain,
    q_up,
    query_gain,
    key_up,
    value_up,
    attn_out,
    cache_latent,
    cache_rope,
    lengths,
    moe_gain,
    route,
    route_weight,
    expert_gate,
    expert_up,
    expert_down,
):
    score_scale = QK ** (-0.5)
    tp_count = lax.axis_size("tp")
    tp_index = lax.axis_index("tp")
    normed = rms_scaled(tokens, attn_gain).astype(jnp.bfloat16)
    q_part = jnp.dot(normed, q_down, preferred_element_type=jnp.float32).astype(jnp.bfloat16)
    kv_part = jnp.dot(normed, kv_down, preferred_element_type=jnp.float32).astype(jnp.bfloat16)
    both = gathered_copies(jnp.concatenate([q_part, kv_part], axis=0), "tp", 1)
    q_raw, kv_raw = jnp.split(both, 2, axis=0)
    new_rope = jnp.dot(normed, rope_down, preferred_element_type=jnp.float32).astype(jnp.bfloat16)
    q_lat = rms_scaled(q_raw, q_latent_gain).astype(jnp.bfloat16)
    latent_new = rms_scaled(kv_raw, kv_latent_gain).astype(jnp.bfloat16)
    kv_cols = kv_part.shape[1]
    new_latent = lax.dynamic_slice_in_dim(latent_new, tp_index * kv_cols, kv_cols, 1)
    heads_here = query_gain.shape[0]
    seq_count = tokens.shape[0]
    query_head = rms_scaled(
        jnp.dot(q_lat, q_up, preferred_element_type=jnp.float32).reshape(seq_count, heads_here, QK),
        query_gain,
    )
    query_head = jnp.concatenate(
        [query_head[..., :NOPE], rotate_last(query_head[..., NOPE:], lengths[:, None])], -1
    ).astype(jnp.bfloat16)
    absorbed = jnp.einsum(
        "shn,rhn->shr",
        query_head[..., :NOPE],
        key_up.reshape(-1, heads_here, NOPE),
        preferred_element_type=jnp.float32,
    ).astype(jnp.bfloat16)
    rot_query = query_head[..., NOPE:]
    absorbed_mine, rot_mine = sent_together((absorbed, rot_query), "tp", 0, 1, 2)
    seqs_mine = cache_latent.shape[0]
    first_seq = tp_index * seqs_mine
    len_mine = lax.dynamic_slice_in_dim(lengths, first_seq, seqs_mine, 0)
    latent_mine = lax.dynamic_slice_in_dim(latent_new, first_seq, seqs_mine, 0)
    key_new = rotate_last(
        lax.dynamic_slice_in_dim(new_rope, first_seq, seqs_mine, 0).astype(jnp.float32), len_mine
    ).astype(jnp.bfloat16)
    positions = jnp.arange(cache_latent.shape[1], dtype=jnp.int32)
    rotated_keys = rotate_rows(cache_rope.astype(jnp.float32), positions).astype(jnp.bfloat16)
    scores = (
        jnp.einsum("shr,sjr->shj", absorbed_mine, cache_latent, preferred_element_type=jnp.float32)
        + jnp.einsum("shp,spj->shj", rot_mine, rotated_keys, preferred_element_type=jnp.float32)
    ) * score_scale
    self_score = (
        jnp.einsum("shr,sr->sh", absorbed_mine, latent_mine, preferred_element_type=jnp.float32)
        + jnp.einsum("shp,sp->sh", rot_mine, key_new, preferred_element_type=jnp.float32)
    ) * score_scale
    valid_keys = positions[None, :] < len_mine[:, None]
    masked = jnp.where(valid_keys[:, None, :], scores, -jnp.inf)
    row_max = jnp.maximum(jnp.max(masked, axis=-1), self_score)
    weights = jnp.exp(masked - row_max[..., None])
    self_weight = jnp.exp(self_score - row_max)
    total_weight = jnp.sum(weights, axis=-1) + self_weight
    latent_sum = jnp.einsum(
        "shj,sjr->shr",
        weights.astype(jnp.bfloat16),
        cache_latent,
        preferred_element_type=jnp.float32,
    )
    latent_sum = (
        latent_sum
        + self_weight.astype(jnp.bfloat16).astype(jnp.float32)[..., None]
        * latent_mine.astype(jnp.float32)[:, None, :]
    )
    attended = (latent_sum / total_weight[..., None]).astype(jnp.bfloat16)
    attended_heads = lax.all_to_all(attended, "tp", split_axis=1, concat_axis=0, tiled=True)
    head_values = (
        jnp.einsum(
            "shr,rhv->shv",
            attended_heads,
            value_up.reshape(-1, heads_here, VDIM),
            preferred_element_type=jnp.float32,
        )
        .astype(jnp.bfloat16)
        .reshape(seq_count, heads_here * VDIM)
    )
    head_sum = of_everyone(
        jnp.dot(head_values, attn_out, preferred_element_type=jnp.float32).astype(jnp.bfloat16),
        "tp",
    ).astype(jnp.float32)
    attn_resid = (tokens.astype(jnp.float32) + head_sum).astype(jnp.bfloat16)
    moe_input = rms_scaled(attn_resid, moe_gain).astype(jnp.bfloat16)
    group_of = route[:, 0] // EPG
    order = jnp.arange(seq_count, dtype=jnp.int32)
    earlier = (group_of[:, None] == group_of[None, :]) & (order[None, :] < order[:, None])
    slot = group_of * GROUP_CAP + jnp.sum(earlier, axis=1, dtype=jnp.int32)
    chips = lax.axis_size(CHIPS)
    cores = lax.axis_size(CORE)
    chips_in_group = EPG // cores
    slots = chips // chips_in_group * GROUP_CAP
    placing = (jnp.arange(slots, dtype=jnp.int32)[:, None] == slot[None, :]).astype(jnp.bfloat16)
    lane = jnp.arange(EXTRA, dtype=jnp.int32)
    named = (route % EPG)[:, :, None] == lane[None, None, :]
    weight_cols = jnp.sum(jnp.where(named, route_weight[..., None], 0.0), axis=1).astype(jnp.bfloat16)
    width = tokens.shape[1]
    rows = jnp.concatenate([moe_input, weight_cols], axis=1)
    packed = jnp.dot(placing, rows, preferred_element_type=jnp.float32).astype(jnp.bfloat16)
    packed = jnp.broadcast_to(
        packed.reshape(-1, 1, GROUP_CAP, width + EXTRA),
        (slots // GROUP_CAP, chips_in_group, GROUP_CAP, width + EXTRA),
    ).reshape(chips, GROUP_CAP, width + EXTRA)
    arrived = lax.all_to_all(packed, CHIPS, 0, 0, tiled=True).reshape(-1, width + EXTRA)
    swap = [(i, cores - 1 - i) for i in range(cores)]
    other = lax.ppermute(arrived, CORE, swap)
    expert_here = lax.axis_index(EP) % EPG
    mine = lane == expert_here

    def expert(block):
        inside = block[:, :width]
        gate_pre = jnp.dot(inside, expert_gate[0], preferred_element_type=jnp.float32)
        up_pre = jnp.dot(inside, expert_up[0], preferred_element_type=jnp.float32)
        hidden = (jax.nn.silu(gate_pre) * up_pre).astype(jnp.bfloat16)
        scale = jnp.sum(
            jnp.where(mine, block[:, width:].astype(jnp.float32), 0.0), axis=1, keepdims=True
        )
        return jnp.dot(hidden, expert_down[0], preferred_element_type=jnp.float32) * scale

    own = expert(arrived)
    back = lax.ppermute(expert(other).astype(jnp.bfloat16), CORE, swap)
    sums = (own + back.astype(jnp.float32)).astype(jnp.bfloat16)
    returned = lax.all_to_all(
        sums.reshape(chips, GROUP_CAP, width), CHIPS, 0, 0, tiled=True
    ).reshape(-1, chips_in_group, GROUP_CAP, width)
    totals = jnp.sum(returned.astype(jnp.float32), axis=1).astype(jnp.bfloat16)
    picked = jnp.dot(
        placing.T, totals.reshape(slots, width), preferred_element_type=jnp.float32
    ).astype(jnp.bfloat16)
    quarter_cols = width // tp_count
    residual = lax.dynamic_slice_in_dim(attn_resid, tp_index * quarter_cols, quarter_cols, 1)
    mixed_out = (residual.astype(jnp.float32) + sent_and_summed(picked, "tp", 1)).astype(
        jnp.bfloat16
    )
    return (mixed_out, new_latent, new_rope)


def solution(mesh):
    torus = Mesh(mesh.devices.reshape(8, 8, 2, mesh.shape["tp"]), ("ep_0", "ep_1", "ep_2", "tp"))
    placed = (
        P(EP, None),
        P(),
        P(None, "tp"),
        P(None, "tp"),
        P(),
        P(),
        P(),
        P(None, "tp"),
        P("tp", None),
        P(None, "tp"),
        P(None, "tp"),
        P("tp", None),
        P(EP_TP, None, None),
        P(EP_TP, None, None),
        P(EP),
        P(),
        P(EP, None),
        P(EP, None),
        P(EP, None, "tp"),
        P(EP, None, "tp"),
        P(EP, "tp", None),
    )
    return jax.shard_map(
        shards,
        mesh=torus,
        in_specs=placed,
        out_specs=(P(EP, "tp"), P(EP, "tp"), P(EP, None)),
        check_vma=False,
    )
```

```python
import jax
import jax.numpy as jnp
from jax import lax
from jax.experimental import pallas as pl
from jax.sharding import Mesh
from jax.sharding import PartitionSpec as P

NOPE = 64
VDIM = 64
QK = 96
EPG = 8
EP = ("ep_0", "ep_1", "ep_2")
CHIPS = ("ep_0", "ep_1")
CORE = "ep_2"
GROUP_CAP = 2
EXTRA = 128
EP_TP = ("ep_0", "ep_1", "ep_2", "tp")


EPS = 1e-06
ROPE_BASE = 10000.0


def rms_scaled(values_in, gain_vec):
    values_in = values_in.astype(jnp.float32)
    return (
        values_in
        * lax.rsqrt(jnp.mean(values_in * values_in, axis=-1, keepdims=True) + EPS)
        * gain_vec
    )


def rotate_last(values_in, positions):
    half_dim = values_in.shape[-1] // 2
    inverse = ROPE_BASE ** (-jnp.arange(half_dim, dtype=jnp.float32) / half_dim)
    angles = positions.astype(jnp.float32)[..., None] * inverse
    lower_half = values_in[..., :half_dim]
    upper_half = values_in[..., half_dim:]
    return jnp.concatenate(
        [
            lower_half * jnp.cos(angles) - upper_half * jnp.sin(angles),
            upper_half * jnp.cos(angles) + lower_half * jnp.sin(angles),
        ],
        -1,
    )


def rotate_rows(values_in, positions):
    half_dim = values_in.shape[1] // 2
    inverse = ROPE_BASE ** (-jnp.arange(half_dim, dtype=jnp.float32) / half_dim)
    angles = inverse[:, None] * positions.astype(jnp.float32)[None, :]
    lower_half = values_in[:, :half_dim]
    upper_half = values_in[:, half_dim:]
    return jnp.concatenate(
        [
            lower_half * jnp.cos(angles) - upper_half * jnp.sin(angles),
            upper_half * jnp.cos(angles) + lower_half * jnp.sin(angles),
        ],
        1,
    )


F32 = jnp.float32
BF16 = jnp.bfloat16
NEG = -1e30


def dot(a, b):
    return jnp.dot(a, b, preferred_element_type=F32)


def dot_t(a, b):
    return lax.dot_general(a, b, (((1,), (1,)), ((), ())), preferred_element_type=F32)


def run(body, outs, *args, flops=2_000_000):
    moved = sum(a.size * a.dtype.itemsize for a in args)
    return pl.pallas_call(
        body,
        out_shape=outs,
        cost_estimate=pl.CostEstimate(flops=flops, transcendentals=0, bytes_accessed=moved),
    )(*args)


def down_body(tok_ref, gain_ref, q_ref, kv_ref, rope_ref, both_ref, new_rope_ref):
    normed = rms_scaled(tok_ref[...], gain_ref[...]).astype(BF16)
    rows = normed.shape[0]
    q_part = dot(normed, q_ref[...]).astype(BF16)
    kv_part = dot(normed, kv_ref[...]).astype(BF16)
    for i in range(both_ref.shape[0]):
        both_ref[i, :rows, :] = q_part
        both_ref[i, rows:, :] = kv_part
    new_rope_ref[...] = dot(normed, rope_ref[...]).astype(BF16)


def query_body(
    arr_ref, q_gain_ref, kv_gain_ref, q_up_ref, head_gain_ref, key_up_ref, cos_ref, sin_ref,
    send_ref, latent_ref,
):
    peers, both, _ = arr_ref.shape
    rows = both // 2
    rank = key_up_ref.shape[0]
    half = cos_ref.shape[1]
    q_raw = jnp.concatenate([arr_ref[i, :rows, :] for i in range(peers)], axis=1)
    kv_raw = jnp.concatenate([arr_ref[i, rows:, :] for i in range(peers)], axis=1)
    latent_ref[...] = rms_scaled(kv_raw, kv_gain_ref[...]).astype(BF16)
    q_lat = rms_scaled(q_raw, q_gain_ref[...]).astype(BF16)
    query = dot(q_lat, q_up_ref[...])
    each = rows // peers
    for h in range(head_gain_ref.shape[0]):
        one = rms_scaled(query[:, h * QK : (h + 1) * QK], head_gain_ref[h : h + 1, :])
        lower = one[:, NOPE : NOPE + half]
        upper = one[:, NOPE + half :]
        turned = jnp.concatenate(
            [
                lower * cos_ref[...] - upper * sin_ref[...],
                upper * cos_ref[...] + lower * sin_ref[...],
            ],
            axis=1,
        )
        absorbed = dot_t(one[:, :NOPE].astype(BF16), key_up_ref[:, h * NOPE : (h + 1) * NOPE])
        for i in range(peers):
            at = slice(h * each, (h + 1) * each)
            send_ref[i, at, :rank] = absorbed[i * each : (i + 1) * each].astype(BF16)
            send_ref[i, at, rank:] = turned[i * each : (i + 1) * each].astype(BF16)


def attend_body(arr_ref, cache_ref, keys_ref, latent_ref, key_new_ref, len_ref, out_ref):
    seqs, places, rank = cache_ref.shape
    peers, each, _ = arr_ref.shape
    rows = peers * each
    arrived = arr_ref[...].reshape(rows, arr_ref.shape[2])
    absorbed = arrived[:, :rank]
    turned = arrived[:, rank:]
    scale = QK ** (-0.5)
    row_seq = lax.broadcasted_iota(jnp.int32, (rows, 1), 0) % seqs
    scores = jnp.zeros((rows, places), F32)
    for s in range(seqs):
        part = dot_t(absorbed, cache_ref[s]) + dot(turned, keys_ref[s])
        scores = jnp.where(row_seq == s, part, scores)
    spread = rows // seqs
    latent = jnp.concatenate([latent_ref[...].astype(F32)] * spread, axis=0)
    key_new = jnp.concatenate([key_new_ref[...].astype(F32)] * spread, axis=0)
    self_score = (
        jnp.sum(absorbed.astype(F32) * latent, axis=1, keepdims=True)
        + jnp.sum(turned.astype(F32) * key_new, axis=1, keepdims=True)
    ) * scale
    place = lax.broadcasted_iota(jnp.int32, (rows, places), 1)
    valid = place < len_ref[...]
    scores = jnp.where(valid, scores * scale, NEG)
    top = jnp.maximum(jnp.max(scores, axis=1, keepdims=True), self_score)
    weights = jnp.where(valid, jnp.exp(scores - top), 0.0)
    self_weight = jnp.exp(self_score - top)
    total = jnp.sum(weights, axis=1, keepdims=True) + self_weight
    summed = self_weight.astype(BF16).astype(F32) * latent
    for s in range(seqs):
        summed = summed + dot(jnp.where(row_seq == s, weights, 0.0).astype(BF16), cache_ref[s])
    out_ref[...] = (summed / total).astype(BF16).reshape(out_ref.shape)


def heads_body(arr_ref, value_ref, out_w_ref, out_ref):
    peers, each, rank = arr_ref.shape
    rows = peers * each
    heads = value_ref.shape[1] // VDIM
    seqs = each // heads
    values = dot(arr_ref[...].reshape(rows, rank), value_ref[...]).astype(BF16)
    to = lax.broadcasted_iota(jnp.int32, (rows // heads, rows), 0)
    at = lax.broadcasted_iota(jnp.int32, (rows // heads, rows), 1)
    column = lax.broadcasted_iota(jnp.int32, (rows // heads, heads * VDIM), 1)
    picked = jnp.zeros((rows // heads, heads * VDIM), F32)
    for h in range(heads):
        chosen = (at == (to // seqs) * each + h * seqs + to % seqs).astype(BF16)
        picked = jnp.where(column // VDIM == h, dot(chosen, values), picked)
    partial = dot(picked.astype(BF16), out_w_ref[...]).astype(BF16)
    for i in range(out_ref.shape[0]):
        out_ref[i] = partial


def expert_body(rows_ref, mine_ref, gate_ref, up_ref, down_ref, out_ref):
    width = down_ref.shape[1]
    inside = rows_ref[:, :width]
    gate_pre = dot(inside, gate_ref[...])
    up_pre = dot(inside, up_ref[...])
    hidden = (gate_pre / (1.0 + jnp.exp(-gate_pre)) * up_pre).astype(BF16)
    scale = jnp.sum(rows_ref[:, width:].astype(F32) * mine_ref[...], axis=1, keepdims=True)
    out_ref[...] = (dot(hidden, down_ref[...]) * scale).astype(out_ref.dtype)


def shards(
    tokens,
    attn_gain,
    q_down,
    kv_down,
    rope_down,
    q_latent_gain,
    kv_latent_gain,
    q_up,
    query_gain,
    key_up,
    value_up,
    attn_out,
    cache_latent,
    cache_rope,
    lengths,
    moe_gain,
    route,
    route_weight,
    expert_gate,
    expert_up,
    expert_down,
):
    tp_count = lax.axis_size("tp")
    tp_index = lax.axis_index("tp")
    seq_count, width = tokens.shape
    kv_cols = kv_down.shape[1]
    rank = cache_latent.shape[2]
    heads_here = query_gain.shape[0]
    seqs_mine = cache_latent.shape[0]
    first_seq = tp_index * seqs_mine
    both, new_rope = run(
        down_body,
        (
            jax.ShapeDtypeStruct((tp_count, 2 * seq_count, kv_cols), BF16),
            jax.ShapeDtypeStruct((seq_count, rope_down.shape[1]), BF16),
        ),
        tokens,
        attn_gain[None],
        q_down,
        kv_down,
        rope_down,
    )
    latents = lax.all_to_all(both, "tp", 0, 0, tiled=True)
    half_dim = rope_down.shape[1] // 2
    inverse = ROPE_BASE ** (-jnp.arange(half_dim, dtype=F32) / half_dim)
    angles = lengths.astype(F32)[:, None] * inverse
    each = heads_here * seqs_mine
    send, latent_new = run(
        query_body,
        (
            jax.ShapeDtypeStruct((tp_count, each, rank + 2 * half_dim), BF16),
            jax.ShapeDtypeStruct((seq_count, rank), BF16),
        ),
        latents,
        q_latent_gain[None],
        kv_latent_gain[None],
        q_up,
        query_gain,
        key_up,
        jnp.cos(angles),
        jnp.sin(angles),
    )
    queries = lax.all_to_all(send, "tp", 0, 0, tiled=True)
    new_latent = lax.dynamic_slice_in_dim(latent_new, tp_index * kv_cols, kv_cols, 1)
    len_mine = lax.dynamic_slice_in_dim(lengths, first_seq, seqs_mine, 0)
    latent_mine = lax.dynamic_slice_in_dim(latent_new, first_seq, seqs_mine, 0)
    key_new = rotate_last(
        lax.dynamic_slice_in_dim(new_rope, first_seq, seqs_mine, 0).astype(F32), len_mine
    ).astype(BF16)
    positions = jnp.arange(cache_latent.shape[1], dtype=jnp.int32)
    rotated_keys = rotate_rows(cache_rope.astype(F32), positions).astype(BF16)
    attended = run(
        attend_body,
        jax.ShapeDtypeStruct((tp_count, each, rank), BF16),
        queries,
        cache_latent,
        rotated_keys,
        latent_mine,
        key_new,
        jnp.tile(len_mine, tp_count * heads_here)[:, None],
    )
    attended_heads = lax.all_to_all(attended, "tp", 0, 0, tiled=True)
    partials = run(
        heads_body,
        jax.ShapeDtypeStruct((tp_count, seq_count, width), BF16),
        attended_heads,
        value_up,
        attn_out,
    )
    head_sum = lax.all_to_all(partials, "tp", 0, 0, tiled=True).astype(F32).sum(axis=0)
    attn_resid = (tokens.astype(jnp.float32) + head_sum).astype(jnp.bfloat16)
    moe_input = rms_scaled(attn_resid, moe_gain).astype(jnp.bfloat16)
    group_of = route[:, 0] // EPG
    order = jnp.arange(seq_count, dtype=jnp.int32)
    earlier = (group_of[:, None] == group_of[None, :]) & (order[None, :] < order[:, None])
    slot = group_of * GROUP_CAP + jnp.sum(earlier, axis=1, dtype=jnp.int32)
    chips = lax.axis_size(CHIPS)
    cores = lax.axis_size(CORE)
    chips_in_group = EPG // cores
    slots = chips // chips_in_group * GROUP_CAP
    placing = (jnp.arange(slots, dtype=jnp.int32)[:, None] == slot[None, :]).astype(jnp.bfloat16)
    lane = jnp.arange(EXTRA, dtype=jnp.int32)
    named = (route % EPG)[:, :, None] == lane[None, None, :]
    weight_cols = jnp.sum(jnp.where(named, route_weight[..., None], 0.0), axis=1).astype(jnp.bfloat16)
    rows = jnp.concatenate([moe_input, weight_cols], axis=1)
    packed = jnp.dot(placing, rows, preferred_element_type=jnp.float32).astype(jnp.bfloat16)
    packed = jnp.broadcast_to(
        packed.reshape(-1, 1, GROUP_CAP, width + EXTRA),
        (slots // GROUP_CAP, chips_in_group, GROUP_CAP, width + EXTRA),
    ).reshape(chips, GROUP_CAP, width + EXTRA)
    arrived = lax.all_to_all(packed, CHIPS, 0, 0, tiled=True).reshape(-1, width + EXTRA)
    swap = [(i, cores - 1 - i) for i in range(cores)]
    other = lax.ppermute(arrived, CORE, swap)
    mine = (lane == lax.axis_index(EP) % EPG).astype(F32)[None]

    def expert(block, kind):
        return run(
            expert_body,
            jax.ShapeDtypeStruct((block.shape[0], width), kind),
            block,
            mine,
            expert_gate[0],
            expert_up[0],
            expert_down[0],
            flops=100_000_000,
        )

    own = expert(arrived, F32)
    sent_back = lax.ppermute(expert(other, BF16), CORE, swap)
    quarter_cols = width // tp_count
    sums = (own + sent_back.astype(F32)).astype(BF16)
    sums = sums.reshape(chips, GROUP_CAP, tp_count, quarter_cols).swapaxes(1, 2)
    returned = lax.all_to_all(
        sums.reshape(chips * tp_count, GROUP_CAP, quarter_cols), (*CHIPS, "tp"), 0, 0, tiled=True
    ).reshape(-1, chips_in_group * tp_count, GROUP_CAP, quarter_cols)
    totals = jnp.sum(returned.astype(F32), axis=1).reshape(slots, quarter_cols)
    high = totals.astype(BF16)
    picked = jnp.dot(placing.T, high, preferred_element_type=F32)
    residual = lax.dynamic_slice_in_dim(attn_resid, tp_index * quarter_cols, quarter_cols, 1)
    mixed_out = (residual.astype(F32) + picked).astype(BF16)
    return (mixed_out, new_latent, new_rope)


def solution(mesh):
    torus = Mesh(mesh.devices.reshape(8, 8, 2, mesh.shape["tp"]), ("ep_0", "ep_1", "ep_2", "tp"))
    placed = (
        P(EP, None),
        P(),
        P(None, "tp"),
        P(None, "tp"),
        P(),
        P(),
        P(),
        P(None, "tp"),
        P("tp", None),
        P(None, "tp"),
        P(None, "tp"),
        P("tp", None),
        P(EP_TP, None, None),
        P(EP_TP, None, None),
        P(EP),
        P(),
        P(EP, None),
        P(EP, None),
        P(EP, None, "tp"),
        P(EP, None, "tp"),
        P(EP, "tp", None),
    )
    return jax.shard_map(
        shards,
        mesh=torus,
        in_specs=placed,
        out_specs=(P(EP, "tp"), P(EP, "tp"), P(EP, None)),
        check_vma=False,
    )
```

```python
import jax
import jax.numpy as jnp
import numpy as np
from jax import lax
from jax.experimental import pallas as pl
from jax.experimental.pallas import tpu as pltpu
from jax.sharding import Mesh
from jax.sharding import PartitionSpec as P

NOPE = 64
VDIM = 64
QK = 96
EPG = 8
EP = ("ep_0", "ep_1", "ep_2")
CHIPS = ("ep_0", "ep_1")
CORE = "ep_2"
GROUP_CAP = 2
EXTRA = 128
EP_TP = ("ep_0", "ep_1", "ep_2", "tp")


EPS = 1e-06
ROPE_BASE = 10000.0
F32 = jnp.float32
BF16 = jnp.bfloat16
NEG = -1e30


def rms_scaled(values_in, gain_vec):
    values_in = values_in.astype(jnp.float32)
    return (
        values_in
        * lax.rsqrt(jnp.mean(values_in * values_in, axis=-1, keepdims=True) + EPS)
        * gain_vec
    )


def dot(a, b):
    return jnp.dot(a, b, preferred_element_type=F32)


def dot_t(a, b):
    return lax.dot_general(a, b, (((1,), (1,)), ((), ())), preferred_element_type=F32)


def near(array):
    return pltpu.with_memory_space_constraint(array, pltpu.VMEM)


def far(array):
    return pltpu.with_memory_space_constraint(array, pltpu.HBM)


def run(body, outs, *args, flops=2_000_000, scalars=0):
    moved = sum(a.size * a.dtype.itemsize for a in args)
    return pl.pallas_call(
        body,
        compiler_params=pltpu.CompilerParams(vmem_limit_bytes=16 * 1024 * 1024),
        in_specs=[pl.BlockSpec(memory_space=pltpu.SMEM)] * scalars
        + [pl.BlockSpec(memory_space=pltpu.VMEM)] * (len(args) - scalars),
        out_shape=jax.tree.map(lambda o: pltpu.VMEM(o.shape, o.dtype), outs),
        cost_estimate=pl.CostEstimate(flops=flops, transcendentals=0, bytes_accessed=moved),
    )(*args)


def fetch_body(*refs):
    count = (len(refs) - 1) // 2
    sems = refs[-1]
    copies = [
        pltpu.make_async_copy(refs[i], refs[count + i], sems.at[i]) for i in range(count)
    ]
    for copy in copies:
        copy.start()
    for copy in copies:
        copy.wait()


def fetched(*arrays):
    moved = sum(a.size * a.dtype.itemsize for a in arrays)
    return pl.pallas_call(
        fetch_body,
        compiler_params=pltpu.CompilerParams(vmem_limit_bytes=1024 * 1024),
        in_specs=[pl.BlockSpec(memory_space=pltpu.HBM)] * len(arrays),
        out_specs=[pl.BlockSpec(memory_space=pltpu.VMEM)] * len(arrays),
        out_shape=[pltpu.VMEM(a.shape, a.dtype) for a in arrays],
        scratch_shapes=[pltpu.SemaphoreType.DMA((len(arrays),))],
        cost_estimate=pl.CostEstimate(flops=2_000_000, transcendentals=0, bytes_accessed=moved),
    )(*[far(a) for a in arrays])


def down_body(*refs):
    hbm, (both_ref, new_rope_ref), near_refs, sems = refs[:5], refs[5:7], refs[7:12], refs[12]
    copies = [pltpu.make_async_copy(hbm[i], near_refs[i], sems.at[i]) for i in range(5)]
    for copy in copies:
        copy.start()
    tok_ref, gain_ref, q_ref, kv_ref, rope_ref = near_refs
    copies[0].wait()
    copies[1].wait()
    normed = rms_scaled(tok_ref[...], gain_ref[...]).astype(BF16)
    rows = normed.shape[0]
    copies[2].wait()
    q_part = dot(normed, q_ref[...]).astype(BF16)
    copies[3].wait()
    kv_part = dot(normed, kv_ref[...]).astype(BF16)
    for i in range(both_ref.shape[0]):
        both_ref[i, :rows, :] = q_part
        both_ref[i, rows:, :] = kv_part
    copies[4].wait()
    new_rope_ref[...] = dot_t(normed, rope_ref[...]).astype(BF16)


def down(outs, *args):
    moved = sum(a.size * a.dtype.itemsize for a in args)
    return pl.pallas_call(
        down_body,
        compiler_params=pltpu.CompilerParams(vmem_limit_bytes=16 * 1024 * 1024),
        in_specs=[pl.BlockSpec(memory_space=pltpu.HBM)] * len(args),
        out_specs=[pl.BlockSpec(memory_space=pltpu.VMEM)] * len(outs),
        out_shape=[pltpu.VMEM(o.shape, o.dtype) for o in outs],
        scratch_shapes=[pltpu.VMEM(a.shape, a.dtype) for a in args]
        + [pltpu.SemaphoreType.DMA((len(args),))],
        cost_estimate=pl.CostEstimate(flops=2_000_000, transcendentals=0, bytes_accessed=moved),
    )(*[far(a) for a in args])


def query_body(
    arr_ref, q_gain_ref, kv_gain_ref, q_up_ref, head_gain_ref, key_up_ref, cos_ref, sin_ref,
    send_ref, latent_ref,
):
    peers, both, _ = arr_ref.shape
    rows = both // 2
    rank = key_up_ref.shape[0]
    half = cos_ref.shape[1]
    q_raw = jnp.concatenate([arr_ref[i, :rows, :] for i in range(peers)], axis=1)
    kv_raw = jnp.concatenate([arr_ref[i, rows:, :] for i in range(peers)], axis=1)
    latent_ref[...] = rms_scaled(kv_raw, kv_gain_ref[...]).astype(BF16)
    q_lat = rms_scaled(q_raw, q_gain_ref[...]).astype(BF16)
    query = dot_t(q_lat, q_up_ref[...])
    each = rows // peers
    for h in range(head_gain_ref.shape[0]):
        one = rms_scaled(query[:, h * QK : (h + 1) * QK], head_gain_ref[h : h + 1, :])
        lower = one[:, NOPE : NOPE + half]
        upper = one[:, NOPE + half :]
        turned = jnp.concatenate(
            [
                lower * cos_ref[...] - upper * sin_ref[...],
                upper * cos_ref[...] + lower * sin_ref[...],
            ],
            axis=1,
        )
        absorbed = dot_t(one[:, :NOPE].astype(BF16), key_up_ref[:, h * NOPE : (h + 1) * NOPE])
        for i in range(peers):
            at = slice(h * each, (h + 1) * each)
            send_ref[i, at, :rank] = absorbed[i * each : (i + 1) * each].astype(BF16)
            send_ref[i, at, rank:] = turned[i * each : (i + 1) * each].astype(BF16)


def keys_body(rope_ref, cos_ref, sin_ref, out_ref):
    half = cos_ref.shape[0]
    for s in range(rope_ref.shape[0]):
        lower = rope_ref[s, :half, :].astype(F32)
        upper = rope_ref[s, half:, :].astype(F32)
        out_ref[s, :half, :] = (lower * cos_ref[...] - upper * sin_ref[...]).astype(BF16)
        out_ref[s, half:, :] = (upper * cos_ref[...] + lower * sin_ref[...]).astype(BF16)


def place_body(route_ref, weight_ref, placing_ref, weights_ref):
    topk, rows = route_ref.shape
    slots = placing_ref.shape[0]
    group = route_ref[0:1, :] // EPG
    first = lax.broadcasted_iota(jnp.int32, (rows, rows), 0)
    second = lax.broadcasted_iota(jnp.int32, (rows, rows), 1)
    column = jnp.sum(jnp.where(first == second, group, 0), axis=1, keepdims=True)
    earlier = jnp.where((column == group) & (first < second), 1, 0)
    slot = group * GROUP_CAP + jnp.sum(earlier, axis=0, keepdims=True)
    placing = (lax.broadcasted_iota(jnp.int32, (slots, rows), 0) == slot).astype(BF16)
    placing_ref[...] = placing
    lane = lax.broadcasted_iota(jnp.int32, (EXTRA, rows), 0)
    table = jnp.zeros((EXTRA, rows), F32)
    for k in range(topk):
        table = table + jnp.where(route_ref[k : k + 1, :] % EPG == lane, weight_ref[k : k + 1, :], 0.0)
    weights_ref[...] = dot_t(placing, table.astype(BF16)).astype(BF16)


def attend_body(
    first_ref, arr_ref, cache_ref, keys_ref, latent_ref, rope_ref, cos_ref, sin_ref, len_ref, out_ref
):
    seqs, places, rank = cache_ref.shape
    peers, each, _ = arr_ref.shape
    rows = peers * each
    half = cos_ref.shape[1]
    arrived = arr_ref[...].reshape(rows, arr_ref.shape[2])
    absorbed = arrived[:, :rank]
    turned = arrived[:, rank:]
    scale = QK ** (-0.5)
    row_seq = lax.broadcasted_iota(jnp.int32, (rows, 1), 0) % seqs
    every = latent_ref.shape[0]
    chosen = lax.broadcasted_iota(jnp.int32, (rows, every), 1) == row_seq + first_ref[0]
    lengths = jnp.sum(jnp.where(chosen, len_ref[...], 0), axis=1, keepdims=True)
    chosen = chosen.astype(BF16)
    latent = dot(chosen, latent_ref[...])
    lower = rope_ref[:, :half].astype(F32)
    upper = rope_ref[:, half:].astype(F32)
    key_new = jnp.concatenate(
        [
            lower * cos_ref[...] - upper * sin_ref[...],
            upper * cos_ref[...] + lower * sin_ref[...],
        ],
        axis=1,
    )
    key_new = dot(chosen, key_new.astype(BF16))
    self_score = (
        jnp.sum(absorbed.astype(F32) * latent, axis=1, keepdims=True)
        + jnp.sum(turned.astype(F32) * key_new, axis=1, keepdims=True)
    ) * scale
    scores = jnp.zeros((rows, places), F32)
    for s in range(seqs):
        part = dot_t(absorbed, cache_ref[s]) + dot(turned, keys_ref[s])
        scores = jnp.where(row_seq == s, part, scores)
    valid = lax.broadcasted_iota(jnp.int32, (rows, places), 1) < lengths
    scores = jnp.where(valid, scores * scale, NEG)
    top = jnp.maximum(jnp.max(scores, axis=1, keepdims=True), self_score)
    weights = jnp.where(valid, jnp.exp(scores - top), 0.0)
    self_weight = jnp.exp(self_score - top)
    total = jnp.sum(weights, axis=1, keepdims=True) + self_weight
    summed = self_weight.astype(BF16).astype(F32) * latent
    for s in range(seqs):
        summed = summed + dot(jnp.where(row_seq == s, weights, 0.0).astype(BF16), cache_ref[s])
    out_ref[...] = (summed / total).astype(BF16).reshape(out_ref.shape)


def heads_body(arr_ref, value_ref, out_w_ref, out_ref):
    peers, each, rank = arr_ref.shape
    rows = peers * each
    heads = value_ref.shape[1] // VDIM
    seqs = each // heads
    values = dot(arr_ref[...].reshape(rows, rank), value_ref[...]).astype(BF16)
    to = lax.broadcasted_iota(jnp.int32, (rows // heads, rows), 0)
    at = lax.broadcasted_iota(jnp.int32, (rows // heads, rows), 1)
    column = lax.broadcasted_iota(jnp.int32, (rows // heads, heads * VDIM), 1)
    picked = jnp.zeros((rows // heads, heads * VDIM), F32)
    for h in range(heads):
        chosen = (at == (to // seqs) * each + h * seqs + to % seqs).astype(BF16)
        picked = jnp.where(column // VDIM == h, dot(chosen, values), picked)
    partial = dot(picked.astype(BF16), out_w_ref[...]).astype(BF16)
    for i in range(out_ref.shape[0]):
        out_ref[i] = partial


def expert_body(rows_ref, mine_ref, gate_ref, up_ref, down_ref, out_ref):
    width = down_ref.shape[1]
    inside = rows_ref[:, :width]
    gate_pre = dot(inside, gate_ref[...])
    up_pre = dot(inside, up_ref[...])
    hidden = (gate_pre / (1.0 + jnp.exp(-gate_pre)) * up_pre).astype(BF16)
    scale = jnp.sum(rows_ref[:, width:].astype(F32) * mine_ref[...], axis=1, keepdims=True)
    out_ref[...] = (dot(hidden, down_ref[...]) * scale).astype(out_ref.dtype)


def shards(
    tokens,
    attn_gain,
    q_down,
    kv_down,
    rope_down,
    q_latent_gain,
    kv_latent_gain,
    q_up,
    query_gain,
    key_up,
    value_up,
    attn_out,
    cache_latent,
    cache_rope,
    lengths,
    moe_gain,
    route,
    route_weight,
    expert_gate,
    expert_up,
    expert_down,
):
    tp_count = lax.axis_size("tp")
    tp_index = lax.axis_index("tp")
    seq_count, width = tokens.shape
    kv_cols = kv_down.shape[1]
    rank = cache_latent.shape[2]
    heads_here = query_gain.shape[0]
    seqs_mine = cache_latent.shape[0]
    both, new_rope = down(
        (
            jax.ShapeDtypeStruct((tp_count, 2 * seq_count, kv_cols), BF16),
            jax.ShapeDtypeStruct((seq_count, rope_down.shape[1]), BF16),
        ),
        tokens,
        attn_gain[None],
        q_down,
        kv_down,
        rope_down.T,
    )
    half_dim = rope_down.shape[1] // 2
    turns = ROPE_BASE ** (-np.arange(half_dim, dtype=np.float32) / np.float32(half_dim))
    turns = turns.astype(np.float32)[:, None] * np.arange(cache_latent.shape[1], dtype=np.float32)
    cos_table = jnp.asarray(np.cos(turns.astype(np.float64)).astype(np.float32))
    sin_table = jnp.asarray(np.sin(turns.astype(np.float64)).astype(np.float32))
    both, q_up, key_up, cache_latent, lengths = lax.optimization_barrier(
        (both, q_up, key_up, cache_latent, lengths)
    )
    latents = lax.all_to_all(both, "tp", 0, 0, tiled=True)
    q_up_t, key_up, q_gain, kv_gain, head_gain, cache, cos_table, sin_table, cache_rope = fetched(
        q_up.T,
        key_up,
        q_latent_gain[None],
        kv_latent_gain[None],
        query_gain,
        cache_latent,
        cos_table,
        sin_table,
        cache_rope,
    )
    inverse = ROPE_BASE ** (-jnp.arange(half_dim, dtype=F32) / half_dim)
    angles = lengths.astype(F32)[:, None] * inverse
    cosines = near(jnp.cos(angles))
    sines = near(jnp.sin(angles))
    each = heads_here * seqs_mine
    send, latent_new = run(
        query_body,
        (
            jax.ShapeDtypeStruct((tp_count, each, rank + 2 * half_dim), BF16),
            jax.ShapeDtypeStruct((seq_count, rank), BF16),
        ),
        near(latents),
        near(q_gain),
        near(kv_gain),
        near(q_up_t),
        near(head_gain),
        near(key_up),
        cosines,
        sines,
    )
    send, cache_rope = lax.optimization_barrier((send, cache_rope))
    queries = lax.all_to_all(send, "tp", 0, 0, tiled=True)
    new_latent = lax.dynamic_slice_in_dim(latent_new, tp_index * kv_cols, kv_cols, 1)
    rotated_keys = run(
        keys_body,
        jax.ShapeDtypeStruct(cache_rope.shape, BF16),
        near(cache_rope),
        near(cos_table),
        near(sin_table),
    )
    attended = run(
        attend_body,
        jax.ShapeDtypeStruct((tp_count, each, rank), BF16),
        (tp_index * seqs_mine)[None].astype(jnp.int32),
        near(queries),
        near(cache),
        near(rotated_keys),
        near(latent_new),
        near(new_rope),
        cosines,
        sines,
        near(lengths[None]),
        scalars=1,
    )
    attended_heads = lax.all_to_all(attended, "tp", 0, 0, tiled=True)
    partials = run(
        heads_body,
        jax.ShapeDtypeStruct((tp_count, seq_count, width), BF16),
        near(attended_heads),
        near(value_up),
        near(attn_out),
    )
    head_sum = lax.all_to_all(partials, "tp", 0, 0, tiled=True).astype(F32).sum(axis=0)
    attn_resid = (tokens.astype(jnp.float32) + head_sum).astype(jnp.bfloat16)
    moe_input = rms_scaled(attn_resid, moe_gain).astype(jnp.bfloat16)
    chips = lax.axis_size(CHIPS)
    cores = lax.axis_size(CORE)
    chips_in_group = EPG // cores
    slots = chips // chips_in_group * GROUP_CAP
    placing, packed_weights = run(
        place_body,
        (
            jax.ShapeDtypeStruct((slots, seq_count), BF16),
            jax.ShapeDtypeStruct((slots, EXTRA), BF16),
        ),
        near(route.T),
        near(route_weight.T),
    )
    packed = jnp.dot(placing, moe_input, preferred_element_type=F32).astype(BF16)
    packed = jnp.concatenate([packed, packed_weights], axis=1)
    packed = jnp.broadcast_to(
        packed.reshape(-1, 1, GROUP_CAP, width + EXTRA),
        (slots // GROUP_CAP, chips_in_group, GROUP_CAP, width + EXTRA),
    ).reshape(chips, GROUP_CAP, width + EXTRA)
    arrived = lax.all_to_all(packed, CHIPS, 0, 0, tiled=True).reshape(-1, width + EXTRA)
    swap = [(i, cores - 1 - i) for i in range(cores)]
    other = lax.ppermute(arrived, CORE, swap)
    lane = jnp.arange(EXTRA, dtype=jnp.int32)
    mine = (lane == lax.axis_index(EP) % EPG).astype(F32)[None]

    def expert(block, kind):
        return run(
            expert_body,
            jax.ShapeDtypeStruct((block.shape[0], width), kind),
            near(block),
            near(mine),
            near(expert_gate[0]),
            near(expert_up[0]),
            near(expert_down[0]),
            flops=100_000_000,
        )

    own = expert(arrived, F32)
    sent_back = lax.ppermute(expert(other, BF16), CORE, swap)
    quarter_cols = width // tp_count
    sums = (own + sent_back.astype(F32)).astype(BF16)
    sums = sums.reshape(chips, GROUP_CAP, tp_count, quarter_cols).swapaxes(1, 2)
    returned = lax.all_to_all(
        sums.reshape(chips * tp_count, GROUP_CAP, quarter_cols), (*CHIPS, "tp"), 0, 0, tiled=True
    ).reshape(-1, chips_in_group * tp_count, GROUP_CAP, quarter_cols)
    totals = jnp.sum(returned.astype(F32), axis=1).reshape(slots, quarter_cols)
    high = totals.astype(BF16)
    picked = jnp.dot(placing.T, high, preferred_element_type=F32)
    residual = lax.dynamic_slice_in_dim(attn_resid, tp_index * quarter_cols, quarter_cols, 1)
    mixed_out = (residual.astype(F32) + picked).astype(BF16)
    return (mixed_out, new_latent, new_rope)


def solution(mesh):
    torus = Mesh(mesh.devices.reshape(8, 8, 2, mesh.shape["tp"]), ("ep_0", "ep_1", "ep_2", "tp"))
    placed = (
        P(EP, None),
        P(),
        P(None, "tp"),
        P(None, "tp"),
        P(),
        P(),
        P(),
        P(None, "tp"),
        P("tp", None),
        P(None, "tp"),
        P(None, "tp"),
        P("tp", None),
        P(EP_TP, None, None),
        P(EP_TP, None, None),
        P(EP),
        P(),
        P(EP, None),
        P(EP, None),
        P(EP, None, "tp"),
        P(EP, None, "tp"),
        P(EP, "tp", None),
    )
    return jax.shard_map(
        shards,
        mesh=torus,
        in_specs=placed,
        out_specs=(P(EP, "tp"), P(EP, "tp"), P(EP, None)),
        check_vma=False,
    )
```

```python
import jax
import jax.numpy as jnp
import numpy as np
from jax import lax
from jax.experimental import pallas as pl
from jax.experimental.pallas import tpu as pltpu
from jax.sharding import Mesh
from jax.sharding import PartitionSpec as P

NOPE = 64
VDIM = 64
QK = 96
EPG = 8
EP = ("ep_0", "ep_1", "ep_2")
CHIPS = ("ep_0", "ep_1")
CORE = "ep_2"
GROUP_CAP = 2
EXTRA = 128
EP_TP = ("ep_0", "ep_1", "ep_2", "tp")


EPS = 1e-06
ROPE_BASE = 10000.0
F32 = jnp.float32
BF16 = jnp.bfloat16
NEG = -1e30


def rms_scaled(values_in, gain_vec):
    values_in = values_in.astype(jnp.float32)
    return (
        values_in
        * lax.rsqrt(jnp.mean(values_in * values_in, axis=-1, keepdims=True) + EPS)
        * gain_vec
    )


def dot(a, b):
    return jnp.dot(a, b, preferred_element_type=F32)


def dot_t(a, b):
    return lax.dot_general(a, b, (((1,), (1,)), ((), ())), preferred_element_type=F32)


def near(array):
    return pltpu.with_memory_space_constraint(array, pltpu.VMEM)


def far(array):
    return pltpu.with_memory_space_constraint(array, pltpu.HBM)


def run(body, outs, *args, flops=2_000_000, scalars=0, hbm_in=0, hbm_out=0, sems=0):
    moved = sum(a.size * a.dtype.itemsize for a in args)
    spaces = [pltpu.SMEM] * scalars + [pltpu.HBM] * hbm_in
    spaces += [pltpu.VMEM] * (len(args) - len(spaces))
    kinds = [pltpu.VMEM] * (len(outs) - hbm_out) + [pltpu.HBM] * hbm_out
    place_in = {pltpu.SMEM: lambda a: a, pltpu.HBM: far, pltpu.VMEM: near}
    return pl.pallas_call(
        body,
        compiler_params=pltpu.CompilerParams(vmem_limit_bytes=16 * 1024 * 1024),
        in_specs=[pl.BlockSpec(memory_space=kind) for kind in spaces],
        out_specs=[pl.BlockSpec(memory_space=kind) for kind in kinds],
        out_shape=[kind(o.shape, o.dtype) for kind, o in zip(kinds, outs)],
        scratch_shapes=[pltpu.SemaphoreType.DMA((sems,))] if sems else [],
        cost_estimate=pl.CostEstimate(flops=flops, transcendentals=0, bytes_accessed=moved),
    )(*[place_in[kind](a) for kind, a in zip(spaces, args)])


def place(route_ref, weight_ref, placing_ref, weights_ref):
    topk, rows = route_ref.shape
    slots = placing_ref.shape[0]
    group = route_ref[0:1, :] // EPG
    first = lax.broadcasted_iota(jnp.int32, (rows, rows), 0)
    second = lax.broadcasted_iota(jnp.int32, (rows, rows), 1)
    column = jnp.sum(jnp.where(first == second, group, 0), axis=1, keepdims=True)
    earlier = jnp.where((column == group) & (first < second), 1, 0)
    slot = group * GROUP_CAP + jnp.sum(earlier, axis=0, keepdims=True)
    placing = (lax.broadcasted_iota(jnp.int32, (slots, rows), 0) == slot).astype(BF16)
    placing_ref[...] = placing
    lane = lax.broadcasted_iota(jnp.int32, (EXTRA, rows), 0)
    table = jnp.zeros((EXTRA, rows), F32)
    for k in range(topk):
        table = table + jnp.where(route_ref[k : k + 1, :] % EPG == lane, weight_ref[k : k + 1, :], 0.0)
    weights_ref[...] = dot_t(placing, table.astype(BF16)).astype(BF16)


OWN = 9
MADE = 6


def down_body(*refs):
    count = (len(refs) - MADE - 1) // 2
    hbm, made, last = refs[:count], refs[count : count + MADE], refs[count + MADE : -1]
    sems = refs[-1]
    near_refs = last[count - OWN :] + last[: count - OWN]
    copies = [pltpu.make_async_copy(hbm[i], near_refs[i], sems.at[i]) for i in range(count)]
    for copy in copies:
        copy.start()
    tok_ref, gain_ref, q_ref, kv_ref, rope_ref, len_ref, turn_ref, route_ref, weight_ref = near_refs[
        :OWN
    ]
    both_ref, new_rope_ref, cos_ref, sin_ref, placing_ref, weights_ref = made
    copies[0].wait()
    copies[1].wait()
    normed = rms_scaled(tok_ref[...], gain_ref[...]).astype(BF16)
    rows = normed.shape[0]
    copies[2].wait()
    q_part = dot(normed, q_ref[...]).astype(BF16)
    copies[3].wait()
    kv_part = dot(normed, kv_ref[...]).astype(BF16)
    for i in range(both_ref.shape[0]):
        both_ref[i, :rows, :] = q_part
        both_ref[i, rows:, :] = kv_part
    for i in range(4, OWN):
        copies[i].wait()
    new_rope_ref[...] = dot_t(normed, rope_ref[...]).astype(BF16)
    first = lax.broadcasted_iota(jnp.int32, (rows, rows), 0)
    second = lax.broadcasted_iota(jnp.int32, (rows, rows), 1)
    lengths = jnp.sum(jnp.where(first == second, len_ref[...], 0), axis=1, keepdims=True)
    angles = lengths.astype(F32) * turn_ref[...]
    cos_ref[...] = jnp.cos(angles)
    sin_ref[...] = jnp.sin(angles)
    place(route_ref, weight_ref, placing_ref, weights_ref)
    for copy in copies[OWN:]:
        copy.wait()


def down(made, own, others):
    args = (*own, *others)
    moved = sum(a.size * a.dtype.itemsize for a in args)
    outs = [pltpu.VMEM(o.shape, o.dtype) for o in (*made, *others)]
    return pl.pallas_call(
        down_body,
        compiler_params=pltpu.CompilerParams(vmem_limit_bytes=16 * 1024 * 1024),
        in_specs=[pl.BlockSpec(memory_space=pltpu.HBM)] * len(args),
        out_specs=[pl.BlockSpec(memory_space=pltpu.VMEM)] * len(outs),
        out_shape=outs,
        scratch_shapes=[pltpu.VMEM(a.shape, a.dtype) for a in own]
        + [pltpu.SemaphoreType.DMA((len(args),))],
        cost_estimate=pl.CostEstimate(flops=2_000_000, transcendentals=0, bytes_accessed=moved),
    )(*[far(a) for a in args])


def query_body(
    index_ref, cache_hbm, arr_ref, q_gain_ref, kv_gain_ref, q_up_ref, head_gain_ref, key_up_ref,
    cos_ref, sin_ref, send_ref, latent_ref, mine_ref, cache_ref, sem,
):
    copy = pltpu.make_async_copy(cache_hbm, cache_ref, sem.at[0])
    copy.start()
    peers, both, cols = arr_ref.shape
    rows = both // 2
    rank = key_up_ref.shape[0]
    half = cos_ref.shape[1]
    q_raw = jnp.concatenate([arr_ref[i, :rows, :] for i in range(peers)], axis=1)
    kv_raw = jnp.concatenate([arr_ref[i, rows:, :] for i in range(peers)], axis=1)
    latent = rms_scaled(kv_raw, kv_gain_ref[...]).astype(BF16)
    latent_ref[...] = latent
    mine = latent[:, :cols]
    for i in range(1, peers):
        mine = jnp.where(index_ref[0] == i, latent[:, i * cols : (i + 1) * cols], mine)
    mine_ref[...] = mine
    q_lat = rms_scaled(q_raw, q_gain_ref[...]).astype(BF16)
    query = dot_t(q_lat, q_up_ref[...])
    each = rows // peers
    for h in range(head_gain_ref.shape[0]):
        one = rms_scaled(query[:, h * QK : (h + 1) * QK], head_gain_ref[h : h + 1, :])
        lower = one[:, NOPE : NOPE + half]
        upper = one[:, NOPE + half :]
        turned = jnp.concatenate(
            [
                lower * cos_ref[...] - upper * sin_ref[...],
                upper * cos_ref[...] + lower * sin_ref[...],
            ],
            axis=1,
        )
        absorbed = dot_t(one[:, :NOPE].astype(BF16), key_up_ref[:, h * NOPE : (h + 1) * NOPE])
        for i in range(peers):
            at = slice(h * each, (h + 1) * each)
            send_ref[i, at, :rank] = absorbed[i * each : (i + 1) * each].astype(BF16)
            send_ref[i, at, rank:] = turned[i * each : (i + 1) * each].astype(BF16)
    copy.wait()


def attend_body(
    index_ref, arr_ref, cache_ref, keys_ref, cos_table_ref, sin_table_ref, latent_ref, mine_ref,
    rope_ref, cos_ref, sin_ref, len_ref, out_ref, latent_out, rope_out, sems,
):
    copies = [
        pltpu.make_async_copy(mine_ref, latent_out, sems.at[0]),
        pltpu.make_async_copy(rope_ref, rope_out, sems.at[1]),
    ]
    for copy in copies:
        copy.start()
    seqs, places, rank = cache_ref.shape
    peers, each, _ = arr_ref.shape
    rows = peers * each
    half = cos_ref.shape[1]
    arrived = arr_ref[...].reshape(rows, arr_ref.shape[2])
    absorbed = arrived[:, :rank]
    turned = arrived[:, rank:]
    scale = QK ** (-0.5)
    row_seq = lax.broadcasted_iota(jnp.int32, (rows, 1), 0) % seqs
    every = latent_ref.shape[0]
    chosen = lax.broadcasted_iota(jnp.int32, (rows, every), 1) == row_seq + index_ref[0] * seqs
    lengths = jnp.sum(jnp.where(chosen, len_ref[...], 0), axis=1, keepdims=True)
    chosen = chosen.astype(BF16)
    latent = dot(chosen, latent_ref[...])
    lower = rope_ref[:, :half].astype(F32)
    upper = rope_ref[:, half:].astype(F32)
    key_new = jnp.concatenate(
        [
            lower * cos_ref[...] - upper * sin_ref[...],
            upper * cos_ref[...] + lower * sin_ref[...],
        ],
        axis=1,
    )
    key_new = dot(chosen, key_new.astype(BF16))
    self_score = (
        jnp.sum(absorbed.astype(F32) * latent, axis=1, keepdims=True)
        + jnp.sum(turned.astype(F32) * key_new, axis=1, keepdims=True)
    ) * scale
    scores = jnp.zeros((rows, places), F32)
    for s in range(seqs):
        below = keys_ref[s, :half, :].astype(F32)
        above = keys_ref[s, half:, :].astype(F32)
        keys = jnp.concatenate(
            [
                below * cos_table_ref[...] - above * sin_table_ref[...],
                above * cos_table_ref[...] + below * sin_table_ref[...],
            ],
            axis=0,
        ).astype(BF16)
        part = dot_t(absorbed, cache_ref[s]) + dot(turned, keys)
        scores = jnp.where(row_seq == s, part, scores)
    valid = lax.broadcasted_iota(jnp.int32, (rows, places), 1) < lengths
    scores = jnp.where(valid, scores * scale, NEG)
    top = jnp.maximum(jnp.max(scores, axis=1, keepdims=True), self_score)
    weights = jnp.where(valid, jnp.exp(scores - top), 0.0)
    self_weight = jnp.exp(self_score - top)
    total = jnp.sum(weights, axis=1, keepdims=True) + self_weight
    summed = self_weight.astype(BF16).astype(F32) * latent
    for s in range(seqs):
        summed = summed + dot(jnp.where(row_seq == s, weights, 0.0).astype(BF16), cache_ref[s])
    out_ref[...] = (summed / total).astype(BF16).reshape(out_ref.shape)
    for copy in copies:
        copy.wait()


def heads_body(arr_ref, value_ref, out_w_ref, out_ref):
    peers, each, rank = arr_ref.shape
    rows = peers * each
    heads = value_ref.shape[1] // VDIM
    seqs = each // heads
    values = dot(arr_ref[...].reshape(rows, rank), value_ref[...]).astype(BF16)
    to = lax.broadcasted_iota(jnp.int32, (rows // heads, rows), 0)
    at = lax.broadcasted_iota(jnp.int32, (rows // heads, rows), 1)
    column = lax.broadcasted_iota(jnp.int32, (rows // heads, heads * VDIM), 1)
    picked = jnp.zeros((rows // heads, heads * VDIM), F32)
    for h in range(heads):
        chosen = (at == (to // seqs) * each + h * seqs + to % seqs).astype(BF16)
        picked = jnp.where(column // VDIM == h, dot(chosen, values), picked)
    partial = dot(picked.astype(BF16), out_w_ref[...]).astype(BF16)
    for i in range(out_ref.shape[0]):
        out_ref[i] = partial


def expert_body(rows_ref, mine_ref, gate_ref, up_ref, down_ref, out_ref):
    width = down_ref.shape[1]
    inside = rows_ref[:, :width]
    gate_pre = dot(inside, gate_ref[...])
    up_pre = dot(inside, up_ref[...])
    hidden = (gate_pre / (1.0 + jnp.exp(-gate_pre)) * up_pre).astype(BF16)
    scale = jnp.sum(rows_ref[:, width:].astype(F32) * mine_ref[...], axis=1, keepdims=True)
    out_ref[...] = (dot(hidden, down_ref[...]) * scale).astype(out_ref.dtype)


def shards(
    tokens,
    attn_gain,
    q_down,
    kv_down,
    rope_down,
    q_latent_gain,
    kv_latent_gain,
    q_up,
    query_gain,
    key_up,
    value_up,
    attn_out,
    cache_latent,
    cache_rope,
    lengths,
    moe_gain,
    route,
    route_weight,
    expert_gate,
    expert_up,
    expert_down,
):
    tp_count = lax.axis_size("tp")
    tp_index = lax.axis_index("tp")
    seq_count, width = tokens.shape
    kv_cols = kv_down.shape[1]
    rank = cache_latent.shape[2]
    heads_here = query_gain.shape[0]
    seqs_mine = cache_latent.shape[0]
    index = tp_index.astype(jnp.int32)[None]
    half_dim = rope_down.shape[1] // 2
    each = heads_here * seqs_mine
    chips = lax.axis_size(CHIPS)
    cores = lax.axis_size(CORE)
    chips_in_group = EPG // cores
    slots = chips // chips_in_group * GROUP_CAP
    turns = ROPE_BASE ** (-np.arange(half_dim, dtype=np.float32) / np.float32(half_dim))
    turns = turns.astype(np.float32)
    angles = turns[:, None] * np.arange(cache_latent.shape[1], dtype=np.float32)
    cos_table = jnp.asarray(np.cos(angles.astype(np.float64)).astype(np.float32))
    sin_table = jnp.asarray(np.sin(angles.astype(np.float64)).astype(np.float32))
    (
        both, new_rope, cosines, sines, placing, packed_weights,
        q_up_t, key_near, q_gain, kv_gain, head_gain, cos_table, sin_table, keys, lens,
    ) = down(
        (
            jax.ShapeDtypeStruct((tp_count, 2 * seq_count, kv_cols), BF16),
            jax.ShapeDtypeStruct((seq_count, rope_down.shape[1]), BF16),
            jax.ShapeDtypeStruct((seq_count, half_dim), F32),
            jax.ShapeDtypeStruct((seq_count, half_dim), F32),
            jax.ShapeDtypeStruct((slots, seq_count), BF16),
            jax.ShapeDtypeStruct((slots, EXTRA), BF16),
        ),
        (
            tokens,
            attn_gain[None],
            q_down,
            kv_down,
            rope_down.T,
            lengths[None],
            jnp.asarray(turns[None]),
            route.T,
            route_weight.T,
        ),
        (
            q_up.T,
            key_up,
            q_latent_gain[None],
            kv_latent_gain[None],
            query_gain,
            cos_table,
            sin_table,
            cache_rope,
            lengths[None],
        ),
    )
    both, index = lax.optimization_barrier((both, index))
    latents = lax.all_to_all(both, "tp", 0, 0, tiled=True)
    send, latent_new, mine_new, cache = run(
        query_body,
        (
            jax.ShapeDtypeStruct((tp_count, each, rank + 2 * half_dim), BF16),
            jax.ShapeDtypeStruct((seq_count, rank), BF16),
            jax.ShapeDtypeStruct((seq_count, kv_cols), BF16),
            jax.ShapeDtypeStruct(cache_latent.shape, BF16),
        ),
        index,
        cache_latent,
        latents,
        q_gain,
        kv_gain,
        q_up_t,
        head_gain,
        key_near,
        cosines,
        sines,
        scalars=1,
        hbm_in=1,
        sems=1,
    )
    queries = lax.all_to_all(send, "tp", 0, 0, tiled=True)
    attended, new_latent, new_rope = run(
        attend_body,
        (
            jax.ShapeDtypeStruct((tp_count, each, rank), BF16),
            jax.ShapeDtypeStruct((seq_count, kv_cols), BF16),
            jax.ShapeDtypeStruct(new_rope.shape, BF16),
        ),
        index,
        queries,
        cache,
        keys,
        cos_table,
        sin_table,
        latent_new,
        mine_new,
        new_rope,
        cosines,
        sines,
        lens,
        scalars=1,
        hbm_out=2,
        sems=2,
    )
    attended_heads = lax.all_to_all(attended, "tp", 0, 0, tiled=True)
    (partials,) = run(
        heads_body,
        (jax.ShapeDtypeStruct((tp_count, seq_count, width), BF16),),
        attended_heads,
        value_up,
        attn_out,
    )
    head_sum = lax.all_to_all(partials, "tp", 0, 0, tiled=True).astype(F32).sum(axis=0)
    attn_resid = (tokens.astype(jnp.float32) + head_sum).astype(jnp.bfloat16)
    moe_input = rms_scaled(attn_resid, moe_gain).astype(jnp.bfloat16)
    packed = jnp.dot(placing, moe_input, preferred_element_type=F32).astype(BF16)
    packed = jnp.concatenate([packed, packed_weights], axis=1)
    packed = jnp.broadcast_to(
        packed.reshape(-1, 1, GROUP_CAP, width + EXTRA),
        (slots // GROUP_CAP, chips_in_group, GROUP_CAP, width + EXTRA),
    ).reshape(chips, GROUP_CAP, width + EXTRA)
    arrived = lax.all_to_all(packed, CHIPS, 0, 0, tiled=True).reshape(-1, width + EXTRA)
    swap = [(i, cores - 1 - i) for i in range(cores)]
    other = lax.ppermute(arrived, CORE, swap)
    lane = jnp.arange(EXTRA, dtype=jnp.int32)
    mine = (lane == lax.axis_index(EP) % EPG).astype(F32)[None]

    def expert(block, kind):
        return run(
            expert_body,
            (jax.ShapeDtypeStruct((block.shape[0], width), kind),),
            block,
            mine,
            expert_gate[0],
            expert_up[0],
            expert_down[0],
            flops=100_000_000,
        )[0]

    own = expert(arrived, F32)
    sent_back = lax.ppermute(expert(other, BF16), CORE, swap)
    quarter_cols = width // tp_count
    sums = (own + sent_back.astype(F32)).astype(BF16)
    sums, first_col = lax.optimization_barrier((sums, tp_index * quarter_cols))
    sums = sums.reshape(chips, GROUP_CAP, tp_count, quarter_cols).swapaxes(1, 2)
    returned = lax.all_to_all(
        sums.reshape(chips * tp_count, GROUP_CAP, quarter_cols), (*CHIPS, "tp"), 0, 0, tiled=True
    ).reshape(-1, chips_in_group * tp_count, GROUP_CAP, quarter_cols)
    totals = jnp.sum(returned.astype(F32), axis=1).reshape(slots, quarter_cols)
    high = totals.astype(BF16)
    picked = jnp.dot(placing.T, high, preferred_element_type=F32)
    residual = lax.dynamic_slice_in_dim(
        attn_resid, first_col, quarter_cols, 1, allow_negative_indices=False
    )
    mixed_out = (residual.astype(F32) + picked).astype(BF16)
    return (mixed_out, new_latent, new_rope)


def solution(mesh):
    torus = Mesh(mesh.devices.reshape(8, 8, 2, mesh.shape["tp"]), ("ep_0", "ep_1", "ep_2", "tp"))
    placed = (
        P(EP, None),
        P(),
        P(None, "tp"),
        P(None, "tp"),
        P(),
        P(),
        P(),
        P(None, "tp"),
        P("tp", None),
        P(None, "tp"),
        P(None, "tp"),
        P("tp", None),
        P(EP_TP, None, None),
        P(EP_TP, None, None),
        P(EP),
        P(),
        P(EP, None),
        P(EP, None),
        P(EP, None, "tp"),
        P(EP, None, "tp"),
        P(EP, "tp", None),
    )
    return jax.shard_map(
        shards,
        mesh=torus,
        in_specs=placed,
        out_specs=(P(EP, "tp"), P(EP, "tp"), P(EP, None)),
        check_vma=False,
    )
```

```python
import jax
import jax.numpy as jnp
import numpy as np
from jax import lax
from jax.experimental import pallas as pl
from jax.experimental.pallas import tpu as pltpu
from jax.sharding import Mesh
from jax.sharding import PartitionSpec as P

NOPE = 64
VDIM = 64
QK = 96
EPG = 8
EP = ("ep_0", "ep_1", "ep_2")
CHIPS = ("ep_0", "ep_1")
CORE = "ep_2"
GROUP_CAP = 2
EXTRA = 128
EP_TP = ("ep_0", "ep_1", "ep_2", "tp")


EPS = 1e-06
ROPE_BASE = 10000.0
F32 = jnp.float32
BF16 = jnp.bfloat16
NEG = -1e30


def rms_scaled(values_in, gain_vec):
    values_in = values_in.astype(jnp.float32)
    return (
        values_in
        * lax.rsqrt(jnp.mean(values_in * values_in, axis=-1, keepdims=True) + EPS)
        * gain_vec
    )


def dot(a, b):
    return jnp.dot(a, b, preferred_element_type=F32)


def dot_t(a, b):
    return lax.dot_general(a, b, (((1,), (1,)), ((), ())), preferred_element_type=F32)


def near(array):
    return pltpu.with_memory_space_constraint(array, pltpu.VMEM)


def far(array):
    return pltpu.with_memory_space_constraint(array, pltpu.HBM)


def run(body, outs, *args, flops=2_000_000, scalars=0, hbm_in=0, hbm_out=0, sems=0):
    moved = sum(a.size * a.dtype.itemsize for a in args)
    spaces = [pltpu.SMEM] * scalars + [pltpu.HBM] * hbm_in
    spaces += [pltpu.VMEM] * (len(args) - len(spaces))
    kinds = [pltpu.VMEM] * (len(outs) - hbm_out) + [pltpu.HBM] * hbm_out
    place_in = {pltpu.SMEM: lambda a: a, pltpu.HBM: far, pltpu.VMEM: near}
    return pl.pallas_call(
        body,
        compiler_params=pltpu.CompilerParams(vmem_limit_bytes=16 * 1024 * 1024),
        in_specs=[pl.BlockSpec(memory_space=kind) for kind in spaces],
        out_specs=[pl.BlockSpec(memory_space=kind) for kind in kinds],
        out_shape=[kind(o.shape, o.dtype) for kind, o in zip(kinds, outs)],
        scratch_shapes=[pltpu.SemaphoreType.DMA((sems,))] if sems else [],
        cost_estimate=pl.CostEstimate(flops=flops, transcendentals=0, bytes_accessed=moved),
    )(*[place_in[kind](a) for kind, a in zip(spaces, args)])


def place(route_ref, weight_ref, placing_ref, weights_ref):
    topk, rows = route_ref.shape
    slots = placing_ref.shape[0]
    group = route_ref[0:1, :] // EPG
    first = lax.broadcasted_iota(jnp.int32, (rows, rows), 0)
    second = lax.broadcasted_iota(jnp.int32, (rows, rows), 1)
    column = jnp.sum(jnp.where(first == second, group, 0), axis=1, keepdims=True)
    earlier = jnp.where((column == group) & (first < second), 1, 0)
    slot = group * GROUP_CAP + jnp.sum(earlier, axis=0, keepdims=True)
    placing = (lax.broadcasted_iota(jnp.int32, (slots, rows), 0) == slot).astype(BF16)
    placing_ref[...] = placing
    lane = lax.broadcasted_iota(jnp.int32, (EXTRA, rows), 0)
    table = jnp.zeros((EXTRA, rows), F32)
    for k in range(topk):
        table = table + jnp.where(route_ref[k : k + 1, :] % EPG == lane, weight_ref[k : k + 1, :], 0.0)
    weights_ref[...] = dot_t(placing, table.astype(BF16)).astype(BF16)


OWN = 9
MADE = 6


def down_body(*refs):
    count = (len(refs) - MADE - 1) // 2
    hbm, made, last = refs[:count], refs[count : count + MADE], refs[count + MADE : -1]
    sems = refs[-1]
    near_refs = last[count - OWN :] + last[: count - OWN]
    copies = [pltpu.make_async_copy(hbm[i], near_refs[i], sems.at[i]) for i in range(count)]
    for copy in copies:
        copy.start()
    tok_ref, gain_ref, q_ref, kv_ref, rope_ref, len_ref, turn_ref, route_ref, weight_ref = near_refs[
        :OWN
    ]
    both_ref, new_rope_ref, cos_ref, sin_ref, placing_ref, weights_ref = made
    copies[0].wait()
    copies[1].wait()
    normed = rms_scaled(tok_ref[...], gain_ref[...]).astype(BF16)
    rows = normed.shape[0]
    copies[2].wait()
    q_part = dot(normed, q_ref[...]).astype(BF16)
    copies[3].wait()
    kv_part = dot(normed, kv_ref[...]).astype(BF16)
    for i in range(both_ref.shape[0]):
        both_ref[i, :rows, :] = q_part
        both_ref[i, rows:, :] = kv_part
    for i in range(4, OWN):
        copies[i].wait()
    new_rope_ref[...] = dot_t(normed, rope_ref[...]).astype(BF16)
    first = lax.broadcasted_iota(jnp.int32, (rows, rows), 0)
    second = lax.broadcasted_iota(jnp.int32, (rows, rows), 1)
    lengths = jnp.sum(jnp.where(first == second, len_ref[...], 0), axis=1, keepdims=True)
    angles = lengths.astype(F32) * turn_ref[...]
    cos_ref[...] = jnp.cos(angles)
    sin_ref[...] = jnp.sin(angles)
    place(route_ref, weight_ref, placing_ref, weights_ref)
    for copy in copies[OWN:]:
        copy.wait()


def down(made, own, others):
    args = (*own, *others)
    moved = sum(a.size * a.dtype.itemsize for a in args)
    outs = [pltpu.VMEM(o.shape, o.dtype) for o in (*made, *others)]
    return pl.pallas_call(
        down_body,
        compiler_params=pltpu.CompilerParams(vmem_limit_bytes=16 * 1024 * 1024),
        in_specs=[pl.BlockSpec(memory_space=pltpu.HBM)] * len(args),
        out_specs=[pl.BlockSpec(memory_space=pltpu.VMEM)] * len(outs),
        out_shape=outs,
        scratch_shapes=[pltpu.VMEM(a.shape, a.dtype) for a in own]
        + [pltpu.SemaphoreType.DMA((len(args),))],
        cost_estimate=pl.CostEstimate(flops=2_000_000, transcendentals=0, bytes_accessed=moved),
    )(*[far(a) for a in args])


def query_body(
    index_ref, cache_hbm, arr_ref, q_gain_ref, kv_gain_ref, q_up_ref, head_gain_ref, key_up_ref,
    cos_ref, sin_ref, send_ref, latent_ref, mine_ref, cache_ref, sem,
):
    copy = pltpu.make_async_copy(cache_hbm, cache_ref, sem.at[0])
    copy.start()
    peers, both, cols = arr_ref.shape
    rows = both // 2
    rank = key_up_ref.shape[0]
    half = cos_ref.shape[1]
    q_raw = jnp.concatenate([arr_ref[i, :rows, :] for i in range(peers)], axis=1)
    kv_raw = jnp.concatenate([arr_ref[i, rows:, :] for i in range(peers)], axis=1)
    latent = rms_scaled(kv_raw, kv_gain_ref[...]).astype(BF16)
    latent_ref[...] = latent
    mine = latent[:, :cols]
    for i in range(1, peers):
        mine = jnp.where(index_ref[0] == i, latent[:, i * cols : (i + 1) * cols], mine)
    mine_ref[...] = mine
    q_lat = rms_scaled(q_raw, q_gain_ref[...]).astype(BF16)
    query = dot_t(q_lat, q_up_ref[...])
    each = rows // peers
    for h in range(head_gain_ref.shape[0]):
        one = rms_scaled(query[:, h * QK : (h + 1) * QK], head_gain_ref[h : h + 1, :])
        lower = one[:, NOPE : NOPE + half]
        upper = one[:, NOPE + half :]
        turned = jnp.concatenate(
            [
                lower * cos_ref[...] - upper * sin_ref[...],
                upper * cos_ref[...] + lower * sin_ref[...],
            ],
            axis=1,
        )
        absorbed = dot_t(one[:, :NOPE].astype(BF16), key_up_ref[:, h * NOPE : (h + 1) * NOPE])
        for i in range(peers):
            at = slice(h * each, (h + 1) * each)
            send_ref[i, at, :rank] = absorbed[i * each : (i + 1) * each].astype(BF16)
            send_ref[i, at, rank:] = turned[i * each : (i + 1) * each].astype(BF16)
    copy.wait()


def attend_body(
    index_ref, gate_hbm, up_hbm, down_hbm, arr_ref, cache_ref, keys_ref, cos_table_ref, sin_table_ref, latent_ref, mine_ref,
    rope_ref, cos_ref, sin_ref, len_ref, out_ref, packed_ref, latent_out, rope_out, sems,
):
    width, units = gate_hbm.shape
    copies = [
        pltpu.make_async_copy(mine_ref, latent_out, sems.at[0]),
        pltpu.make_async_copy(rope_ref, rope_out, sems.at[1]),
        pltpu.make_async_copy(gate_hbm, packed_ref.at[:width], sems.at[2]),
        pltpu.make_async_copy(up_hbm, packed_ref.at[width : 2 * width], sems.at[3]),
    ]
    for j in range(width // units):
        at = 2 * width + j * units
        copies.append(
            pltpu.make_async_copy(
                down_hbm.at[:, j * units : (j + 1) * units],
                packed_ref.at[at : at + units],
                sems.at[4 + j],
            )
        )
    for copy in copies:
        copy.start()
    seqs, places, rank = cache_ref.shape
    peers, each, _ = arr_ref.shape
    rows = peers * each
    half = cos_ref.shape[1]
    arrived = arr_ref[...].reshape(rows, arr_ref.shape[2])
    absorbed = arrived[:, :rank]
    turned = arrived[:, rank:]
    scale = QK ** (-0.5)
    row_seq = lax.broadcasted_iota(jnp.int32, (rows, 1), 0) % seqs
    every = latent_ref.shape[0]
    chosen = lax.broadcasted_iota(jnp.int32, (rows, every), 1) == row_seq + index_ref[0] * seqs
    lengths = jnp.sum(jnp.where(chosen, len_ref[...], 0), axis=1, keepdims=True)
    chosen = chosen.astype(BF16)
    latent = dot(chosen, latent_ref[...])
    lower = rope_ref[:, :half].astype(F32)
    upper = rope_ref[:, half:].astype(F32)
    key_new = jnp.concatenate(
        [
            lower * cos_ref[...] - upper * sin_ref[...],
            upper * cos_ref[...] + lower * sin_ref[...],
        ],
        axis=1,
    )
    key_new = dot(chosen, key_new.astype(BF16))
    self_score = (
        jnp.sum(absorbed.astype(F32) * latent, axis=1, keepdims=True)
        + jnp.sum(turned.astype(F32) * key_new, axis=1, keepdims=True)
    ) * scale
    scores = jnp.zeros((rows, places), F32)
    for s in range(seqs):
        below = keys_ref[s, :half, :].astype(F32)
        above = keys_ref[s, half:, :].astype(F32)
        keys = jnp.concatenate(
            [
                below * cos_table_ref[...] - above * sin_table_ref[...],
                above * cos_table_ref[...] + below * sin_table_ref[...],
            ],
            axis=0,
        ).astype(BF16)
        part = dot_t(absorbed, cache_ref[s]) + dot(turned, keys)
        scores = jnp.where(row_seq == s, part, scores)
    valid = lax.broadcasted_iota(jnp.int32, (rows, places), 1) < lengths
    scores = jnp.where(valid, scores * scale, NEG)
    top = jnp.maximum(jnp.max(scores, axis=1, keepdims=True), self_score)
    weights = jnp.where(valid, jnp.exp(scores - top), 0.0)
    self_weight = jnp.exp(self_score - top)
    total = jnp.sum(weights, axis=1, keepdims=True) + self_weight
    summed = self_weight.astype(BF16).astype(F32) * latent
    for s in range(seqs):
        summed = summed + dot(jnp.where(row_seq == s, weights, 0.0).astype(BF16), cache_ref[s])
    out_ref[...] = (summed / total).astype(BF16).reshape(out_ref.shape)
    for copy in copies:
        copy.wait()


def heads_body(arr_ref, value_ref, out_w_ref, out_ref):
    peers, each, rank = arr_ref.shape
    rows = peers * each
    heads = value_ref.shape[1] // VDIM
    seqs = each // heads
    values = dot(arr_ref[...].reshape(rows, rank), value_ref[...]).astype(BF16)
    to = lax.broadcasted_iota(jnp.int32, (rows // heads, rows), 0)
    at = lax.broadcasted_iota(jnp.int32, (rows // heads, rows), 1)
    column = lax.broadcasted_iota(jnp.int32, (rows // heads, heads * VDIM), 1)
    picked = jnp.zeros((rows // heads, heads * VDIM), F32)
    for h in range(heads):
        chosen = (at == (to // seqs) * each + h * seqs + to % seqs).astype(BF16)
        picked = jnp.where(column // VDIM == h, dot(chosen, values), picked)
    partial = dot(picked.astype(BF16), out_w_ref[...]).astype(BF16)
    for i in range(out_ref.shape[0]):
        out_ref[i] = partial


def experts_body(index_ref, rows_ref, own_ref, other_ref, out_ref):
    width = out_ref.shape[1]
    units = own_ref.shape[1]
    inside = rows_ref[:, :width]
    extra = rows_ref[:, width:].astype(F32)
    lane = lax.broadcasted_iota(jnp.int32, extra.shape, 1)
    here = index_ref[0]
    there = here + 1 - 2 * (here % 2)
    hidden, scales = [], []
    for weights_ref, place_in in ((own_ref, here), (other_ref, there)):
        gate_pre = dot(inside, weights_ref[:width, :])
        up_pre = dot(inside, weights_ref[width : 2 * width, :])
        hidden.append((gate_pre / (1.0 + jnp.exp(-gate_pre)) * up_pre).astype(BF16))
        scales.append(jnp.sum(jnp.where(lane == place_in, extra, 0.0), axis=1, keepdims=True))
    for j in range(width // units):
        at = 2 * width + j * units
        summed = dot(hidden[0], own_ref[at : at + units, :]) * scales[0]
        summed = summed + dot(hidden[1], other_ref[at : at + units, :]) * scales[1]
        out_ref[:, j * units : (j + 1) * units] = summed.astype(BF16)


def shards(
    tokens,
    attn_gain,
    q_down,
    kv_down,
    rope_down,
    q_latent_gain,
    kv_latent_gain,
    q_up,
    query_gain,
    key_up,
    value_up,
    attn_out,
    cache_latent,
    cache_rope,
    lengths,
    moe_gain,
    route,
    route_weight,
    expert_gate,
    expert_up,
    expert_down,
):
    tp_count = lax.axis_size("tp")
    tp_index = lax.axis_index("tp")
    seq_count, width = tokens.shape
    kv_cols = kv_down.shape[1]
    rank = cache_latent.shape[2]
    heads_here = query_gain.shape[0]
    seqs_mine = cache_latent.shape[0]
    index = tp_index.astype(jnp.int32)[None]
    half_dim = rope_down.shape[1] // 2
    each = heads_here * seqs_mine
    chips = lax.axis_size(CHIPS)
    cores = lax.axis_size(CORE)
    chips_in_group = EPG // cores
    slots = chips // chips_in_group * GROUP_CAP
    turns = ROPE_BASE ** (-np.arange(half_dim, dtype=np.float32) / np.float32(half_dim))
    turns = turns.astype(np.float32)
    angles = turns[:, None] * np.arange(cache_latent.shape[1], dtype=np.float32)
    cos_table = jnp.asarray(np.cos(angles.astype(np.float64)).astype(np.float32))
    sin_table = jnp.asarray(np.sin(angles.astype(np.float64)).astype(np.float32))
    (
        both, new_rope, cosines, sines, placing, packed_weights,
        q_up_t, key_near, q_gain, kv_gain, head_gain, cos_table, sin_table, keys, lens,
    ) = down(
        (
            jax.ShapeDtypeStruct((tp_count, 2 * seq_count, kv_cols), BF16),
            jax.ShapeDtypeStruct((seq_count, rope_down.shape[1]), BF16),
            jax.ShapeDtypeStruct((seq_count, half_dim), F32),
            jax.ShapeDtypeStruct((seq_count, half_dim), F32),
            jax.ShapeDtypeStruct((slots, seq_count), BF16),
            jax.ShapeDtypeStruct((slots, EXTRA), BF16),
        ),
        (
            tokens,
            attn_gain[None],
            q_down,
            kv_down,
            rope_down.T,
            lengths[None],
            jnp.asarray(turns[None]),
            route.T,
            route_weight.T,
        ),
        (
            q_up.T,
            key_up,
            q_latent_gain[None],
            kv_latent_gain[None],
            query_gain,
            cos_table,
            sin_table,
            cache_rope,
            lengths[None],
        ),
    )
    expert_here = (lax.axis_index(EP) % EPG).astype(jnp.int32)[None]
    quarter_cols = width // tp_count
    first_col = (tp_index * quarter_cols).astype(jnp.int32)
    both, index, expert_here, first_col = lax.optimization_barrier(
        (both, index, expert_here, first_col)
    )
    latents = lax.all_to_all(both, "tp", 0, 0, tiled=True)
    send, latent_new, mine_new, cache = run(
        query_body,
        (
            jax.ShapeDtypeStruct((tp_count, each, rank + 2 * half_dim), BF16),
            jax.ShapeDtypeStruct((seq_count, rank), BF16),
            jax.ShapeDtypeStruct((seq_count, kv_cols), BF16),
            jax.ShapeDtypeStruct(cache_latent.shape, BF16),
        ),
        index,
        cache_latent,
        latents,
        q_gain,
        kv_gain,
        q_up_t,
        head_gain,
        key_near,
        cosines,
        sines,
        scalars=1,
        hbm_in=1,
        sems=1,
    )
    queries = lax.all_to_all(send, "tp", 0, 0, tiled=True)
    units = expert_gate.shape[2]
    attended, own_weights, new_latent, new_rope = run(
        attend_body,
        (
            jax.ShapeDtypeStruct((tp_count, each, rank), BF16),
            jax.ShapeDtypeStruct((3 * width, units), BF16),
            jax.ShapeDtypeStruct((seq_count, kv_cols), BF16),
            jax.ShapeDtypeStruct(new_rope.shape, BF16),
        ),
        index,
        expert_gate[0],
        expert_up[0],
        expert_down[0],
        queries,
        cache,
        keys,
        cos_table,
        sin_table,
        latent_new,
        mine_new,
        new_rope,
        cosines,
        sines,
        lens,
        scalars=1,
        hbm_in=3,
        hbm_out=2,
        sems=4 + width // units,
    )
    swap = [(i, cores - 1 - i) for i in range(cores)]
    other_weights = lax.ppermute(own_weights, CORE, swap)
    attended_heads = lax.all_to_all(attended, "tp", 0, 0, tiled=True)
    (partials,) = run(
        heads_body,
        (jax.ShapeDtypeStruct((tp_count, seq_count, width), BF16),),
        attended_heads,
        value_up,
        attn_out,
    )
    head_sum = lax.all_to_all(partials, "tp", 0, 0, tiled=True).astype(F32).sum(axis=0)
    attn_resid = (tokens.astype(jnp.float32) + head_sum).astype(jnp.bfloat16)
    moe_input = rms_scaled(attn_resid, moe_gain).astype(jnp.bfloat16)
    packed = jnp.dot(placing, moe_input, preferred_element_type=F32).astype(BF16)
    packed = jnp.concatenate([packed, packed_weights], axis=1)
    packed = jnp.broadcast_to(
        packed.reshape(-1, 1, GROUP_CAP, width + EXTRA),
        (slots // GROUP_CAP, chips_in_group, GROUP_CAP, width + EXTRA),
    ).reshape(chips, GROUP_CAP, width + EXTRA)
    arrived = lax.all_to_all(packed, CHIPS, 0, 0, tiled=True).reshape(-1, width + EXTRA)
    (sums,) = run(
        experts_body,
        (jax.ShapeDtypeStruct((arrived.shape[0], width), BF16),),
        expert_here,
        arrived,
        own_weights,
        other_weights,
        flops=100_000_000,
        scalars=1,
    )
    sums = sums.reshape(chips, GROUP_CAP, tp_count, quarter_cols).swapaxes(1, 2)
    returned = lax.all_to_all(
        sums.reshape(chips * tp_count, GROUP_CAP, quarter_cols), (*CHIPS, "tp"), 0, 0, tiled=True
    ).reshape(-1, chips_in_group * tp_count, GROUP_CAP, quarter_cols)
    totals = jnp.sum(returned.astype(F32), axis=1).reshape(slots, quarter_cols)
    high = totals.astype(BF16)
    picked = jnp.dot(placing.T, high, preferred_element_type=F32)
    residual = lax.dynamic_slice_in_dim(
        attn_resid, first_col, quarter_cols, 1, allow_negative_indices=False
    )
    mixed_out = (residual.astype(F32) + picked).astype(BF16)
    return (mixed_out, new_latent, new_rope)


def solution(mesh):
    torus = Mesh(mesh.devices.reshape(8, 8, 2, mesh.shape["tp"]), ("ep_0", "ep_1", "ep_2", "tp"))
    placed = (
        P(EP, None),
        P(),
        P(None, "tp"),
        P(None, "tp"),
        P(),
        P(),
        P(),
        P(None, "tp"),
        P("tp", None),
        P(None, "tp"),
        P(None, "tp"),
        P("tp", None),
        P(EP_TP, None, None),
        P(EP_TP, None, None),
        P(EP),
        P(),
        P(EP, None),
        P(EP, None),
        P(EP, None, "tp"),
        P(EP, None, "tp"),
        P(EP, "tp", None),
    )
    return jax.shard_map(
        shards,
        mesh=torus,
        in_specs=placed,
        out_specs=(P(EP, "tp"), P(EP, "tp"), P(EP, None)),
        check_vma=False,
    )
```

```python
import jax
import jax.numpy as jnp
import numpy as np
from jax import lax
from jax.experimental import pallas as pl
from jax.experimental.pallas import tpu as pltpu
from jax.sharding import Mesh
from jax.sharding import PartitionSpec as P

NOPE = 64
VDIM = 64
QK = 96
EPG = 8
EP = ("ep_0", "ep_1", "ep_2")
CHIPS = ("ep_1", "ep_0")
CORE = "ep_2"
GROUP_CAP = 2
EXTRA = 128
EP_TP = ("ep_0", "ep_1", "ep_2", "tp")


EPS = 1e-06
ROPE_BASE = 10000.0
F32 = jnp.float32
BF16 = jnp.bfloat16
NEG = -1e30


def rms_scaled(values_in, gain_vec):
    values_in = values_in.astype(jnp.float32)
    return (
        values_in
        * lax.rsqrt(jnp.mean(values_in * values_in, axis=-1, keepdims=True) + EPS)
        * gain_vec
    )


def dot(a, b):
    return jnp.dot(a, b, preferred_element_type=F32)


def dot_t(a, b):
    return lax.dot_general(a, b, (((1,), (1,)), ((), ())), preferred_element_type=F32)


def near(array):
    return pltpu.with_memory_space_constraint(array, pltpu.VMEM)


def far(array):
    return pltpu.with_memory_space_constraint(array, pltpu.HBM)


def run(body, outs, *args, flops=2_000_000, scalars=0, hbm_in=0, hbm_out=0, sems=0, scratch=()):
    moved = sum(a.size * a.dtype.itemsize for a in args)
    spaces = [pltpu.SMEM] * scalars + [pltpu.HBM] * hbm_in
    spaces += [pltpu.VMEM] * (len(args) - len(spaces))
    kinds = [pltpu.VMEM] * (len(outs) - hbm_out) + [pltpu.HBM] * hbm_out
    place_in = {pltpu.SMEM: lambda a: a, pltpu.HBM: far, pltpu.VMEM: near}
    return pl.pallas_call(
        body,
        compiler_params=pltpu.CompilerParams(vmem_limit_bytes=16 * 1024 * 1024),
        in_specs=[pl.BlockSpec(memory_space=kind) for kind in spaces],
        out_specs=[pl.BlockSpec(memory_space=kind) for kind in kinds],
        out_shape=[kind(o.shape, o.dtype) for kind, o in zip(kinds, outs)],
        scratch_shapes=[*scratch] + ([pltpu.SemaphoreType.DMA((sems,))] if sems else []),
        cost_estimate=pl.CostEstimate(flops=flops, transcendentals=0, bytes_accessed=moved),
    )(*[place_in[kind](a) for kind, a in zip(spaces, args)])


def place(route_ref, weight_ref, placing_ref, turned_ref, weights_ref, parts):
    topk, rows = route_ref.shape
    slots = placing_ref.shape[0]
    group = route_ref[0:1, :] // EPG
    group = group % parts * (slots // GROUP_CAP // parts) + group // parts
    first = lax.broadcasted_iota(jnp.int32, (rows, rows), 0)
    second = lax.broadcasted_iota(jnp.int32, (rows, rows), 1)
    column = jnp.sum(jnp.where(first == second, group, 0), axis=1, keepdims=True)
    earlier = jnp.where((column == group) & (first < second), 1, 0)
    slot = group * GROUP_CAP + jnp.sum(earlier, axis=0, keepdims=True)
    placing = (lax.broadcasted_iota(jnp.int32, (slots, rows), 0) == slot).astype(BF16)
    placing_ref[...] = placing
    slot_column = jnp.sum(jnp.where(first == second, slot, 0), axis=1, keepdims=True)
    turned_ref[...] = (
        lax.broadcasted_iota(jnp.int32, (rows, slots), 1) == slot_column
    ).astype(BF16)
    lane = lax.broadcasted_iota(jnp.int32, (EXTRA, rows), 0)
    table = jnp.zeros((EXTRA, rows), F32)
    for k in range(topk):
        table = table + jnp.where(route_ref[k : k + 1, :] % EPG == lane, weight_ref[k : k + 1, :], 0.0)
    weights_ref[...] = dot_t(placing, table.astype(BF16)).astype(BF16)


OWN = 9
MADE = 7


def down_body(parts, *refs):
    count = (len(refs) - MADE - 1) // 2
    hbm, made, last = refs[:count], refs[count : count + MADE], refs[count + MADE : -1]
    sems = refs[-1]
    near_refs = last[count - OWN :] + last[: count - OWN]
    copies = [pltpu.make_async_copy(hbm[i], near_refs[i], sems.at[i]) for i in range(count)]
    for copy in copies:
        copy.start()
    tok_ref, gain_ref, q_ref, kv_ref, rope_ref, len_ref, turn_ref, route_ref, weight_ref = near_refs[
        :OWN
    ]
    both_ref, new_rope_ref, cos_ref, sin_ref, placing_ref, turned_ref, weights_ref = made
    copies[0].wait()
    copies[1].wait()
    normed = rms_scaled(tok_ref[...], gain_ref[...]).astype(BF16)
    rows = normed.shape[0]
    copies[2].wait()
    q_part = dot(normed, q_ref[...]).astype(BF16)
    copies[3].wait()
    kv_part = dot(normed, kv_ref[...]).astype(BF16)
    for i in range(both_ref.shape[0]):
        both_ref[i, :rows, :] = q_part
        both_ref[i, rows:, :] = kv_part
    for i in range(4, OWN):
        copies[i].wait()
    new_rope_ref[...] = dot_t(normed, rope_ref[...]).astype(BF16)
    first = lax.broadcasted_iota(jnp.int32, (rows, rows), 0)
    second = lax.broadcasted_iota(jnp.int32, (rows, rows), 1)
    lengths = jnp.sum(jnp.where(first == second, len_ref[...], 0), axis=1, keepdims=True)
    angles = lengths.astype(F32) * turn_ref[...]
    cos_ref[...] = jnp.cos(angles)
    sin_ref[...] = jnp.sin(angles)
    place(route_ref, weight_ref, placing_ref, turned_ref, weights_ref, parts)
    for copy in copies[OWN:]:
        copy.wait()


def down(made, own, others, parts):
    args = (*own, *others)
    moved = sum(a.size * a.dtype.itemsize for a in args)
    outs = [pltpu.VMEM(o.shape, o.dtype) for o in (*made, *others)]
    return pl.pallas_call(
        lambda *refs: down_body(parts, *refs),
        compiler_params=pltpu.CompilerParams(vmem_limit_bytes=16 * 1024 * 1024),
        in_specs=[pl.BlockSpec(memory_space=pltpu.HBM)] * len(args),
        out_specs=[pl.BlockSpec(memory_space=pltpu.VMEM)] * len(outs),
        out_shape=outs,
        scratch_shapes=[pltpu.VMEM(a.shape, a.dtype) for a in own]
        + [pltpu.SemaphoreType.DMA((len(args),))],
        cost_estimate=pl.CostEstimate(flops=2_000_000, transcendentals=0, bytes_accessed=moved),
    )(*[far(a) for a in args])


def query_body(
    index_ref, cache_hbm, arr_ref, q_gain_ref, kv_gain_ref, q_up_ref, head_gain_ref, key_up_ref,
    cos_ref, sin_ref, send_ref, latent_ref, mine_ref, cache_ref, sem,
):
    copy = pltpu.make_async_copy(cache_hbm, cache_ref, sem.at[0])
    copy.start()
    peers, both, cols = arr_ref.shape
    rows = both // 2
    rank = key_up_ref.shape[0]
    half = cos_ref.shape[1]
    q_raw = jnp.concatenate([arr_ref[i, :rows, :] for i in range(peers)], axis=1)
    kv_raw = jnp.concatenate([arr_ref[i, rows:, :] for i in range(peers)], axis=1)
    latent = rms_scaled(kv_raw, kv_gain_ref[...]).astype(BF16)
    latent_ref[...] = latent
    mine = latent[:, :cols]
    for i in range(1, peers):
        mine = jnp.where(index_ref[0] == i, latent[:, i * cols : (i + 1) * cols], mine)
    mine_ref[...] = mine
    q_lat = rms_scaled(q_raw, q_gain_ref[...]).astype(BF16)
    query = dot_t(q_lat, q_up_ref[...])
    each = rows // peers
    for h in range(head_gain_ref.shape[0]):
        one = rms_scaled(query[:, h * QK : (h + 1) * QK], head_gain_ref[h : h + 1, :])
        lower = one[:, NOPE : NOPE + half]
        upper = one[:, NOPE + half :]
        turned = jnp.concatenate(
            [
                lower * cos_ref[...] - upper * sin_ref[...],
                upper * cos_ref[...] + lower * sin_ref[...],
            ],
            axis=1,
        )
        absorbed = dot_t(one[:, :NOPE].astype(BF16), key_up_ref[:, h * NOPE : (h + 1) * NOPE])
        for i in range(peers):
            at = slice(h * each, (h + 1) * each)
            send_ref[i, at, :rank] = absorbed[i * each : (i + 1) * each].astype(BF16)
            send_ref[i, at, rank:] = turned[i * each : (i + 1) * each].astype(BF16)
    copy.wait()


def attend_body(
    index_ref, arr_ref, cache_ref, keys_ref, cos_table_ref, sin_table_ref, latent_ref, mine_ref,
    rope_ref, cos_ref, sin_ref, len_ref, out_ref, latent_out, rope_out, sems,
):
    copies = [
        pltpu.make_async_copy(mine_ref, latent_out, sems.at[0]),
        pltpu.make_async_copy(rope_ref, rope_out, sems.at[1]),
    ]
    for copy in copies:
        copy.start()
    seqs, places, rank = cache_ref.shape
    peers, each, _ = arr_ref.shape
    rows = peers * each
    half = cos_ref.shape[1]
    arrived = arr_ref[...].reshape(rows, arr_ref.shape[2])
    absorbed = arrived[:, :rank]
    turned = arrived[:, rank:]
    scale = QK ** (-0.5)
    row_seq = lax.broadcasted_iota(jnp.int32, (rows, 1), 0) % seqs
    every = latent_ref.shape[0]
    chosen = lax.broadcasted_iota(jnp.int32, (rows, every), 1) == row_seq + index_ref[0] * seqs
    lengths = jnp.sum(jnp.where(chosen, len_ref[...], 0), axis=1, keepdims=True)
    chosen = chosen.astype(BF16)
    latent = dot(chosen, latent_ref[...])
    lower = rope_ref[:, :half].astype(F32)
    upper = rope_ref[:, half:].astype(F32)
    key_new = jnp.concatenate(
        [
            lower * cos_ref[...] - upper * sin_ref[...],
            upper * cos_ref[...] + lower * sin_ref[...],
        ],
        axis=1,
    )
    key_new = dot(chosen, key_new.astype(BF16))
    self_score = (
        jnp.sum(absorbed.astype(F32) * latent, axis=1, keepdims=True)
        + jnp.sum(turned.astype(F32) * key_new, axis=1, keepdims=True)
    ) * scale
    scores = jnp.zeros((rows, places), F32)
    for s in range(seqs):
        below = keys_ref[s, :half, :].astype(F32)
        above = keys_ref[s, half:, :].astype(F32)
        keys = jnp.concatenate(
            [
                below * cos_table_ref[...] - above * sin_table_ref[...],
                above * cos_table_ref[...] + below * sin_table_ref[...],
            ],
            axis=0,
        ).astype(BF16)
        part = dot_t(absorbed, cache_ref[s]) + dot(turned, keys)
        scores = jnp.where(row_seq == s, part, scores)
    valid = lax.broadcasted_iota(jnp.int32, (rows, places), 1) < lengths
    scores = jnp.where(valid, scores * scale, NEG)
    top = jnp.maximum(jnp.max(scores, axis=1, keepdims=True), self_score)
    weights = jnp.where(valid, jnp.exp(scores - top), 0.0)
    self_weight = jnp.exp(self_score - top)
    total = jnp.sum(weights, axis=1, keepdims=True) + self_weight
    summed = self_weight.astype(BF16).astype(F32) * latent
    for s in range(seqs):
        summed = summed + dot(jnp.where(row_seq == s, weights, 0.0).astype(BF16), cache_ref[s])
    out_ref[...] = (summed / total).astype(BF16).reshape(out_ref.shape)
    for copy in copies:
        copy.wait()


def weights_body(gate_ref, up_ref, down_ref, out_ref):
    width, units = gate_ref.shape
    out_ref[:width, :] = gate_ref[...]
    out_ref[width : 2 * width, :] = up_ref[...]
    for j in range(width // units):
        at = 2 * width + j * units
        out_ref[at : at + units, :] = down_ref[:, j * units : (j + 1) * units]


def moe_body(arr_ref, tok_ref, gain_ref, placing_ref, weights_ref, resid_ref, out_ref):
    head_sum = arr_ref[0].astype(F32)
    for i in range(1, arr_ref.shape[0]):
        head_sum = head_sum + arr_ref[i].astype(F32)
    resid = (tok_ref[...].astype(F32) + head_sum).astype(BF16)
    resid_ref[...] = resid
    width = resid.shape[1]
    moe_input = rms_scaled(resid, gain_ref[...]).astype(BF16)
    out_ref[:, :width] = dot(placing_ref[...], moe_input).astype(BF16)
    out_ref[:, width:] = weights_ref[...]


def heads_body(arr_ref, value_ref, out_w_ref, out_ref):
    peers, each, rank = arr_ref.shape
    rows = peers * each
    heads = value_ref.shape[1] // VDIM
    seqs = each // heads
    values = dot(arr_ref[...].reshape(rows, rank), value_ref[...]).astype(BF16)
    to = lax.broadcasted_iota(jnp.int32, (rows // heads, rows), 0)
    at = lax.broadcasted_iota(jnp.int32, (rows // heads, rows), 1)
    column = lax.broadcasted_iota(jnp.int32, (rows // heads, heads * VDIM), 1)
    picked = jnp.zeros((rows // heads, heads * VDIM), F32)
    for h in range(heads):
        chosen = (at == (to // seqs) * each + h * seqs + to % seqs).astype(BF16)
        picked = jnp.where(column // VDIM == h, dot(chosen, values), picked)
    partial = dot(picked.astype(BF16), out_w_ref[...]).astype(BF16)
    for i in range(out_ref.shape[0]):
        out_ref[i] = partial


def experts_body(index_ref, rows_ref, own_ref, other_ref, out_ref):
    chips, quarters, cap, quarter = out_ref.shape
    width = quarters * quarter
    units = own_ref.shape[1]
    inside = rows_ref[:, :width]
    extra = rows_ref[:, width:].astype(F32)
    lane = lax.broadcasted_iota(jnp.int32, extra.shape, 1)
    here = index_ref[0]
    there = here + 1 - 2 * (here % 2)
    hidden, scales = [], []
    for weights_ref, place_in in ((own_ref, here), (other_ref, there)):
        gate_pre = dot(inside, weights_ref[:width, :])
        up_pre = dot(inside, weights_ref[width : 2 * width, :])
        hidden.append((gate_pre / (1.0 + jnp.exp(-gate_pre)) * up_pre).astype(BF16))
        scales.append(jnp.sum(jnp.where(lane == place_in, extra, 0.0), axis=1, keepdims=True))
    for q in range(quarters):
        pieces = []
        for j in range(q * quarter // units, (q + 1) * quarter // units):
            at = 2 * width + j * units
            summed = dot(hidden[0], own_ref[at : at + units, :]) * scales[0]
            pieces.append(summed + dot(hidden[1], other_ref[at : at + units, :]) * scales[1])
        whole = jnp.concatenate(pieces, axis=1).astype(BF16)
        out_ref[:, q] = whole.reshape(chips, cap, quarter)


def mix_body(index_ref, arr_ref, placing_ref, resid_ref, out_hbm, out_ref, sem):
    parts, near_chips, planes, quarters, cap, quarter = arr_ref.shape
    totals = []
    for p in range(parts):
        total = jnp.zeros((planes, cap, quarter), F32)
        for y in range(near_chips):
            for x in range(quarters):
                total = total + arr_ref[p, y, :, x].astype(F32)
        totals.append(total.reshape(planes * cap, quarter))
    picked = dot(placing_ref[...], jnp.concatenate(totals, axis=0).astype(BF16))
    resid = resid_ref[:, :quarter]
    for i in range(1, quarters):
        resid = jnp.where(index_ref[0] == i, resid_ref[:, i * quarter : (i + 1) * quarter], resid)
    out_ref[...] = (resid.astype(F32) + picked).astype(BF16)
    copy = pltpu.make_async_copy(out_ref, out_hbm, sem.at[0])
    copy.start()
    copy.wait()


def shards(
    tokens,
    attn_gain,
    q_down,
    kv_down,
    rope_down,
    q_latent_gain,
    kv_latent_gain,
    q_up,
    query_gain,
    key_up,
    value_up,
    attn_out,
    cache_latent,
    cache_rope,
    lengths,
    moe_gain,
    route,
    route_weight,
    expert_gate,
    expert_up,
    expert_down,
):
    tp_count = lax.axis_size("tp")
    tp_index = lax.axis_index("tp")
    seq_count, width = tokens.shape
    kv_cols = kv_down.shape[1]
    rank = cache_latent.shape[2]
    heads_here = query_gain.shape[0]
    seqs_mine = cache_latent.shape[0]
    index = tp_index.astype(jnp.int32)[None]
    half_dim = rope_down.shape[1] // 2
    each = heads_here * seqs_mine
    chips = lax.axis_size(CHIPS)
    cores = lax.axis_size(CORE)
    chips_in_group = EPG // cores
    slots = chips // chips_in_group * GROUP_CAP
    planes = lax.axis_size(CHIPS[1])
    parts = chips // planes // chips_in_group
    turns = ROPE_BASE ** (-np.arange(half_dim, dtype=np.float32) / np.float32(half_dim))
    turns = turns.astype(np.float32)
    angles = turns[:, None] * np.arange(cache_latent.shape[1], dtype=np.float32)
    cos_table = jnp.asarray(np.cos(angles.astype(np.float64)).astype(np.float32))
    sin_table = jnp.asarray(np.sin(angles.astype(np.float64)).astype(np.float32))
    (
        both, new_rope, cosines, sines, placing, placing_t, packed_weights,
        q_up_t, key_near, q_gain, kv_gain, head_gain, cos_table, sin_table, keys, lens,
    ) = down(
        (
            jax.ShapeDtypeStruct((tp_count, 2 * seq_count, kv_cols), BF16),
            jax.ShapeDtypeStruct((seq_count, rope_down.shape[1]), BF16),
            jax.ShapeDtypeStruct((seq_count, half_dim), F32),
            jax.ShapeDtypeStruct((seq_count, half_dim), F32),
            jax.ShapeDtypeStruct((slots, seq_count), BF16),
            jax.ShapeDtypeStruct((seq_count, slots), BF16),
            jax.ShapeDtypeStruct((slots, EXTRA), BF16),
        ),
        (
            tokens,
            attn_gain[None],
            q_down,
            kv_down,
            rope_down.T,
            lengths[None],
            jnp.asarray(turns[None]),
            route.T,
            route_weight.T,
        ),
        (
            q_up.T,
            key_up,
            q_latent_gain[None],
            kv_latent_gain[None],
            query_gain,
            cos_table,
            sin_table,
            cache_rope,
            lengths[None],
        ),
        parts,
    )
    expert_here = (lax.axis_index(EP) % EPG).astype(jnp.int32)[None]
    quarter_cols = width // tp_count
    both, index, expert_here = lax.optimization_barrier((both, index, expert_here))
    latents = lax.all_to_all(both, "tp", 0, 0, tiled=True)
    send, latent_new, mine_new, cache = run(
        query_body,
        (
            jax.ShapeDtypeStruct((tp_count, each, rank + 2 * half_dim), BF16),
            jax.ShapeDtypeStruct((seq_count, rank), BF16),
            jax.ShapeDtypeStruct((seq_count, kv_cols), BF16),
            jax.ShapeDtypeStruct(cache_latent.shape, BF16),
        ),
        index,
        cache_latent,
        latents,
        q_gain,
        kv_gain,
        q_up_t,
        head_gain,
        key_near,
        cosines,
        sines,
        scalars=1,
        hbm_in=1,
        sems=1,
    )
    queries = lax.all_to_all(send, "tp", 0, 0, tiled=True)
    units = expert_gate.shape[2]
    attended, new_latent, new_rope = run(
        attend_body,
        (
            jax.ShapeDtypeStruct((tp_count, each, rank), BF16),
            jax.ShapeDtypeStruct((seq_count, kv_cols), BF16),
            jax.ShapeDtypeStruct(new_rope.shape, BF16),
        ),
        index,
        queries,
        cache,
        keys,
        cos_table,
        sin_table,
        latent_new,
        mine_new,
        new_rope,
        cosines,
        sines,
        lens,
        scalars=1,
        hbm_out=2,
        sems=2,
    )
    attended_heads = lax.all_to_all(attended, "tp", 0, 0, tiled=True)
    (partials,) = run(
        heads_body,
        (jax.ShapeDtypeStruct((tp_count, seq_count, width), BF16),),
        attended_heads,
        value_up,
        attn_out,
    )
    partials, gate, up, lower = lax.optimization_barrier(
        (partials, expert_gate[0], expert_up[0], expert_down[0])
    )
    summands = lax.all_to_all(partials, "tp", 0, 0, tiled=True)
    (own_weights,) = run(
        weights_body, (jax.ShapeDtypeStruct((3 * width, units), BF16),), gate, up, lower
    )
    swap = [(i, cores - 1 - i) for i in range(cores)]
    other_weights = lax.ppermute(own_weights, CORE, swap)
    attn_resid, packed = run(
        moe_body,
        (
            jax.ShapeDtypeStruct((seq_count, width), BF16),
            jax.ShapeDtypeStruct((slots, width + EXTRA), BF16),
        ),
        summands,
        tokens,
        moe_gain[None],
        placing,
        packed_weights,
    )
    packed = jnp.broadcast_to(
        packed.reshape(parts, 1, planes, GROUP_CAP, width + EXTRA),
        (parts, chips_in_group, planes, GROUP_CAP, width + EXTRA),
    ).reshape(chips, GROUP_CAP, width + EXTRA)
    arrived = lax.all_to_all(packed, CHIPS, 0, 0, tiled=True).reshape(-1, width + EXTRA)
    (sums,) = run(
        experts_body,
        (jax.ShapeDtypeStruct((chips, tp_count, GROUP_CAP, quarter_cols), BF16),),
        expert_here,
        arrived,
        own_weights,
        other_weights,
        flops=100_000_000,
        scalars=1,
    )
    returned = lax.all_to_all(
        sums.reshape(chips * tp_count, GROUP_CAP, quarter_cols), (*CHIPS, "tp"), 0, 0, tiled=True
    ).reshape(parts, chips_in_group, planes, tp_count, GROUP_CAP, quarter_cols)
    (mixed_out,) = run(
        mix_body,
        (jax.ShapeDtypeStruct((seq_count, quarter_cols), BF16),),
        index,
        returned,
        placing_t,
        attn_resid,
        scalars=1,
        hbm_out=1,
        sems=1,
        scratch=(pltpu.VMEM((seq_count, quarter_cols), BF16),),
    )
    return (mixed_out, new_latent, new_rope)


def solution(mesh):
    torus = Mesh(mesh.devices.reshape(8, 8, 2, mesh.shape["tp"]), ("ep_0", "ep_1", "ep_2", "tp"))
    placed = (
        P(EP, None),
        P(),
        P(None, "tp"),
        P(None, "tp"),
        P(),
        P(),
        P(),
        P(None, "tp"),
        P("tp", None),
        P(None, "tp"),
        P(None, "tp"),
        P("tp", None),
        P(EP_TP, None, None),
        P(EP_TP, None, None),
        P(EP),
        P(),
        P(EP, None),
        P(EP, None),
        P(EP, None, "tp"),
        P(EP, None, "tp"),
        P(EP, "tp", None),
    )
    return jax.shard_map(
        shards,
        mesh=torus,
        in_specs=placed,
        out_specs=(P(EP, "tp"), P(EP, "tp"), P(EP, None)),
        check_vma=False,
    )
```

```python
import jax
import jax.numpy as jnp
import numpy as np
from jax import lax
from jax.experimental import pallas as pl
from jax.experimental.pallas import tpu as pltpu
from jax.sharding import Mesh
from jax.sharding import PartitionSpec as P

NOPE = 64
VDIM = 64
QK = 96
EPG = 8
EP = ("ep_0", "ep_1", "ep_2")
CHIPS = ("ep_1", "ep_0")
CORE = "ep_2"
GROUP_CAP = 2
EXTRA = 128
EP_TP = ("ep_0", "ep_1", "ep_2", "tp")


EPS = 1e-06
ROPE_BASE = 10000.0
F32 = jnp.float32
BF16 = jnp.bfloat16
NEG = -1e30


def rms_scaled(values_in, gain_vec):
    values_in = values_in.astype(jnp.float32)
    return (
        values_in
        * lax.rsqrt(jnp.mean(values_in * values_in, axis=-1, keepdims=True) + EPS)
        * gain_vec
    )


def dot(a, b):
    return jnp.dot(a, b, preferred_element_type=F32)


def dot_t(a, b):
    return lax.dot_general(a, b, (((1,), (1,)), ((), ())), preferred_element_type=F32)


def near(array):
    return pltpu.with_memory_space_constraint(array, pltpu.VMEM)


def far(array):
    return pltpu.with_memory_space_constraint(array, pltpu.HBM)


def run(body, outs, *args, flops=2_000_000, scalars=0, hbm_in=0, hbm_out=0, sems=0, scratch=()):
    moved = sum(a.size * a.dtype.itemsize for a in args)
    spaces = [pltpu.SMEM] * scalars + [pltpu.HBM] * hbm_in
    spaces += [pltpu.VMEM] * (len(args) - len(spaces))
    kinds = [pltpu.VMEM] * (len(outs) - hbm_out) + [pltpu.HBM] * hbm_out
    place_in = {pltpu.SMEM: lambda a: a, pltpu.HBM: far, pltpu.VMEM: near}
    return pl.pallas_call(
        body,
        compiler_params=pltpu.CompilerParams(vmem_limit_bytes=16 * 1024 * 1024),
        in_specs=[pl.BlockSpec(memory_space=kind) for kind in spaces],
        out_specs=[pl.BlockSpec(memory_space=kind) for kind in kinds],
        out_shape=[kind(o.shape, o.dtype) for kind, o in zip(kinds, outs)],
        scratch_shapes=[*scratch] + ([pltpu.SemaphoreType.DMA((sems,))] if sems else []),
        cost_estimate=pl.CostEstimate(flops=flops, transcendentals=0, bytes_accessed=moved),
    )(*[place_in[kind](a) for kind, a in zip(spaces, args)])


def place(route_ref, weight_ref, placing_ref, turned_ref, weights_ref, parts):
    topk, rows = route_ref.shape
    slots = placing_ref.shape[0]
    group = route_ref[0:1, :] // EPG
    group = group % parts * (slots // GROUP_CAP // parts) + group // parts
    first = lax.broadcasted_iota(jnp.int32, (rows, rows), 0)
    second = lax.broadcasted_iota(jnp.int32, (rows, rows), 1)
    column = jnp.sum(jnp.where(first == second, group, 0), axis=1, keepdims=True)
    earlier = jnp.where((column == group) & (first < second), 1, 0)
    slot = group * GROUP_CAP + jnp.sum(earlier, axis=0, keepdims=True)
    placing = (lax.broadcasted_iota(jnp.int32, (slots, rows), 0) == slot).astype(BF16)
    placing_ref[...] = placing
    slot_column = jnp.sum(jnp.where(first == second, slot, 0), axis=1, keepdims=True)
    turned_ref[...] = (
        lax.broadcasted_iota(jnp.int32, (rows, slots), 1) == slot_column
    ).astype(BF16)
    lane = lax.broadcasted_iota(jnp.int32, (EXTRA, rows), 0)
    table = jnp.zeros((EXTRA, rows), F32)
    for k in range(topk):
        table = table + jnp.where(route_ref[k : k + 1, :] % EPG == lane, weight_ref[k : k + 1, :], 0.0)
    weights_ref[...] = dot_t(placing, table.astype(BF16)).astype(BF16)


OWN = 9
MADE = 7


def down_body(parts, *refs):
    count = (len(refs) - MADE - 1) // 2
    hbm, made, last = refs[:count], refs[count : count + MADE], refs[count + MADE : -1]
    sems = refs[-1]
    near_refs = last[count - OWN :] + last[: count - OWN]
    copies = [pltpu.make_async_copy(hbm[i], near_refs[i], sems.at[i]) for i in range(count)]
    for copy in copies:
        copy.start()
    tok_ref, gain_ref, q_ref, kv_ref, rope_ref, len_ref, turn_ref, route_ref, weight_ref = near_refs[
        :OWN
    ]
    both_ref, new_rope_ref, cos_ref, sin_ref, placing_ref, turned_ref, weights_ref = made
    copies[0].wait()
    copies[1].wait()
    normed = rms_scaled(tok_ref[...], gain_ref[...]).astype(BF16)
    rows = normed.shape[0]
    copies[2].wait()
    q_part = dot(normed, q_ref[...]).astype(BF16)
    copies[3].wait()
    kv_part = dot(normed, kv_ref[...]).astype(BF16)
    for i in range(both_ref.shape[0]):
        both_ref[i, :rows, :] = q_part
        both_ref[i, rows:, :] = kv_part
    for i in range(4, OWN):
        copies[i].wait()
    new_rope_ref[...] = dot_t(normed, rope_ref[...]).astype(BF16)
    first = lax.broadcasted_iota(jnp.int32, (rows, rows), 0)
    second = lax.broadcasted_iota(jnp.int32, (rows, rows), 1)
    lengths = jnp.sum(jnp.where(first == second, len_ref[...], 0), axis=1, keepdims=True)
    angles = lengths.astype(F32) * turn_ref[...]
    cos_ref[...] = jnp.cos(angles)
    sin_ref[...] = jnp.sin(angles)
    place(route_ref, weight_ref, placing_ref, turned_ref, weights_ref, parts)
    for copy in copies[OWN:]:
        copy.wait()


def down(made, own, others, parts):
    args = (*own, *others)
    moved = sum(a.size * a.dtype.itemsize for a in args)
    outs = [pltpu.VMEM(o.shape, o.dtype) for o in (*made, *others)]
    return pl.pallas_call(
        lambda *refs: down_body(parts, *refs),
        compiler_params=pltpu.CompilerParams(vmem_limit_bytes=16 * 1024 * 1024),
        in_specs=[pl.BlockSpec(memory_space=pltpu.HBM)] * len(args),
        out_specs=[pl.BlockSpec(memory_space=pltpu.VMEM)] * len(outs),
        out_shape=outs,
        scratch_shapes=[pltpu.VMEM(a.shape, a.dtype) for a in own]
        + [pltpu.SemaphoreType.DMA((len(args),))],
        cost_estimate=pl.CostEstimate(flops=2_000_000, transcendentals=0, bytes_accessed=moved),
    )(*[far(a) for a in args])


def query_body(
    index_ref, cache_hbm, arr_ref, q_gain_ref, kv_gain_ref, q_up_ref, head_gain_ref, key_up_ref,
    cos_ref, sin_ref, send_ref, latent_ref, mine_ref, cache_ref, sem,
):
    copies = [
        pltpu.make_async_copy(cache_hbm.at[s], cache_ref.at[s], sem.at[s])
        for s in range(cache_ref.shape[0])
    ]
    for copy in copies:
        copy.start()
    peers, both, cols = arr_ref.shape
    rows = both // 2
    rank = key_up_ref.shape[0]
    half = cos_ref.shape[1]
    q_raw = jnp.concatenate([arr_ref[i, :rows, :] for i in range(peers)], axis=1)
    kv_raw = jnp.concatenate([arr_ref[i, rows:, :] for i in range(peers)], axis=1)
    latent = rms_scaled(kv_raw, kv_gain_ref[...]).astype(BF16)
    latent_ref[...] = latent
    mine = latent[:, :cols]
    for i in range(1, peers):
        mine = jnp.where(index_ref[0] == i, latent[:, i * cols : (i + 1) * cols], mine)
    mine_ref[...] = mine
    q_lat = rms_scaled(q_raw, q_gain_ref[...]).astype(BF16)
    query = dot_t(q_lat, q_up_ref[...])
    each = rows // peers
    for h in range(head_gain_ref.shape[0]):
        one = rms_scaled(query[:, h * QK : (h + 1) * QK], head_gain_ref[h : h + 1, :])
        lower = one[:, NOPE : NOPE + half]
        upper = one[:, NOPE + half :]
        turned = jnp.concatenate(
            [
                lower * cos_ref[...] - upper * sin_ref[...],
                upper * cos_ref[...] + lower * sin_ref[...],
            ],
            axis=1,
        )
        absorbed = dot_t(one[:, :NOPE].astype(BF16), key_up_ref[:, h * NOPE : (h + 1) * NOPE])
        for i in range(peers):
            at = slice(h * each, (h + 1) * each)
            send_ref[i, at, :rank] = absorbed[i * each : (i + 1) * each].astype(BF16)
            send_ref[i, at, rank:] = turned[i * each : (i + 1) * each].astype(BF16)
    for copy in copies:
        copy.wait()


def attend_body(
    index_ref, arr_ref, cache_ref, keys_ref, cos_table_ref, sin_table_ref, latent_ref, mine_ref,
    rope_ref, cos_ref, sin_ref, len_ref, out_ref, latent_out, rope_out, sems,
):
    copies = [
        pltpu.make_async_copy(mine_ref, latent_out, sems.at[0]),
        pltpu.make_async_copy(rope_ref, rope_out, sems.at[1]),
    ]
    for copy in copies:
        copy.start()
    seqs, places, rank = cache_ref.shape
    peers, each, _ = arr_ref.shape
    rows = peers * each
    half = cos_ref.shape[1]
    arrived = arr_ref[...].reshape(rows, arr_ref.shape[2])
    absorbed = arrived[:, :rank]
    turned = arrived[:, rank:]
    scale = QK ** (-0.5)
    row_seq = lax.broadcasted_iota(jnp.int32, (rows, 1), 0) % seqs
    every = latent_ref.shape[0]
    chosen = lax.broadcasted_iota(jnp.int32, (rows, every), 1) == row_seq + index_ref[0] * seqs
    lengths = jnp.sum(jnp.where(chosen, len_ref[...], 0), axis=1, keepdims=True)
    chosen = chosen.astype(BF16)
    latent = dot(chosen, latent_ref[...])
    lower = rope_ref[:, :half].astype(F32)
    upper = rope_ref[:, half:].astype(F32)
    key_new = jnp.concatenate(
        [
            lower * cos_ref[...] - upper * sin_ref[...],
            upper * cos_ref[...] + lower * sin_ref[...],
        ],
        axis=1,
    )
    key_new = dot(chosen, key_new.astype(BF16))
    self_score = (
        jnp.sum(absorbed.astype(F32) * latent, axis=1, keepdims=True)
        + jnp.sum(turned.astype(F32) * key_new, axis=1, keepdims=True)
    ) * scale
    scores = jnp.zeros((rows, places), F32)
    for s in range(seqs):
        below = keys_ref[s, :half, :].astype(F32)
        above = keys_ref[s, half:, :].astype(F32)
        keys = jnp.concatenate(
            [
                below * cos_table_ref[...] - above * sin_table_ref[...],
                above * cos_table_ref[...] + below * sin_table_ref[...],
            ],
            axis=0,
        ).astype(BF16)
        part = dot_t(absorbed, cache_ref[s]) + dot(turned, keys)
        scores = jnp.where(row_seq == s, part, scores)
    valid = lax.broadcasted_iota(jnp.int32, (rows, places), 1) < lengths
    scores = jnp.where(valid, scores * scale, NEG)
    top = jnp.maximum(jnp.max(scores, axis=1, keepdims=True), self_score)
    weights = jnp.where(valid, jnp.exp(scores - top), 0.0)
    self_weight = jnp.exp(self_score - top)
    total = jnp.sum(weights, axis=1, keepdims=True) + self_weight
    summed = self_weight.astype(BF16).astype(F32) * latent
    for s in range(seqs):
        summed = summed + dot(jnp.where(row_seq == s, weights, 0.0).astype(BF16), cache_ref[s])
    out_ref[...] = (summed / total).astype(BF16).reshape(out_ref.shape)
    for copy in copies:
        copy.wait()


def weights_body(gate_ref, up_ref, down_ref, out_ref):
    width, units = gate_ref.shape
    out_ref[:width, :] = gate_ref[...]
    out_ref[width : 2 * width, :] = up_ref[...]
    for j in range(width // units):
        at = 2 * width + j * units
        out_ref[at : at + units, :] = down_ref[:, j * units : (j + 1) * units]


def moe_body(arr_ref, tok_ref, gain_ref, placing_ref, weights_ref, resid_ref, out_ref):
    head_sum = arr_ref[0].astype(F32)
    for i in range(1, arr_ref.shape[0]):
        head_sum = head_sum + arr_ref[i].astype(F32)
    resid = (tok_ref[...].astype(F32) + head_sum).astype(BF16)
    resid_ref[...] = resid
    width = resid.shape[1]
    moe_input = rms_scaled(resid, gain_ref[...]).astype(BF16)
    parts, copies, planes, cap, _ = out_ref.shape
    rows = dot(placing_ref[...], moe_input).astype(BF16)
    for p in range(parts):
        at = slice(p * planes * cap, (p + 1) * planes * cap)
        main = rows[at].reshape(planes, cap, width)
        side = weights_ref[at, :].reshape(planes, cap, EXTRA)
        for i in range(copies):
            out_ref[p, i, :, :, :width] = main
            out_ref[p, i, :, :, width:] = side


def heads_body(arr_ref, value_ref, out_w_ref, out_ref):
    peers, each, rank = arr_ref.shape
    rows = peers * each
    heads = value_ref.shape[1] // VDIM
    seqs = each // heads
    values = dot(arr_ref[...].reshape(rows, rank), value_ref[...]).astype(BF16)
    to = lax.broadcasted_iota(jnp.int32, (rows // heads, rows), 0)
    at = lax.broadcasted_iota(jnp.int32, (rows // heads, rows), 1)
    column = lax.broadcasted_iota(jnp.int32, (rows // heads, heads * VDIM), 1)
    picked = jnp.zeros((rows // heads, heads * VDIM), F32)
    for h in range(heads):
        chosen = (at == (to // seqs) * each + h * seqs + to % seqs).astype(BF16)
        picked = jnp.where(column // VDIM == h, dot(chosen, values), picked)
    partial = dot(picked.astype(BF16), out_w_ref[...]).astype(BF16)
    for i in range(out_ref.shape[0]):
        out_ref[i] = partial


def experts_body(index_ref, rows_ref, own_ref, other_ref, out_ref):
    chips, quarters, cap, quarter = out_ref.shape
    width = quarters * quarter
    units = own_ref.shape[1]
    inside = rows_ref[:, :, :width].reshape(chips * cap, width)
    extra = rows_ref[:, :, width:].reshape(chips * cap, EXTRA).astype(F32)
    lane = lax.broadcasted_iota(jnp.int32, extra.shape, 1)
    here = index_ref[0]
    there = here + 1 - 2 * (here % 2)
    hidden, scales = [], []
    for weights_ref, place_in in ((own_ref, here), (other_ref, there)):
        gate_pre = dot(inside, weights_ref[:width, :])
        up_pre = dot(inside, weights_ref[width : 2 * width, :])
        hidden.append((gate_pre / (1.0 + jnp.exp(-gate_pre)) * up_pre).astype(BF16))
        scales.append(jnp.sum(jnp.where(lane == place_in, extra, 0.0), axis=1, keepdims=True))
    for q in range(quarters):
        pieces = []
        for j in range(q * quarter // units, (q + 1) * quarter // units):
            at = 2 * width + j * units
            summed = dot(hidden[0], own_ref[at : at + units, :]) * scales[0]
            pieces.append(summed + dot(hidden[1], other_ref[at : at + units, :]) * scales[1])
        whole = jnp.concatenate(pieces, axis=1).astype(BF16)
        out_ref[:, q] = whole.reshape(chips, cap, quarter)


def mix_body(index_ref, arr_ref, placing_ref, resid_ref, out_hbm, out_ref, sem):
    parts, near_chips, planes, quarters, cap, quarter = arr_ref.shape
    totals = []
    for p in range(parts):
        total = jnp.zeros((planes, cap, quarter), F32)
        for y in range(near_chips):
            for x in range(quarters):
                total = total + arr_ref[p, y, :, x].astype(F32)
        totals.append(total.reshape(planes * cap, quarter))
    picked = dot(placing_ref[...], jnp.concatenate(totals, axis=0).astype(BF16))
    resid = resid_ref[:, :quarter]
    for i in range(1, quarters):
        resid = jnp.where(index_ref[0] == i, resid_ref[:, i * quarter : (i + 1) * quarter], resid)
    out_ref[...] = (resid.astype(F32) + picked).astype(BF16)
    copy = pltpu.make_async_copy(out_ref, out_hbm, sem.at[0])
    copy.start()
    copy.wait()


def shards(
    tokens,
    attn_gain,
    q_down,
    kv_down,
    rope_down,
    q_latent_gain,
    kv_latent_gain,
    q_up,
    query_gain,
    key_up,
    value_up,
    attn_out,
    cache_latent,
    cache_rope,
    lengths,
    moe_gain,
    route,
    route_weight,
    expert_gate,
    expert_up,
    expert_down,
):
    tp_count = lax.axis_size("tp")
    tp_index = lax.axis_index("tp")
    seq_count, width = tokens.shape
    kv_cols = kv_down.shape[1]
    rank = cache_latent.shape[2]
    heads_here = query_gain.shape[0]
    seqs_mine = cache_latent.shape[0]
    index = tp_index.astype(jnp.int32)[None]
    half_dim = rope_down.shape[1] // 2
    each = heads_here * seqs_mine
    chips = lax.axis_size(CHIPS)
    cores = lax.axis_size(CORE)
    chips_in_group = EPG // cores
    slots = chips // chips_in_group * GROUP_CAP
    planes = lax.axis_size(CHIPS[1])
    parts = chips // planes // chips_in_group
    turns = ROPE_BASE ** (-np.arange(half_dim, dtype=np.float32) / np.float32(half_dim))
    turns = turns.astype(np.float32)
    angles = turns[:, None] * np.arange(cache_latent.shape[1], dtype=np.float32)
    cos_table = jnp.asarray(np.cos(angles.astype(np.float64)).astype(np.float32))
    sin_table = jnp.asarray(np.sin(angles.astype(np.float64)).astype(np.float32))
    (
        both, new_rope, cosines, sines, placing, placing_t, packed_weights,
        q_up_t, key_near, q_gain, kv_gain, head_gain, cos_table, sin_table, keys, lens,
    ) = down(
        (
            jax.ShapeDtypeStruct((tp_count, 2 * seq_count, kv_cols), BF16),
            jax.ShapeDtypeStruct((seq_count, rope_down.shape[1]), BF16),
            jax.ShapeDtypeStruct((seq_count, half_dim), F32),
            jax.ShapeDtypeStruct((seq_count, half_dim), F32),
            jax.ShapeDtypeStruct((slots, seq_count), BF16),
            jax.ShapeDtypeStruct((seq_count, slots), BF16),
            jax.ShapeDtypeStruct((slots, EXTRA), BF16),
        ),
        (
            tokens,
            attn_gain[None],
            q_down,
            kv_down,
            rope_down.T,
            lengths[None],
            jnp.asarray(turns[None]),
            route.T,
            route_weight.T,
        ),
        (
            q_up.T,
            key_up,
            q_latent_gain[None],
            kv_latent_gain[None],
            query_gain,
            cos_table,
            sin_table,
            cache_rope,
            lengths[None],
        ),
        parts,
    )
    expert_here = (lax.axis_index(EP) % EPG).astype(jnp.int32)[None]
    quarter_cols = width // tp_count
    both, index, expert_here = lax.optimization_barrier((both, index, expert_here))
    latents = lax.all_to_all(both, "tp", 0, 0, tiled=True)
    send, latent_new, mine_new, cache = run(
        query_body,
        (
            jax.ShapeDtypeStruct((tp_count, each, rank + 2 * half_dim), BF16),
            jax.ShapeDtypeStruct((seq_count, rank), BF16),
            jax.ShapeDtypeStruct((seq_count, kv_cols), BF16),
            jax.ShapeDtypeStruct(cache_latent.shape, BF16),
        ),
        index,
        cache_latent,
        latents,
        q_gain,
        kv_gain,
        q_up_t,
        head_gain,
        key_near,
        cosines,
        sines,
        scalars=1,
        hbm_in=1,
        sems=seqs_mine,
    )
    queries = lax.all_to_all(send, "tp", 0, 0, tiled=True)
    units = expert_gate.shape[2]
    attended, new_latent, new_rope = run(
        attend_body,
        (
            jax.ShapeDtypeStruct((tp_count, each, rank), BF16),
            jax.ShapeDtypeStruct((seq_count, kv_cols), BF16),
            jax.ShapeDtypeStruct(new_rope.shape, BF16),
        ),
        index,
        queries,
        cache,
        keys,
        cos_table,
        sin_table,
        latent_new,
        mine_new,
        new_rope,
        cosines,
        sines,
        lens,
        scalars=1,
        hbm_out=2,
        sems=2,
    )
    attended_heads = lax.all_to_all(attended, "tp", 0, 0, tiled=True)
    (partials,) = run(
        heads_body,
        (jax.ShapeDtypeStruct((tp_count, seq_count, width), BF16),),
        attended_heads,
        value_up,
        attn_out,
    )
    partials, gate, up, lower = lax.optimization_barrier(
        (partials, expert_gate[0], expert_up[0], expert_down[0])
    )
    summands = lax.all_to_all(partials, "tp", 0, 0, tiled=True)
    (own_weights,) = run(
        weights_body, (jax.ShapeDtypeStruct((3 * width, units), BF16),), gate, up, lower
    )
    swap = [(i, cores - 1 - i) for i in range(cores)]
    other_weights = lax.ppermute(own_weights, CORE, swap)
    attn_resid, packed = run(
        moe_body,
        (
            jax.ShapeDtypeStruct((seq_count, width), BF16),
            jax.ShapeDtypeStruct(
                (parts, chips_in_group, planes, GROUP_CAP, width + EXTRA), BF16
            ),
        ),
        summands,
        tokens,
        moe_gain[None],
        placing,
        packed_weights,
    )
    packed = packed.reshape(chips, GROUP_CAP, width + EXTRA)
    arrived = lax.all_to_all(packed, CHIPS, 0, 0, tiled=True)
    (sums,) = run(
        experts_body,
        (jax.ShapeDtypeStruct((chips, tp_count, GROUP_CAP, quarter_cols), BF16),),
        expert_here,
        arrived,
        own_weights,
        other_weights,
        flops=100_000_000,
        scalars=1,
    )
    returned = lax.all_to_all(
        sums.reshape(chips * tp_count, GROUP_CAP, quarter_cols), (*CHIPS, "tp"), 0, 0, tiled=True
    ).reshape(parts, chips_in_group, planes, tp_count, GROUP_CAP, quarter_cols)
    (mixed_out,) = run(
        mix_body,
        (jax.ShapeDtypeStruct((seq_count, quarter_cols), BF16),),
        index,
        returned,
        placing_t,
        attn_resid,
        scalars=1,
        hbm_out=1,
        sems=1,
        scratch=(pltpu.VMEM((seq_count, quarter_cols), BF16),),
    )
    return (mixed_out, new_latent, new_rope)


def solution(mesh):
    torus = Mesh(mesh.devices.reshape(8, 8, 2, mesh.shape["tp"]), ("ep_0", "ep_1", "ep_2", "tp"))
    placed = (
        P(EP, None),
        P(),
        P(None, "tp"),
        P(None, "tp"),
        P(),
        P(),
        P(),
        P(None, "tp"),
        P("tp", None),
        P(None, "tp"),
        P(None, "tp"),
        P("tp", None),
        P(EP_TP, None, None),
        P(EP_TP, None, None),
        P(EP),
        P(),
        P(EP, None),
        P(EP, None),
        P(EP, None, "tp"),
        P(EP, None, "tp"),
        P(EP, "tp", None),
    )
    return jax.shard_map(
        shards,
        mesh=torus,
        in_specs=placed,
        out_specs=(P(EP, "tp"), P(EP, "tp"), P(EP, None)),
        check_vma=False,
    )
```

```python
import jax
import jax.numpy as jnp
import numpy as np
from jax import lax
from jax.experimental import pallas as pl
from jax.experimental.pallas import tpu as pltpu
from jax.sharding import Mesh
from jax.sharding import PartitionSpec as P

NOPE = 64
VDIM = 64
QK = 96
EPG = 8
EP = ("ep_0", "ep_1", "ep_2")
CHIPS = ("ep_1", "ep_0")
CORE = "ep_2"
GROUP_CAP = 2
EXTRA = 128
EP_TP = ("ep_0", "ep_1", "ep_2", "tp")


EPS = 1e-06
ROPE_BASE = 10000.0
F32 = jnp.float32
BF16 = jnp.bfloat16
NEG = -1e30


def rms_scaled(values_in, gain_vec):
    values_in = values_in.astype(jnp.float32)
    return (
        values_in
        * lax.rsqrt(jnp.mean(values_in * values_in, axis=-1, keepdims=True) + EPS)
        * gain_vec
    )


def dot(a, b):
    return jnp.dot(a, b, preferred_element_type=F32)


def dot_t(a, b):
    return lax.dot_general(a, b, (((1,), (1,)), ((), ())), preferred_element_type=F32)


def near(array):
    return pltpu.with_memory_space_constraint(array, pltpu.VMEM)


def far(array):
    return pltpu.with_memory_space_constraint(array, pltpu.HBM)


def run(body, outs, *args, flops=2_000_000, scalars=0, hbm_in=0, hbm_out=0, sems=0, scratch=()):
    moved = sum(a.size * a.dtype.itemsize for a in args)
    spaces = [pltpu.SMEM] * scalars + [pltpu.HBM] * hbm_in
    spaces += [pltpu.VMEM] * (len(args) - len(spaces))
    kinds = [pltpu.VMEM] * (len(outs) - hbm_out) + [pltpu.HBM] * hbm_out
    place_in = {pltpu.SMEM: lambda a: a, pltpu.HBM: far, pltpu.VMEM: near}
    return pl.pallas_call(
        body,
        compiler_params=pltpu.CompilerParams(vmem_limit_bytes=16 * 1024 * 1024),
        in_specs=[pl.BlockSpec(memory_space=kind) for kind in spaces],
        out_specs=[pl.BlockSpec(memory_space=kind) for kind in kinds],
        out_shape=[kind(o.shape, o.dtype) for kind, o in zip(kinds, outs)],
        scratch_shapes=[*scratch] + ([pltpu.SemaphoreType.DMA((sems,))] if sems else []),
        cost_estimate=pl.CostEstimate(flops=flops, transcendentals=0, bytes_accessed=moved),
    )(*[place_in[kind](a) for kind, a in zip(spaces, args)])


def place(route_ref, weight_ref, placing_ref, turned_ref, weights_ref, parts):
    topk, rows = route_ref.shape
    slots = placing_ref.shape[0]
    group = route_ref[0:1, :] // EPG
    group = group % parts * (slots // GROUP_CAP // parts) + group // parts
    first = lax.broadcasted_iota(jnp.int32, (rows, rows), 0)
    second = lax.broadcasted_iota(jnp.int32, (rows, rows), 1)
    column = jnp.sum(jnp.where(first == second, group, 0), axis=1, keepdims=True)
    earlier = jnp.where((column == group) & (first < second), 1, 0)
    slot = group * GROUP_CAP + jnp.sum(earlier, axis=0, keepdims=True)
    placing = (lax.broadcasted_iota(jnp.int32, (slots, rows), 0) == slot).astype(BF16)
    placing_ref[...] = placing
    slot_column = jnp.sum(jnp.where(first == second, slot, 0), axis=1, keepdims=True)
    turned_ref[...] = (
        lax.broadcasted_iota(jnp.int32, (rows, slots), 1) == slot_column
    ).astype(BF16)
    lane = lax.broadcasted_iota(jnp.int32, (EXTRA, rows), 0)
    table = jnp.zeros((EXTRA, rows), F32)
    for k in range(topk):
        table = table + jnp.where(route_ref[k : k + 1, :] % EPG == lane, weight_ref[k : k + 1, :], 0.0)
    weights_ref[...] = dot_t(placing, table.astype(BF16)).astype(BF16)


OWN = 9
MADE = 7


def down_body(parts, *refs):
    count = (len(refs) - MADE - 1) // 2
    hbm, made, last = refs[:count], refs[count : count + MADE], refs[count + MADE : -1]
    sems = refs[-1]
    near_refs = last[count - OWN :] + last[: count - OWN]
    copies = [pltpu.make_async_copy(hbm[i], near_refs[i], sems.at[i]) for i in range(count)]
    for copy in copies:
        copy.start()
    tok_ref, gain_ref, q_ref, kv_ref, rope_ref, len_ref, turn_ref, route_ref, weight_ref = near_refs[
        :OWN
    ]
    both_ref, new_rope_ref, cos_ref, sin_ref, placing_ref, turned_ref, weights_ref = made
    copies[0].wait()
    copies[1].wait()
    normed = rms_scaled(tok_ref[...], gain_ref[...]).astype(BF16)
    rows = normed.shape[0]
    copies[2].wait()
    q_part = dot(normed, q_ref[...]).astype(BF16)
    copies[3].wait()
    kv_part = dot(normed, kv_ref[...]).astype(BF16)
    for i in range(both_ref.shape[0]):
        both_ref[i, :rows, :] = q_part
        both_ref[i, rows:, :] = kv_part
    for i in range(4, OWN):
        copies[i].wait()
    new_rope_ref[...] = dot_t(normed, rope_ref[...]).astype(BF16)
    first = lax.broadcasted_iota(jnp.int32, (rows, rows), 0)
    second = lax.broadcasted_iota(jnp.int32, (rows, rows), 1)
    lengths = jnp.sum(jnp.where(first == second, len_ref[...], 0), axis=1, keepdims=True)
    angles = lengths.astype(F32) * turn_ref[...]
    cos_ref[...] = jnp.cos(angles)
    sin_ref[...] = jnp.sin(angles)
    place(route_ref, weight_ref, placing_ref, turned_ref, weights_ref, parts)
    for copy in copies[OWN:]:
        copy.wait()


def down(made, own, others, parts):
    args = (*own, *others)
    moved = sum(a.size * a.dtype.itemsize for a in args)
    outs = [pltpu.VMEM(o.shape, o.dtype) for o in (*made, *others)]
    return pl.pallas_call(
        lambda *refs: down_body(parts, *refs),
        compiler_params=pltpu.CompilerParams(vmem_limit_bytes=16 * 1024 * 1024),
        in_specs=[pl.BlockSpec(memory_space=pltpu.HBM)] * len(args),
        out_specs=[pl.BlockSpec(memory_space=pltpu.VMEM)] * len(outs),
        out_shape=outs,
        scratch_shapes=[pltpu.VMEM(a.shape, a.dtype) for a in own]
        + [pltpu.SemaphoreType.DMA((len(args),))],
        cost_estimate=pl.CostEstimate(flops=2_000_000, transcendentals=0, bytes_accessed=moved),
    )(*[far(a) for a in args])


def query_body(
    index_ref, cache_hbm, arr_ref, q_gain_ref, kv_gain_ref, q_up_ref, head_gain_ref, key_up_ref,
    cos_ref, sin_ref, send_ref, latent_ref, mine_ref, cache_ref, sem,
):
    copy = pltpu.make_async_copy(cache_hbm, cache_ref, sem.at[0])
    copy.start()
    peers, both, cols = arr_ref.shape
    rows = both // 2
    rank = key_up_ref.shape[0]
    half = cos_ref.shape[1]
    q_raw = jnp.concatenate([arr_ref[i, :rows, :] for i in range(peers)], axis=1)
    kv_raw = jnp.concatenate([arr_ref[i, rows:, :] for i in range(peers)], axis=1)
    latent = rms_scaled(kv_raw, kv_gain_ref[...]).astype(BF16)
    latent_ref[...] = latent
    mine = latent[:, :cols]
    for i in range(1, peers):
        mine = jnp.where(index_ref[0] == i, latent[:, i * cols : (i + 1) * cols], mine)
    mine_ref[...] = mine
    q_lat = rms_scaled(q_raw, q_gain_ref[...]).astype(BF16)
    query = dot_t(q_lat, q_up_ref[...])
    each = rows // peers
    for h in range(head_gain_ref.shape[0]):
        one = rms_scaled(query[:, h * QK : (h + 1) * QK], head_gain_ref[h : h + 1, :])
        lower = one[:, NOPE : NOPE + half]
        upper = one[:, NOPE + half :]
        turned = jnp.concatenate(
            [
                lower * cos_ref[...] - upper * sin_ref[...],
                upper * cos_ref[...] + lower * sin_ref[...],
            ],
            axis=1,
        )
        absorbed = dot_t(one[:, :NOPE].astype(BF16), key_up_ref[:, h * NOPE : (h + 1) * NOPE])
        for i in range(peers):
            at = slice(h * each, (h + 1) * each)
            send_ref[i, at, :rank] = absorbed[i * each : (i + 1) * each].astype(BF16)
            send_ref[i, at, rank:] = turned[i * each : (i + 1) * each].astype(BF16)
    copy.wait()


def attend_body(
    index_ref, arr_ref, cache_ref, keys_ref, cos_table_ref, sin_table_ref, latent_ref, mine_ref,
    rope_ref, cos_ref, sin_ref, len_ref, out_ref, latent_out, rope_out, sems,
):
    copies = [
        pltpu.make_async_copy(mine_ref, latent_out, sems.at[0]),
        pltpu.make_async_copy(rope_ref, rope_out, sems.at[1]),
    ]
    for copy in copies:
        copy.start()
    seqs, places, rank = cache_ref.shape
    peers, each, _ = arr_ref.shape
    rows = peers * each
    half = cos_ref.shape[1]
    arrived = arr_ref[...].reshape(rows, arr_ref.shape[2])
    absorbed = arrived[:, :rank]
    turned = arrived[:, rank:]
    scale = QK ** (-0.5)
    row_seq = lax.broadcasted_iota(jnp.int32, (rows, 1), 0) % seqs
    every = latent_ref.shape[0]
    chosen = lax.broadcasted_iota(jnp.int32, (rows, every), 1) == row_seq + index_ref[0] * seqs
    lengths = jnp.sum(jnp.where(chosen, len_ref[...], 0), axis=1, keepdims=True)
    chosen = chosen.astype(BF16)
    latent = dot(chosen, latent_ref[...])
    lower = rope_ref[:, :half].astype(F32)
    upper = rope_ref[:, half:].astype(F32)
    key_new = jnp.concatenate(
        [
            lower * cos_ref[...] - upper * sin_ref[...],
            upper * cos_ref[...] + lower * sin_ref[...],
        ],
        axis=1,
    )
    key_new = dot(chosen, key_new.astype(BF16))
    self_score = (
        jnp.sum(absorbed.astype(F32) * latent, axis=1, keepdims=True)
        + jnp.sum(turned.astype(F32) * key_new, axis=1, keepdims=True)
    ) * scale
    scores = jnp.zeros((rows, places), F32)
    for s in range(seqs):
        below = keys_ref[s, :half, :].astype(F32)
        above = keys_ref[s, half:, :].astype(F32)
        keys = jnp.concatenate(
            [
                below * cos_table_ref[...] - above * sin_table_ref[...],
                above * cos_table_ref[...] + below * sin_table_ref[...],
            ],
            axis=0,
        ).astype(BF16)
        part = dot_t(absorbed, cache_ref[s]) + dot(turned, keys)
        scores = jnp.where(row_seq == s, part, scores)
    valid = lax.broadcasted_iota(jnp.int32, (rows, places), 1) < lengths
    scores = jnp.where(valid, scores * scale, NEG)
    top = jnp.maximum(jnp.max(scores, axis=1, keepdims=True), self_score)
    weights = jnp.where(valid, jnp.exp(scores - top), 0.0)
    self_weight = jnp.exp(self_score - top)
    total = jnp.sum(weights, axis=1, keepdims=True) + self_weight
    summed = self_weight.astype(BF16).astype(F32) * latent
    for s in range(seqs):
        summed = summed + dot(jnp.where(row_seq == s, weights, 0.0).astype(BF16), cache_ref[s])
    out_ref[...] = (summed / total).astype(BF16).reshape(out_ref.shape)
    for copy in copies:
        copy.wait()


def weights_body(gate_hbm, up_hbm, down_hbm, out_ref, sems):
    width, units = gate_hbm.shape
    copies = [
        pltpu.make_async_copy(gate_hbm, out_ref.at[:width], sems.at[0]),
        pltpu.make_async_copy(up_hbm, out_ref.at[width : 2 * width], sems.at[1]),
    ]
    for j in range(width // units):
        at = 2 * width + j * units
        copies.append(
            pltpu.make_async_copy(
                down_hbm.at[:, j * units : (j + 1) * units],
                out_ref.at[at : at + units],
                sems.at[2 + j],
            )
        )
    for copy in copies:
        copy.start()
    for copy in copies:
        copy.wait()


def moe_body(arr_ref, tok_ref, gain_ref, placing_ref, weights_ref, resid_ref, out_ref):
    head_sum = arr_ref[0].astype(F32)
    for i in range(1, arr_ref.shape[0]):
        head_sum = head_sum + arr_ref[i].astype(F32)
    resid = (tok_ref[...].astype(F32) + head_sum).astype(BF16)
    resid_ref[...] = resid
    width = resid.shape[1]
    moe_input = rms_scaled(resid, gain_ref[...]).astype(BF16)
    parts, copies, planes, cap, _ = out_ref.shape
    rows = dot(placing_ref[...], moe_input).astype(BF16)
    for p in range(parts):
        at = slice(p * planes * cap, (p + 1) * planes * cap)
        main = rows[at].reshape(planes, cap, width)
        side = weights_ref[at, :].reshape(planes, cap, EXTRA)
        for i in range(copies):
            out_ref[p, i, :, :, :width] = main
            out_ref[p, i, :, :, width:] = side


def heads_body(arr_ref, value_ref, out_w_ref, out_ref):
    peers, each, rank = arr_ref.shape
    rows = peers * each
    heads = value_ref.shape[1] // VDIM
    seqs = each // heads
    values = dot(arr_ref[...].reshape(rows, rank), value_ref[...]).astype(BF16)
    to = lax.broadcasted_iota(jnp.int32, (rows // heads, rows), 0)
    at = lax.broadcasted_iota(jnp.int32, (rows // heads, rows), 1)
    column = lax.broadcasted_iota(jnp.int32, (rows // heads, heads * VDIM), 1)
    picked = jnp.zeros((rows // heads, heads * VDIM), F32)
    for h in range(heads):
        chosen = (at == (to // seqs) * each + h * seqs + to % seqs).astype(BF16)
        picked = jnp.where(column // VDIM == h, dot(chosen, values), picked)
    partial = dot(picked.astype(BF16), out_w_ref[...]).astype(BF16)
    for i in range(out_ref.shape[0]):
        out_ref[i] = partial


def experts_body(index_ref, rows_ref, own_ref, other_ref, out_ref):
    chips, quarters, cap, quarter = out_ref.shape
    width = quarters * quarter
    units = own_ref.shape[1]
    inside = rows_ref[:, :, :width].reshape(chips * cap, width)
    extra = rows_ref[:, :, width:].reshape(chips * cap, EXTRA).astype(F32)
    lane = lax.broadcasted_iota(jnp.int32, extra.shape, 1)
    here = index_ref[0]
    there = here + 1 - 2 * (here % 2)
    hidden, scales = [], []
    for weights_ref, place_in in ((own_ref, here), (other_ref, there)):
        gate_pre = dot(inside, weights_ref[:width, :])
        up_pre = dot(inside, weights_ref[width : 2 * width, :])
        hidden.append((gate_pre / (1.0 + jnp.exp(-gate_pre)) * up_pre).astype(BF16))
        scales.append(jnp.sum(jnp.where(lane == place_in, extra, 0.0), axis=1, keepdims=True))
    for q in range(quarters):
        pieces = []
        for j in range(q * quarter // units, (q + 1) * quarter // units):
            at = 2 * width + j * units
            summed = dot(hidden[0], own_ref[at : at + units, :]) * scales[0]
            pieces.append(summed + dot(hidden[1], other_ref[at : at + units, :]) * scales[1])
        whole = jnp.concatenate(pieces, axis=1).astype(BF16)
        out_ref[:, q] = whole.reshape(chips, cap, quarter)


def mix_body(index_ref, arr_ref, placing_ref, resid_ref, out_hbm, out_ref, sem):
    parts, near_chips, planes, quarters, cap, quarter = arr_ref.shape
    totals = []
    for p in range(parts):
        total = jnp.zeros((planes, cap, quarter), F32)
        for y in range(near_chips):
            for x in range(quarters):
                total = total + arr_ref[p, y, :, x].astype(F32)
        totals.append(total.reshape(planes * cap, quarter))
    picked = dot(placing_ref[...], jnp.concatenate(totals, axis=0).astype(BF16))
    resid = resid_ref[:, :quarter]
    for i in range(1, quarters):
        resid = jnp.where(index_ref[0] == i, resid_ref[:, i * quarter : (i + 1) * quarter], resid)
    out_ref[...] = (resid.astype(F32) + picked).astype(BF16)
    copy = pltpu.make_async_copy(out_ref, out_hbm, sem.at[0])
    copy.start()
    copy.wait()


def shards(
    tokens,
    attn_gain,
    q_down,
    kv_down,
    rope_down,
    q_latent_gain,
    kv_latent_gain,
    q_up,
    query_gain,
    key_up,
    value_up,
    attn_out,
    cache_latent,
    cache_rope,
    lengths,
    moe_gain,
    route,
    route_weight,
    expert_gate,
    expert_up,
    expert_down,
):
    tp_count = lax.axis_size("tp")
    tp_index = lax.axis_index("tp")
    seq_count, width = tokens.shape
    kv_cols = kv_down.shape[1]
    rank = cache_latent.shape[2]
    heads_here = query_gain.shape[0]
    seqs_mine = cache_latent.shape[0]
    index = tp_index.astype(jnp.int32)[None]
    half_dim = rope_down.shape[1] // 2
    each = heads_here * seqs_mine
    chips = lax.axis_size(CHIPS)
    cores = lax.axis_size(CORE)
    chips_in_group = EPG // cores
    slots = chips // chips_in_group * GROUP_CAP
    planes = lax.axis_size(CHIPS[1])
    parts = chips // planes // chips_in_group
    turns = ROPE_BASE ** (-np.arange(half_dim, dtype=np.float32) / np.float32(half_dim))
    turns = turns.astype(np.float32)
    angles = turns[:, None] * np.arange(cache_latent.shape[1], dtype=np.float32)
    cos_table = jnp.asarray(np.cos(angles.astype(np.float64)).astype(np.float32))
    sin_table = jnp.asarray(np.sin(angles.astype(np.float64)).astype(np.float32))
    (
        both, new_rope, cosines, sines, placing, placing_t, packed_weights,
        q_up_t, key_near, q_gain, kv_gain, head_gain, cos_table, sin_table, keys, lens,
    ) = down(
        (
            jax.ShapeDtypeStruct((tp_count, 2 * seq_count, kv_cols), BF16),
            jax.ShapeDtypeStruct((seq_count, rope_down.shape[1]), BF16),
            jax.ShapeDtypeStruct((seq_count, half_dim), F32),
            jax.ShapeDtypeStruct((seq_count, half_dim), F32),
            jax.ShapeDtypeStruct((slots, seq_count), BF16),
            jax.ShapeDtypeStruct((seq_count, slots), BF16),
            jax.ShapeDtypeStruct((slots, EXTRA), BF16),
        ),
        (
            tokens,
            attn_gain[None],
            q_down,
            kv_down,
            rope_down.T,
            lengths[None],
            jnp.asarray(turns[None]),
            route.T,
            route_weight.T,
        ),
        (
            q_up.T,
            key_up,
            q_latent_gain[None],
            kv_latent_gain[None],
            query_gain,
            cos_table,
            sin_table,
            cache_rope,
            lengths[None],
        ),
        parts,
    )
    expert_here = (lax.axis_index(EP) % EPG).astype(jnp.int32)[None]
    quarter_cols = width // tp_count
    both, index, expert_here = lax.optimization_barrier((both, index, expert_here))
    latents = lax.all_to_all(both, "tp", 0, 0, tiled=True)
    send, latent_new, mine_new, cache = run(
        query_body,
        (
            jax.ShapeDtypeStruct((tp_count, each, rank + 2 * half_dim), BF16),
            jax.ShapeDtypeStruct((seq_count, rank), BF16),
            jax.ShapeDtypeStruct((seq_count, kv_cols), BF16),
            jax.ShapeDtypeStruct(cache_latent.shape, BF16),
        ),
        index,
        cache_latent,
        latents,
        q_gain,
        kv_gain,
        q_up_t,
        head_gain,
        key_near,
        cosines,
        sines,
        scalars=1,
        hbm_in=1,
        sems=1,
    )
    queries = lax.all_to_all(send, "tp", 0, 0, tiled=True)
    units = expert_gate.shape[2]
    attended, new_latent, new_rope = run(
        attend_body,
        (
            jax.ShapeDtypeStruct((tp_count, each, rank), BF16),
            jax.ShapeDtypeStruct((seq_count, kv_cols), BF16),
            jax.ShapeDtypeStruct(new_rope.shape, BF16),
        ),
        index,
        queries,
        cache,
        keys,
        cos_table,
        sin_table,
        latent_new,
        mine_new,
        new_rope,
        cosines,
        sines,
        lens,
        scalars=1,
        hbm_out=2,
        sems=2,
    )
    attended, gate, up, lower = lax.optimization_barrier(
        (attended, expert_gate[0], expert_up[0], expert_down[0])
    )
    (own_weights,) = run(
        weights_body,
        (jax.ShapeDtypeStruct((3 * width, units), BF16),),
        gate,
        up,
        lower,
        hbm_in=3,
        sems=2 + width // units,
    )
    swap = [(i, cores - 1 - i) for i in range(cores)]
    other_weights = lax.ppermute(own_weights, CORE, swap)
    attended_heads = lax.all_to_all(attended, "tp", 0, 0, tiled=True)
    (partials,) = run(
        heads_body,
        (jax.ShapeDtypeStruct((tp_count, seq_count, width), BF16),),
        attended_heads,
        value_up,
        attn_out,
    )
    summands = lax.all_to_all(partials, "tp", 0, 0, tiled=True)
    attn_resid, packed = run(
        moe_body,
        (
            jax.ShapeDtypeStruct((seq_count, width), BF16),
            jax.ShapeDtypeStruct(
                (parts, chips_in_group, planes, GROUP_CAP, width + EXTRA), BF16
            ),
        ),
        summands,
        tokens,
        moe_gain[None],
        placing,
        packed_weights,
    )
    packed = packed.reshape(chips, GROUP_CAP, width + EXTRA)
    arrived = lax.all_to_all(packed, CHIPS, 0, 0, tiled=True)
    (sums,) = run(
        experts_body,
        (jax.ShapeDtypeStruct((chips, tp_count, GROUP_CAP, quarter_cols), BF16),),
        expert_here,
        arrived,
        own_weights,
        other_weights,
        flops=100_000_000,
        scalars=1,
    )
    returned = lax.all_to_all(
        sums.reshape(chips * tp_count, GROUP_CAP, quarter_cols), (*CHIPS, "tp"), 0, 0, tiled=True
    ).reshape(parts, chips_in_group, planes, tp_count, GROUP_CAP, quarter_cols)
    (mixed_out,) = run(
        mix_body,
        (jax.ShapeDtypeStruct((seq_count, quarter_cols), BF16),),
        index,
        returned,
        placing_t,
        attn_resid,
        scalars=1,
        hbm_out=1,
        sems=1,
        scratch=(pltpu.VMEM((seq_count, quarter_cols), BF16),),
    )
    return (mixed_out, new_latent, new_rope)


def solution(mesh):
    torus = Mesh(mesh.devices.reshape(8, 8, 2, mesh.shape["tp"]), ("ep_0", "ep_1", "ep_2", "tp"))
    placed = (
        P(EP, None),
        P(),
        P(None, "tp"),
        P(None, "tp"),
        P(),
        P(),
        P(),
        P(None, "tp"),
        P("tp", None),
        P(None, "tp"),
        P(None, "tp"),
        P("tp", None),
        P(EP_TP, None, None),
        P(EP_TP, None, None),
        P(EP),
        P(),
        P(EP, None),
        P(EP, None),
        P(EP, None, "tp"),
        P(EP, None, "tp"),
        P(EP, "tp", None),
    )

    return jax.shard_map(
        shards,
        mesh=torus,
        in_specs=placed,
        out_specs=(P(EP, "tp"), P(EP, "tp"), P(EP, None)),
        check_vma=False,
    )
```

```python
import jax
import jax.numpy as jnp
import numpy as np
from jax import lax
from jax.experimental import pallas as pl
from jax.experimental.pallas import tpu as pltpu
from jax.sharding import Mesh
from jax.sharding import PartitionSpec as P

NOPE = 64
VDIM = 64
QK = 96
EPG = 8
EP = ("ep_0", "ep_1", "ep_2")
CHIPS = ("ep_1", "ep_0")
CORE = "ep_2"
GROUP_CAP = 2
EXTRA = 128
EP_TP = ("ep_0", "ep_1", "ep_2", "tp")


EPS = 1e-06
ROPE_BASE = 10000.0
F32 = jnp.float32
BF16 = jnp.bfloat16
NEG = -1e30


def rms_scaled(values_in, gain_vec):
    values_in = values_in.astype(jnp.float32)
    return (
        values_in
        * lax.rsqrt(jnp.mean(values_in * values_in, axis=-1, keepdims=True) + EPS)
        * gain_vec
    )


def dot(a, b):
    return jnp.dot(a, b, preferred_element_type=F32)


def dot_t(a, b):
    return lax.dot_general(a, b, (((1,), (1,)), ((), ())), preferred_element_type=F32)


def near(array):
    return pltpu.with_memory_space_constraint(array, pltpu.VMEM)


def far(array):
    return pltpu.with_memory_space_constraint(array, pltpu.HBM)


def run(body, outs, *args, flops=2_000_000, scalars=0, hbm_in=0, hbm_out=0, sems=0, scratch=()):
    moved = sum(a.size * a.dtype.itemsize for a in args)
    spaces = [pltpu.SMEM] * scalars + [pltpu.HBM] * hbm_in
    spaces += [pltpu.VMEM] * (len(args) - len(spaces))
    kinds = [pltpu.VMEM] * (len(outs) - hbm_out) + [pltpu.HBM] * hbm_out
    place_in = {pltpu.SMEM: lambda a: a, pltpu.HBM: far, pltpu.VMEM: near}
    return pl.pallas_call(
        body,
        compiler_params=pltpu.CompilerParams(vmem_limit_bytes=16 * 1024 * 1024),
        in_specs=[pl.BlockSpec(memory_space=kind) for kind in spaces],
        out_specs=[pl.BlockSpec(memory_space=kind) for kind in kinds],
        out_shape=[kind(o.shape, o.dtype) for kind, o in zip(kinds, outs)],
        scratch_shapes=[*scratch] + ([pltpu.SemaphoreType.DMA((sems,))] if sems else []),
        cost_estimate=pl.CostEstimate(flops=flops, transcendentals=0, bytes_accessed=moved),
    )(*[place_in[kind](a) for kind, a in zip(spaces, args)])


def place(route_ref, weight_ref, placing_ref, turned_ref, weights_ref, parts):
    topk, rows = route_ref.shape
    slots = placing_ref.shape[0]
    group = route_ref[0:1, :] // EPG
    group = group % parts * (slots // GROUP_CAP // parts) + group // parts
    first = lax.broadcasted_iota(jnp.int32, (rows, rows), 0)
    second = lax.broadcasted_iota(jnp.int32, (rows, rows), 1)
    column = jnp.sum(jnp.where(first == second, group, 0), axis=1, keepdims=True)
    earlier = jnp.where((column == group) & (first < second), 1, 0)
    slot = group * GROUP_CAP + jnp.sum(earlier, axis=0, keepdims=True)
    placing = (lax.broadcasted_iota(jnp.int32, (slots, rows), 0) == slot).astype(BF16)
    placing_ref[...] = placing
    slot_column = jnp.sum(jnp.where(first == second, slot, 0), axis=1, keepdims=True)
    turned_ref[...] = (
        lax.broadcasted_iota(jnp.int32, (rows, slots), 1) == slot_column
    ).astype(BF16)
    lane = lax.broadcasted_iota(jnp.int32, (EXTRA, rows), 0)
    table = jnp.zeros((EXTRA, rows), F32)
    for k in range(topk):
        table = table + jnp.where(route_ref[k : k + 1, :] % EPG == lane, weight_ref[k : k + 1, :], 0.0)
    weights_ref[...] = dot_t(placing, table.astype(BF16)).astype(BF16)


OWN = 9
EARLY = 1
MADE = 7


def down_body(parts, *refs):
    count = (len(refs) - MADE - 1) // 2
    hbm, made, last = refs[:count], refs[count : count + MADE], refs[count + MADE : -1]
    sems = refs[-1]
    near_refs = last[count - OWN :] + last[: count - OWN]
    copies = [
        pltpu.make_async_copy(
            hbm[i] if i < count - 1 else hbm[i].at[: near_refs[i].shape[0]],
            near_refs[i],
            sems.at[i],
        )
        for i in range(count)
    ]
    for copy in copies:
        copy.start()
    tok_ref, gain_ref, q_ref, kv_ref, rope_ref, len_ref, turn_ref, route_ref, weight_ref = near_refs[
        :OWN
    ]
    both_ref, new_rope_ref, cos_ref, sin_ref, placing_ref, turned_ref, weights_ref = made
    copies[0].wait()
    copies[1].wait()
    normed = rms_scaled(tok_ref[...], gain_ref[...]).astype(BF16)
    rows = normed.shape[0]
    copies[2].wait()
    q_part = dot(normed, q_ref[...]).astype(BF16)
    copies[3].wait()
    kv_part = dot(normed, kv_ref[...]).astype(BF16)
    for i in range(both_ref.shape[0]):
        both_ref[i, :rows, :] = q_part
        both_ref[i, rows:, :] = kv_part
    for i in range(4, OWN):
        copies[i].wait()
    new_rope_ref[...] = dot_t(normed, rope_ref[...]).astype(BF16)
    first = lax.broadcasted_iota(jnp.int32, (rows, rows), 0)
    second = lax.broadcasted_iota(jnp.int32, (rows, rows), 1)
    lengths = jnp.sum(jnp.where(first == second, len_ref[...], 0), axis=1, keepdims=True)
    angles = lengths.astype(F32) * turn_ref[...]
    cos_ref[...] = jnp.cos(angles)
    sin_ref[...] = jnp.sin(angles)
    place(route_ref, weight_ref, placing_ref, turned_ref, weights_ref, parts)
    for copy in copies[OWN:]:
        copy.wait()


def down(made, own, others, early, parts):
    args = (*own, *others)
    moved = sum(a.size * a.dtype.itemsize for a in args)
    outs = [pltpu.VMEM(o.shape, o.dtype) for o in (*made, *others[:-1], early)]
    return pl.pallas_call(
        lambda *refs: down_body(parts, *refs),
        compiler_params=pltpu.CompilerParams(vmem_limit_bytes=16 * 1024 * 1024),
        in_specs=[pl.BlockSpec(memory_space=pltpu.HBM)] * len(args),
        out_specs=[pl.BlockSpec(memory_space=pltpu.VMEM)] * len(outs),
        out_shape=outs,
        scratch_shapes=[pltpu.VMEM(a.shape, a.dtype) for a in own]
        + [pltpu.SemaphoreType.DMA((len(args),))],
        cost_estimate=pl.CostEstimate(flops=2_000_000, transcendentals=0, bytes_accessed=moved),
    )(*[far(a) for a in args])


def query_body(
    index_ref, cache_hbm, arr_ref, q_gain_ref, kv_gain_ref, q_up_ref, head_gain_ref, key_up_ref,
    cos_ref, sin_ref, send_ref, latent_ref, mine_ref, cache_ref, sem,
):
    copy = pltpu.make_async_copy(cache_hbm.at[EARLY:], cache_ref, sem.at[0])
    copy.start()
    peers, both, cols = arr_ref.shape
    rows = both // 2
    rank = key_up_ref.shape[0]
    half = cos_ref.shape[1]
    q_raw = jnp.concatenate([arr_ref[i, :rows, :] for i in range(peers)], axis=1)
    kv_raw = jnp.concatenate([arr_ref[i, rows:, :] for i in range(peers)], axis=1)
    latent = rms_scaled(kv_raw, kv_gain_ref[...]).astype(BF16)
    latent_ref[...] = latent
    mine = latent[:, :cols]
    for i in range(1, peers):
        mine = jnp.where(index_ref[0] == i, latent[:, i * cols : (i + 1) * cols], mine)
    mine_ref[...] = mine
    q_lat = rms_scaled(q_raw, q_gain_ref[...]).astype(BF16)
    query = dot_t(q_lat, q_up_ref[...])
    each = rows // peers
    for h in range(head_gain_ref.shape[0]):
        one = rms_scaled(query[:, h * QK : (h + 1) * QK], head_gain_ref[h : h + 1, :])
        lower = one[:, NOPE : NOPE + half]
        upper = one[:, NOPE + half :]
        turned = jnp.concatenate(
            [
                lower * cos_ref[...] - upper * sin_ref[...],
                upper * cos_ref[...] + lower * sin_ref[...],
            ],
            axis=1,
        )
        absorbed = dot_t(one[:, :NOPE].astype(BF16), key_up_ref[:, h * NOPE : (h + 1) * NOPE])
        for i in range(peers):
            at = slice(h * each, (h + 1) * each)
            send_ref[i, at, :rank] = absorbed[i * each : (i + 1) * each].astype(BF16)
            send_ref[i, at, rank:] = turned[i * each : (i + 1) * each].astype(BF16)
    copy.wait()


def attend_body(
    index_ref, arr_ref, first_ref, cache_ref, keys_ref, cos_table_ref, sin_table_ref, latent_ref, mine_ref,
    rope_ref, cos_ref, sin_ref, len_ref, out_ref, latent_out, rope_out, sems,
):
    copies = [
        pltpu.make_async_copy(mine_ref, latent_out, sems.at[0]),
        pltpu.make_async_copy(rope_ref, rope_out, sems.at[1]),
    ]
    for copy in copies:
        copy.start()
    later, places, rank = cache_ref.shape
    seqs = later + EARLY
    caches = [first_ref[s] for s in range(EARLY)] + [cache_ref[s] for s in range(later)]
    peers, each, _ = arr_ref.shape
    rows = peers * each
    half = cos_ref.shape[1]
    arrived = arr_ref[...].reshape(rows, arr_ref.shape[2])
    absorbed = arrived[:, :rank]
    turned = arrived[:, rank:]
    scale = QK ** (-0.5)
    row_seq = lax.broadcasted_iota(jnp.int32, (rows, 1), 0) % seqs
    every = latent_ref.shape[0]
    chosen = lax.broadcasted_iota(jnp.int32, (rows, every), 1) == row_seq + index_ref[0] * seqs
    lengths = jnp.sum(jnp.where(chosen, len_ref[...], 0), axis=1, keepdims=True)
    chosen = chosen.astype(BF16)
    latent = dot(chosen, latent_ref[...])
    lower = rope_ref[:, :half].astype(F32)
    upper = rope_ref[:, half:].astype(F32)
    key_new = jnp.concatenate(
        [
            lower * cos_ref[...] - upper * sin_ref[...],
            upper * cos_ref[...] + lower * sin_ref[...],
        ],
        axis=1,
    )
    key_new = dot(chosen, key_new.astype(BF16))
    self_score = (
        jnp.sum(absorbed.astype(F32) * latent, axis=1, keepdims=True)
        + jnp.sum(turned.astype(F32) * key_new, axis=1, keepdims=True)
    ) * scale
    scores = jnp.zeros((rows, places), F32)
    for s in range(seqs):
        below = keys_ref[s, :half, :].astype(F32)
        above = keys_ref[s, half:, :].astype(F32)
        keys = jnp.concatenate(
            [
                below * cos_table_ref[...] - above * sin_table_ref[...],
                above * cos_table_ref[...] + below * sin_table_ref[...],
            ],
            axis=0,
        ).astype(BF16)
        part = dot_t(absorbed, caches[s]) + dot(turned, keys)
        scores = jnp.where(row_seq == s, part, scores)
    valid = lax.broadcasted_iota(jnp.int32, (rows, places), 1) < lengths
    scores = jnp.where(valid, scores * scale, NEG)
    top = jnp.maximum(jnp.max(scores, axis=1, keepdims=True), self_score)
    weights = jnp.where(valid, jnp.exp(scores - top), 0.0)
    self_weight = jnp.exp(self_score - top)
    total = jnp.sum(weights, axis=1, keepdims=True) + self_weight
    summed = self_weight.astype(BF16).astype(F32) * latent
    for s in range(seqs):
        summed = summed + dot(jnp.where(row_seq == s, weights, 0.0).astype(BF16), caches[s])
    out_ref[...] = (summed / total).astype(BF16).reshape(out_ref.shape)
    for copy in copies:
        copy.wait()


def weights_body(gate_hbm, up_hbm, down_hbm, out_ref, sems):
    width, units = gate_hbm.shape
    copies = [
        pltpu.make_async_copy(gate_hbm, out_ref.at[:width], sems.at[0]),
        pltpu.make_async_copy(up_hbm, out_ref.at[width : 2 * width], sems.at[1]),
    ]
    for j in range(width // units):
        at = 2 * width + j * units
        copies.append(
            pltpu.make_async_copy(
                down_hbm.at[:, j * units : (j + 1) * units],
                out_ref.at[at : at + units],
                sems.at[2 + j],
            )
        )
    for copy in copies:
        copy.start()
    for copy in copies:
        copy.wait()


def moe_body(arr_ref, tok_ref, gain_ref, placing_ref, weights_ref, resid_ref, out_ref):
    head_sum = arr_ref[0].astype(F32)
    for i in range(1, arr_ref.shape[0]):
        head_sum = head_sum + arr_ref[i].astype(F32)
    resid = (tok_ref[...].astype(F32) + head_sum).astype(BF16)
    resid_ref[...] = resid
    width = resid.shape[1]
    moe_input = rms_scaled(resid, gain_ref[...]).astype(BF16)
    parts, copies, planes, cap, _ = out_ref.shape
    rows = dot(placing_ref[...], moe_input).astype(BF16)
    for p in range(parts):
        at = slice(p * planes * cap, (p + 1) * planes * cap)
        main = rows[at].reshape(planes, cap, width)
        side = weights_ref[at, :].reshape(planes, cap, EXTRA)
        for i in range(copies):
            out_ref[p, i, :, :, :width] = main
            out_ref[p, i, :, :, width:] = side


def heads_body(arr_ref, value_ref, out_w_ref, out_ref):
    peers, each, rank = arr_ref.shape
    rows = peers * each
    heads = value_ref.shape[1] // VDIM
    seqs = each // heads
    values = dot(arr_ref[...].reshape(rows, rank), value_ref[...]).astype(BF16)
    to = lax.broadcasted_iota(jnp.int32, (rows // heads, rows), 0)
    at = lax.broadcasted_iota(jnp.int32, (rows // heads, rows), 1)
    column = lax.broadcasted_iota(jnp.int32, (rows // heads, heads * VDIM), 1)
    picked = jnp.zeros((rows // heads, heads * VDIM), F32)
    for h in range(heads):
        chosen = (at == (to // seqs) * each + h * seqs + to % seqs).astype(BF16)
        picked = jnp.where(column // VDIM == h, dot(chosen, values), picked)
    partial = dot(picked.astype(BF16), out_w_ref[...]).astype(BF16)
    for i in range(out_ref.shape[0]):
        out_ref[i] = partial


def experts_body(index_ref, rows_ref, own_ref, other_ref, out_ref):
    chips, quarters, cap, quarter = out_ref.shape
    width = quarters * quarter
    units = own_ref.shape[1]
    inside = rows_ref[:, :, :width].reshape(chips * cap, width)
    extra = rows_ref[:, :, width:].reshape(chips * cap, EXTRA).astype(F32)
    lane = lax.broadcasted_iota(jnp.int32, extra.shape, 1)
    here = index_ref[0]
    there = here + 1 - 2 * (here % 2)
    hidden, scales = [], []
    for weights_ref, place_in in ((own_ref, here), (other_ref, there)):
        gate_pre = dot(inside, weights_ref[:width, :])
        up_pre = dot(inside, weights_ref[width : 2 * width, :])
        hidden.append((gate_pre / (1.0 + jnp.exp(-gate_pre)) * up_pre).astype(BF16))
        scales.append(jnp.sum(jnp.where(lane == place_in, extra, 0.0), axis=1, keepdims=True))
    for q in range(quarters):
        pieces = []
        for j in range(q * quarter // units, (q + 1) * quarter // units):
            at = 2 * width + j * units
            summed = dot(hidden[0], own_ref[at : at + units, :]) * scales[0]
            pieces.append(summed + dot(hidden[1], other_ref[at : at + units, :]) * scales[1])
        whole = jnp.concatenate(pieces, axis=1).astype(BF16)
        out_ref[:, q] = whole.reshape(chips, cap, quarter)


def mix_body(index_ref, arr_ref, placing_ref, resid_ref, out_hbm, out_ref, sem):
    parts, near_chips, planes, quarters, cap, quarter = arr_ref.shape
    totals = []
    for p in range(parts):
        total = jnp.zeros((planes, cap, quarter), F32)
        for y in range(near_chips):
            for x in range(quarters):
                total = total + arr_ref[p, y, :, x].astype(F32)
        totals.append(total.reshape(planes * cap, quarter))
    picked = dot(placing_ref[...], jnp.concatenate(totals, axis=0).astype(BF16))
    resid = resid_ref[:, :quarter]
    for i in range(1, quarters):
        resid = jnp.where(index_ref[0] == i, resid_ref[:, i * quarter : (i + 1) * quarter], resid)
    out_ref[...] = (resid.astype(F32) + picked).astype(BF16)
    copy = pltpu.make_async_copy(out_ref, out_hbm, sem.at[0])
    copy.start()
    copy.wait()


def shards(
    tokens,
    attn_gain,
    q_down,
    kv_down,
    rope_down,
    q_latent_gain,
    kv_latent_gain,
    q_up,
    query_gain,
    key_up,
    value_up,
    attn_out,
    cache_latent,
    cache_rope,
    lengths,
    moe_gain,
    route,
    route_weight,
    expert_gate,
    expert_up,
    expert_down,
):
    tp_count = lax.axis_size("tp")
    tp_index = lax.axis_index("tp")
    seq_count, width = tokens.shape
    kv_cols = kv_down.shape[1]
    rank = cache_latent.shape[2]
    heads_here = query_gain.shape[0]
    seqs_mine = cache_latent.shape[0]
    index = tp_index.astype(jnp.int32)[None]
    half_dim = rope_down.shape[1] // 2
    each = heads_here * seqs_mine
    chips = lax.axis_size(CHIPS)
    cores = lax.axis_size(CORE)
    chips_in_group = EPG // cores
    slots = chips // chips_in_group * GROUP_CAP
    planes = lax.axis_size(CHIPS[1])
    parts = chips // planes // chips_in_group
    turns = ROPE_BASE ** (-np.arange(half_dim, dtype=np.float32) / np.float32(half_dim))
    turns = turns.astype(np.float32)
    angles = turns[:, None] * np.arange(cache_latent.shape[1], dtype=np.float32)
    cos_table = jnp.asarray(np.cos(angles.astype(np.float64)).astype(np.float32))
    sin_table = jnp.asarray(np.sin(angles.astype(np.float64)).astype(np.float32))
    (
        both, new_rope, cosines, sines, placing, placing_t, packed_weights,
        q_up_t, key_near, q_gain, kv_gain, head_gain, cos_table, sin_table, keys, lens, cache_first,
    ) = down(
        (
            jax.ShapeDtypeStruct((tp_count, 2 * seq_count, kv_cols), BF16),
            jax.ShapeDtypeStruct((seq_count, rope_down.shape[1]), BF16),
            jax.ShapeDtypeStruct((seq_count, half_dim), F32),
            jax.ShapeDtypeStruct((seq_count, half_dim), F32),
            jax.ShapeDtypeStruct((slots, seq_count), BF16),
            jax.ShapeDtypeStruct((seq_count, slots), BF16),
            jax.ShapeDtypeStruct((slots, EXTRA), BF16),
        ),
        (
            tokens,
            attn_gain[None],
            q_down,
            kv_down,
            rope_down.T,
            lengths[None],
            jnp.asarray(turns[None]),
            route.T,
            route_weight.T,
        ),
        (
            q_up.T,
            key_up,
            q_latent_gain[None],
            kv_latent_gain[None],
            query_gain,
            cos_table,
            sin_table,
            cache_rope,
            lengths[None],
            cache_latent,
        ),
        jax.ShapeDtypeStruct((EARLY, *cache_latent.shape[1:]), BF16),
        parts,
    )
    expert_here = (lax.axis_index(EP) % EPG).astype(jnp.int32)[None]
    quarter_cols = width // tp_count
    both, index, expert_here = lax.optimization_barrier((both, index, expert_here))
    latents = lax.all_to_all(both, "tp", 0, 0, tiled=True)
    send, latent_new, mine_new, cache = run(
        query_body,
        (
            jax.ShapeDtypeStruct((tp_count, each, rank + 2 * half_dim), BF16),
            jax.ShapeDtypeStruct((seq_count, rank), BF16),
            jax.ShapeDtypeStruct((seq_count, kv_cols), BF16),
            jax.ShapeDtypeStruct((seqs_mine - EARLY, *cache_latent.shape[1:]), BF16),
        ),
        index,
        cache_latent,
        latents,
        q_gain,
        kv_gain,
        q_up_t,
        head_gain,
        key_near,
        cosines,
        sines,
        scalars=1,
        hbm_in=1,
        sems=1,
    )
    queries = lax.all_to_all(send, "tp", 0, 0, tiled=True)
    units = expert_gate.shape[2]
    attended, new_latent, new_rope = run(
        attend_body,
        (
            jax.ShapeDtypeStruct((tp_count, each, rank), BF16),
            jax.ShapeDtypeStruct((seq_count, kv_cols), BF16),
            jax.ShapeDtypeStruct(new_rope.shape, BF16),
        ),
        index,
        queries,
        cache_first,
        cache,
        keys,
        cos_table,
        sin_table,
        latent_new,
        mine_new,
        new_rope,
        cosines,
        sines,
        lens,
        scalars=1,
        hbm_out=2,
        sems=2,
    )
    attended_heads = lax.all_to_all(attended, "tp", 0, 0, tiled=True)
    (partials,) = run(
        heads_body,
        (jax.ShapeDtypeStruct((tp_count, seq_count, width), BF16),),
        attended_heads,
        value_up,
        attn_out,
    )
    summands = lax.all_to_all(partials, "tp", 0, 0, tiled=True)
    attn_resid, packed = run(
        moe_body,
        (
            jax.ShapeDtypeStruct((seq_count, width), BF16),
            jax.ShapeDtypeStruct(
                (parts, chips_in_group, planes, GROUP_CAP, width + EXTRA), BF16
            ),
        ),
        summands,
        tokens,
        moe_gain[None],
        placing,
        packed_weights,
    )
    packed = packed.reshape(chips, GROUP_CAP, width + EXTRA)
    packed, gate, up, lower = lax.optimization_barrier(
        (packed, expert_gate[0], expert_up[0], expert_down[0])
    )
    (own_weights,) = run(
        weights_body,
        (jax.ShapeDtypeStruct((3 * width, units), BF16),),
        gate,
        up,
        lower,
        hbm_in=3,
        sems=2 + width // units,
    )
    swap = [(i, cores - 1 - i) for i in range(cores)]
    other_weights = lax.ppermute(own_weights, CORE, swap)
    arrived = lax.all_to_all(packed, CHIPS, 0, 0, tiled=True)
    (sums,) = run(
        experts_body,
        (jax.ShapeDtypeStruct((chips, tp_count, GROUP_CAP, quarter_cols), BF16),),
        expert_here,
        arrived,
        own_weights,
        other_weights,
        flops=100_000_000,
        scalars=1,
    )
    returned = lax.all_to_all(
        sums.reshape(chips * tp_count, GROUP_CAP, quarter_cols), (*CHIPS, "tp"), 0, 0, tiled=True
    ).reshape(parts, chips_in_group, planes, tp_count, GROUP_CAP, quarter_cols)
    (mixed_out,) = run(
        mix_body,
        (jax.ShapeDtypeStruct((seq_count, quarter_cols), BF16),),
        index,
        returned,
        placing_t,
        attn_resid,
        scalars=1,
        hbm_out=1,
        sems=1,
        scratch=(pltpu.VMEM((seq_count, quarter_cols), BF16),),
    )
    return (mixed_out, new_latent, new_rope)


def solution(mesh):
    torus = Mesh(mesh.devices.reshape(8, 8, 2, mesh.shape["tp"]), ("ep_0", "ep_1", "ep_2", "tp"))
    placed = (
        P(EP, None),
        P(),
        P(None, "tp"),
        P(None, "tp"),
        P(),
        P(),
        P(),
        P(None, "tp"),
        P("tp", None),
        P(None, "tp"),
        P(None, "tp"),
        P("tp", None),
        P(EP_TP, None, None),
        P(EP_TP, None, None),
        P(EP),
        P(),
        P(EP, None),
        P(EP, None),
        P(EP, None, "tp"),
        P(EP, None, "tp"),
        P(EP, "tp", None),
    )

    return jax.shard_map(
        shards,
        mesh=torus,
        in_specs=placed,
        out_specs=(P(EP, "tp"), P(EP, "tp"), P(EP, None)),
        check_vma=False,
    )
```

```python
import jax
import jax.numpy as jnp
import numpy as np
from jax import lax
from jax.experimental import pallas as pl
from jax.experimental.pallas import tpu as pltpu
from jax.sharding import Mesh
from jax.sharding import PartitionSpec as P

NOPE = 64
VDIM = 64
QK = 96
EPG = 8
EP = ("ep_0", "ep_1", "ep_2")
CHIPS = ("ep_1", "ep_0")
CORE = "ep_2"
GROUP_CAP = 2
EXTRA = 128
EP_TP = ("ep_0", "ep_1", "ep_2", "tp")


EPS = 1e-06
ROPE_BASE = 10000.0
F32 = jnp.float32
BF16 = jnp.bfloat16
NEG = -1e30


def rms_scaled(values_in, gain_vec):
    values_in = values_in.astype(jnp.float32)
    return (
        values_in
        * lax.rsqrt(jnp.mean(values_in * values_in, axis=-1, keepdims=True) + EPS)
        * gain_vec
    )


def dot(a, b):
    return jnp.dot(a, b, preferred_element_type=F32)


def dot_t(a, b):
    return lax.dot_general(a, b, (((1,), (1,)), ((), ())), preferred_element_type=F32)


def near(array):
    return pltpu.with_memory_space_constraint(array, pltpu.VMEM)


def far(array):
    return pltpu.with_memory_space_constraint(array, pltpu.HBM)


def run(body, outs, *args, flops=2_000_000, scalars=0, hbm_in=0, hbm_out=0, sems=0, scratch=()):
    moved = sum(a.size * a.dtype.itemsize for a in args)
    spaces = [pltpu.SMEM] * scalars + [pltpu.HBM] * hbm_in
    spaces += [pltpu.VMEM] * (len(args) - len(spaces))
    kinds = [pltpu.VMEM] * (len(outs) - hbm_out) + [pltpu.HBM] * hbm_out
    place_in = {pltpu.SMEM: lambda a: a, pltpu.HBM: far, pltpu.VMEM: near}
    return pl.pallas_call(
        body,
        compiler_params=pltpu.CompilerParams(vmem_limit_bytes=16 * 1024 * 1024),
        in_specs=[pl.BlockSpec(memory_space=kind) for kind in spaces],
        out_specs=[pl.BlockSpec(memory_space=kind) for kind in kinds],
        out_shape=[kind(o.shape, o.dtype) for kind, o in zip(kinds, outs)],
        scratch_shapes=[*scratch] + ([pltpu.SemaphoreType.DMA((sems,))] if sems else []),
        cost_estimate=pl.CostEstimate(flops=flops, transcendentals=0, bytes_accessed=moved),
    )(*[place_in[kind](a) for kind, a in zip(spaces, args)])


def place(route_ref, weight_ref, placing_ref, turned_ref, weights_ref, parts):
    topk, rows = route_ref.shape
    slots = placing_ref.shape[0]
    group = route_ref[0:1, :] // EPG
    group = group % parts * (slots // GROUP_CAP // parts) + group // parts
    first = lax.broadcasted_iota(jnp.int32, (rows, rows), 0)
    second = lax.broadcasted_iota(jnp.int32, (rows, rows), 1)
    column = jnp.sum(jnp.where(first == second, group, 0), axis=1, keepdims=True)
    earlier = jnp.where((column == group) & (first < second), 1, 0)
    slot = group * GROUP_CAP + jnp.sum(earlier, axis=0, keepdims=True)
    placing = (lax.broadcasted_iota(jnp.int32, (slots, rows), 0) == slot).astype(BF16)
    placing_ref[...] = placing
    slot_column = jnp.sum(jnp.where(first == second, slot, 0), axis=1, keepdims=True)
    turned_ref[...] = (
        lax.broadcasted_iota(jnp.int32, (rows, slots), 1) == slot_column
    ).astype(BF16)
    lane = lax.broadcasted_iota(jnp.int32, (EXTRA, rows), 0)
    table = jnp.zeros((EXTRA, rows), F32)
    for k in range(topk):
        table = table + jnp.where(route_ref[k : k + 1, :] % EPG == lane, weight_ref[k : k + 1, :], 0.0)
    weights_ref[...] = dot_t(placing, table.astype(BF16)).astype(BF16)


OWN = 9
MADE = 7


def down_body(parts, *refs):
    count = (len(refs) - MADE - 1) // 2
    hbm, made, last = refs[:count], refs[count : count + MADE], refs[count + MADE : -1]
    sems = refs[-1]
    near_refs = last[count - OWN :] + last[: count - OWN]
    copies = [pltpu.make_async_copy(hbm[i], near_refs[i], sems.at[i]) for i in range(count)]
    for i in (2, 3, 0, 1, *range(4, count)):
        copies[i].start()
    tok_ref, gain_ref, q_ref, kv_ref, rope_ref, len_ref, turn_ref, route_ref, weight_ref = near_refs[
        :OWN
    ]
    both_ref, new_rope_ref, cos_ref, sin_ref, placing_ref, turned_ref, weights_ref = made
    copies[0].wait()
    copies[1].wait()
    normed = rms_scaled(tok_ref[...], gain_ref[...]).astype(BF16)
    rows = normed.shape[0]
    copies[2].wait()
    q_part = dot(normed, q_ref[...]).astype(BF16)
    copies[3].wait()
    kv_part = dot(normed, kv_ref[...]).astype(BF16)
    for i in range(both_ref.shape[0]):
        both_ref[i, :rows, :] = q_part
        both_ref[i, rows:, :] = kv_part
    for i in range(4, OWN):
        copies[i].wait()
    new_rope_ref[...] = dot_t(normed, rope_ref[...]).astype(BF16)
    first = lax.broadcasted_iota(jnp.int32, (rows, rows), 0)
    second = lax.broadcasted_iota(jnp.int32, (rows, rows), 1)
    lengths = jnp.sum(jnp.where(first == second, len_ref[...], 0), axis=1, keepdims=True)
    angles = lengths.astype(F32) * turn_ref[...]
    cos_ref[...] = jnp.cos(angles)
    sin_ref[...] = jnp.sin(angles)
    place(route_ref, weight_ref, placing_ref, turned_ref, weights_ref, parts)
    for copy in copies[OWN:]:
        copy.wait()


def down(made, own, others, parts):
    args = (*own, *others)
    moved = sum(a.size * a.dtype.itemsize for a in args)
    outs = [pltpu.VMEM(o.shape, o.dtype) for o in (*made, *others)]
    return pl.pallas_call(
        lambda *refs: down_body(parts, *refs),
        compiler_params=pltpu.CompilerParams(vmem_limit_bytes=16 * 1024 * 1024),
        in_specs=[pl.BlockSpec(memory_space=pltpu.HBM)] * len(args),
        out_specs=[pl.BlockSpec(memory_space=pltpu.VMEM)] * len(outs),
        out_shape=outs,
        scratch_shapes=[pltpu.VMEM(a.shape, a.dtype) for a in own]
        + [pltpu.SemaphoreType.DMA((len(args),))],
        cost_estimate=pl.CostEstimate(flops=2_000_000, transcendentals=0, bytes_accessed=moved),
    )(*[far(a) for a in args])


def query_body(
    index_ref, cache_hbm, arr_ref, q_gain_ref, kv_gain_ref, q_up_ref, head_gain_ref, key_up_ref,
    cos_ref, sin_ref, send_ref, latent_ref, mine_ref, cache_ref, sem,
):
    copy = pltpu.make_async_copy(cache_hbm, cache_ref, sem.at[0])
    copy.start()
    peers, both, cols = arr_ref.shape
    rows = both // 2
    rank = key_up_ref.shape[0]
    half = cos_ref.shape[1]
    q_raw = jnp.concatenate([arr_ref[i, :rows, :] for i in range(peers)], axis=1)
    kv_raw = jnp.concatenate([arr_ref[i, rows:, :] for i in range(peers)], axis=1)
    latent = rms_scaled(kv_raw, kv_gain_ref[...]).astype(BF16)
    latent_ref[...] = latent
    mine = latent[:, :cols]
    for i in range(1, peers):
        mine = jnp.where(index_ref[0] == i, latent[:, i * cols : (i + 1) * cols], mine)
    mine_ref[...] = mine
    q_lat = rms_scaled(q_raw, q_gain_ref[...]).astype(BF16)
    query = dot_t(q_lat, q_up_ref[...])
    each = rows // peers
    for h in range(head_gain_ref.shape[0]):
        one = rms_scaled(query[:, h * QK : (h + 1) * QK], head_gain_ref[h : h + 1, :])
        lower = one[:, NOPE : NOPE + half]
        upper = one[:, NOPE + half :]
        turned = jnp.concatenate(
            [
                lower * cos_ref[...] - upper * sin_ref[...],
                upper * cos_ref[...] + lower * sin_ref[...],
            ],
            axis=1,
        )
        absorbed = dot_t(one[:, :NOPE].astype(BF16), key_up_ref[:, h * NOPE : (h + 1) * NOPE])
        for i in range(peers):
            at = slice(h * each, (h + 1) * each)
            send_ref[i, at, :rank] = absorbed[i * each : (i + 1) * each].astype(BF16)
            send_ref[i, at, rank:] = turned[i * each : (i + 1) * each].astype(BF16)
    copy.wait()


def attend_body(
    index_ref, arr_ref, cache_ref, keys_ref, cos_table_ref, sin_table_ref, latent_ref, mine_ref,
    rope_ref, cos_ref, sin_ref, len_ref, out_ref, latent_out, rope_out, sems,
):
    copies = [
        pltpu.make_async_copy(mine_ref, latent_out, sems.at[0]),
        pltpu.make_async_copy(rope_ref, rope_out, sems.at[1]),
    ]
    for copy in copies:
        copy.start()
    seqs, places, rank = cache_ref.shape
    peers, each, _ = arr_ref.shape
    rows = peers * each
    half = cos_ref.shape[1]
    arrived = arr_ref[...].reshape(rows, arr_ref.shape[2])
    absorbed = arrived[:, :rank]
    turned = arrived[:, rank:]
    scale = QK ** (-0.5)
    row_seq = lax.broadcasted_iota(jnp.int32, (rows, 1), 0) % seqs
    every = latent_ref.shape[0]
    chosen = lax.broadcasted_iota(jnp.int32, (rows, every), 1) == row_seq + index_ref[0] * seqs
    lengths = jnp.sum(jnp.where(chosen, len_ref[...], 0), axis=1, keepdims=True)
    chosen = chosen.astype(BF16)
    latent = dot(chosen, latent_ref[...])
    lower = rope_ref[:, :half].astype(F32)
    upper = rope_ref[:, half:].astype(F32)
    key_new = jnp.concatenate(
        [
            lower * cos_ref[...] - upper * sin_ref[...],
            upper * cos_ref[...] + lower * sin_ref[...],
        ],
        axis=1,
    )
    key_new = dot(chosen, key_new.astype(BF16))
    self_score = (
        jnp.sum(absorbed.astype(F32) * latent, axis=1, keepdims=True)
        + jnp.sum(turned.astype(F32) * key_new, axis=1, keepdims=True)
    ) * scale
    scores = jnp.zeros((rows, places), F32)
    for s in range(seqs):
        below = keys_ref[s, :half, :].astype(F32)
        above = keys_ref[s, half:, :].astype(F32)
        keys = jnp.concatenate(
            [
                below * cos_table_ref[...] - above * sin_table_ref[...],
                above * cos_table_ref[...] + below * sin_table_ref[...],
            ],
            axis=0,
        ).astype(BF16)
        part = dot_t(absorbed, cache_ref[s]) + dot(turned, keys)
        scores = jnp.where(row_seq == s, part, scores)
    valid = lax.broadcasted_iota(jnp.int32, (rows, places), 1) < lengths
    scores = jnp.where(valid, scores * scale, NEG)
    top = jnp.maximum(jnp.max(scores, axis=1, keepdims=True), self_score)
    weights = jnp.where(valid, jnp.exp(scores - top), 0.0)
    self_weight = jnp.exp(self_score - top)
    total = jnp.sum(weights, axis=1, keepdims=True) + self_weight
    summed = self_weight.astype(BF16).astype(F32) * latent
    for s in range(seqs):
        summed = summed + dot(jnp.where(row_seq == s, weights, 0.0).astype(BF16), cache_ref[s])
    out_ref[...] = (summed / total).astype(BF16).reshape(out_ref.shape)
    for copy in copies:
        copy.wait()


def weights_body(gate_hbm, up_hbm, down_hbm, out_ref, sems):
    width, units = gate_hbm.shape
    copies = [
        pltpu.make_async_copy(gate_hbm, out_ref.at[:width], sems.at[0]),
        pltpu.make_async_copy(up_hbm, out_ref.at[width : 2 * width], sems.at[1]),
    ]
    for j in range(width // units):
        at = 2 * width + j * units
        copies.append(
            pltpu.make_async_copy(
                down_hbm.at[:, j * units : (j + 1) * units],
                out_ref.at[at : at + units],
                sems.at[2 + j],
            )
        )
    for copy in copies:
        copy.start()
    for copy in copies:
        copy.wait()


def moe_body(arr_ref, tok_ref, gain_ref, placing_ref, weights_ref, resid_ref, out_ref):
    head_sum = arr_ref[0].astype(F32)
    for i in range(1, arr_ref.shape[0]):
        head_sum = head_sum + arr_ref[i].astype(F32)
    resid = (tok_ref[...].astype(F32) + head_sum).astype(BF16)
    resid_ref[...] = resid
    width = resid.shape[1]
    moe_input = rms_scaled(resid, gain_ref[...]).astype(BF16)
    parts, copies, planes, cap, _ = out_ref.shape
    rows = dot(placing_ref[...], moe_input).astype(BF16)
    for p in range(parts):
        at = slice(p * planes * cap, (p + 1) * planes * cap)
        main = rows[at].reshape(planes, cap, width)
        side = weights_ref[at, :].reshape(planes, cap, EXTRA)
        for i in range(copies):
            out_ref[p, i, :, :, :width] = main
            out_ref[p, i, :, :, width:] = side


def heads_body(arr_ref, value_ref, out_w_ref, out_ref):
    peers, each, rank = arr_ref.shape
    rows = peers * each
    heads = value_ref.shape[1] // VDIM
    seqs = each // heads
    values = dot(arr_ref[...].reshape(rows, rank), value_ref[...]).astype(BF16)
    to = lax.broadcasted_iota(jnp.int32, (rows // heads, rows), 0)
    at = lax.broadcasted_iota(jnp.int32, (rows // heads, rows), 1)
    column = lax.broadcasted_iota(jnp.int32, (rows // heads, heads * VDIM), 1)
    picked = jnp.zeros((rows // heads, heads * VDIM), F32)
    for h in range(heads):
        chosen = (at == (to // seqs) * each + h * seqs + to % seqs).astype(BF16)
        picked = jnp.where(column // VDIM == h, dot(chosen, values), picked)
    partial = dot(picked.astype(BF16), out_w_ref[...]).astype(BF16)
    for i in range(out_ref.shape[0]):
        out_ref[i] = partial


def experts_body(index_ref, rows_ref, own_ref, other_ref, out_ref):
    chips, quarters, cap, quarter = out_ref.shape
    width = quarters * quarter
    units = own_ref.shape[1]
    inside = rows_ref[:, :, :width].reshape(chips * cap, width)
    extra = rows_ref[:, :, width:].reshape(chips * cap, EXTRA).astype(F32)
    lane = lax.broadcasted_iota(jnp.int32, extra.shape, 1)
    here = index_ref[0]
    there = here + 1 - 2 * (here % 2)
    hidden, scales = [], []
    for weights_ref, place_in in ((own_ref, here), (other_ref, there)):
        gate_pre = dot(inside, weights_ref[:width, :])
        up_pre = dot(inside, weights_ref[width : 2 * width, :])
        hidden.append((gate_pre / (1.0 + jnp.exp(-gate_pre)) * up_pre).astype(BF16))
        scales.append(jnp.sum(jnp.where(lane == place_in, extra, 0.0), axis=1, keepdims=True))
    for q in range(quarters):
        pieces = []
        for j in range(q * quarter // units, (q + 1) * quarter // units):
            at = 2 * width + j * units
            summed = dot(hidden[0], own_ref[at : at + units, :]) * scales[0]
            pieces.append(summed + dot(hidden[1], other_ref[at : at + units, :]) * scales[1])
        whole = jnp.concatenate(pieces, axis=1).astype(BF16)
        out_ref[:, q] = whole.reshape(chips, cap, quarter)


def mix_body(index_ref, arr_ref, placing_ref, resid_ref, out_hbm, out_ref, sem):
    parts, near_chips, planes, quarters, cap, quarter = arr_ref.shape
    totals = []
    for p in range(parts):
        total = jnp.zeros((planes, cap, quarter), F32)
        for y in range(near_chips):
            for x in range(quarters):
                total = total + arr_ref[p, y, :, x].astype(F32)
        totals.append(total.reshape(planes * cap, quarter))
    picked = dot(placing_ref[...], jnp.concatenate(totals, axis=0).astype(BF16))
    resid = resid_ref[:, :quarter]
    for i in range(1, quarters):
        resid = jnp.where(index_ref[0] == i, resid_ref[:, i * quarter : (i + 1) * quarter], resid)
    out_ref[...] = (resid.astype(F32) + picked).astype(BF16)
    copy = pltpu.make_async_copy(out_ref, out_hbm, sem.at[0])
    copy.start()
    copy.wait()


def shards(
    tokens,
    attn_gain,
    q_down,
    kv_down,
    rope_down,
    q_latent_gain,
    kv_latent_gain,
    q_up,
    query_gain,
    key_up,
    value_up,
    attn_out,
    cache_latent,
    cache_rope,
    lengths,
    moe_gain,
    route,
    route_weight,
    expert_gate,
    expert_up,
    expert_down,
):
    tp_count = lax.axis_size("tp")
    tp_index = lax.axis_index("tp")
    seq_count, width = tokens.shape
    kv_cols = kv_down.shape[1]
    rank = cache_latent.shape[2]
    heads_here = query_gain.shape[0]
    seqs_mine = cache_latent.shape[0]
    index = tp_index.astype(jnp.int32)[None]
    half_dim = rope_down.shape[1] // 2
    each = heads_here * seqs_mine
    chips = lax.axis_size(CHIPS)
    cores = lax.axis_size(CORE)
    chips_in_group = EPG // cores
    slots = chips // chips_in_group * GROUP_CAP
    planes = lax.axis_size(CHIPS[1])
    parts = chips // planes // chips_in_group
    turns = ROPE_BASE ** (-np.arange(half_dim, dtype=np.float32) / np.float32(half_dim))
    turns = turns.astype(np.float32)
    angles = turns[:, None] * np.arange(cache_latent.shape[1], dtype=np.float32)
    cos_table = jnp.asarray(np.cos(angles.astype(np.float64)).astype(np.float32))
    sin_table = jnp.asarray(np.sin(angles.astype(np.float64)).astype(np.float32))
    (
        both, new_rope, cosines, sines, placing, placing_t, packed_weights,
        q_up_t, key_near, q_gain, kv_gain, head_gain, cos_table, sin_table, keys, lens,
    ) = down(
        (
            jax.ShapeDtypeStruct((tp_count, 2 * seq_count, kv_cols), BF16),
            jax.ShapeDtypeStruct((seq_count, rope_down.shape[1]), BF16),
            jax.ShapeDtypeStruct((seq_count, half_dim), F32),
            jax.ShapeDtypeStruct((seq_count, half_dim), F32),
            jax.ShapeDtypeStruct((slots, seq_count), BF16),
            jax.ShapeDtypeStruct((seq_count, slots), BF16),
            jax.ShapeDtypeStruct((slots, EXTRA), BF16),
        ),
        (
            tokens,
            attn_gain[None],
            q_down,
            kv_down,
            rope_down.T,
            lengths[None],
            jnp.asarray(turns[None]),
            route.T,
            route_weight.T,
        ),
        (
            q_up.T,
            key_up,
            q_latent_gain[None],
            kv_latent_gain[None],
            query_gain,
            cos_table,
            sin_table,
            cache_rope,
            lengths[None],
        ),
        parts,
    )
    expert_here = (lax.axis_index(EP) % EPG).astype(jnp.int32)[None]
    quarter_cols = width // tp_count
    both, index, expert_here = lax.optimization_barrier((both, index, expert_here))
    latents = lax.all_to_all(both, "tp", 0, 0, tiled=True)
    send, latent_new, mine_new, cache = run(
        query_body,
        (
            jax.ShapeDtypeStruct((tp_count, each, rank + 2 * half_dim), BF16),
            jax.ShapeDtypeStruct((seq_count, rank), BF16),
            jax.ShapeDtypeStruct((seq_count, kv_cols), BF16),
            jax.ShapeDtypeStruct(cache_latent.shape, BF16),
        ),
        index,
        cache_latent,
        latents,
        q_gain,
        kv_gain,
        q_up_t,
        head_gain,
        key_near,
        cosines,
        sines,
        scalars=1,
        hbm_in=1,
        sems=1,
    )
    queries = lax.all_to_all(send, "tp", 0, 0, tiled=True)
    units = expert_gate.shape[2]
    attended, new_latent, new_rope = run(
        attend_body,
        (
            jax.ShapeDtypeStruct((tp_count, each, rank), BF16),
            jax.ShapeDtypeStruct((seq_count, kv_cols), BF16),
            jax.ShapeDtypeStruct(new_rope.shape, BF16),
        ),
        index,
        queries,
        cache,
        keys,
        cos_table,
        sin_table,
        latent_new,
        mine_new,
        new_rope,
        cosines,
        sines,
        lens,
        scalars=1,
        hbm_out=2,
        sems=2,
    )
    attended_heads = lax.all_to_all(attended, "tp", 0, 0, tiled=True)
    (partials,) = run(
        heads_body,
        (jax.ShapeDtypeStruct((tp_count, seq_count, width), BF16),),
        attended_heads,
        value_up,
        attn_out,
    )
    summands = lax.all_to_all(partials, "tp", 0, 0, tiled=True)
    attn_resid, packed = run(
        moe_body,
        (
            jax.ShapeDtypeStruct((seq_count, width), BF16),
            jax.ShapeDtypeStruct(
                (parts, chips_in_group, planes, GROUP_CAP, width + EXTRA), BF16
            ),
        ),
        summands,
        tokens,
        moe_gain[None],
        placing,
        packed_weights,
    )
    packed = packed.reshape(chips, GROUP_CAP, width + EXTRA)
    packed, gate, up, lower = lax.optimization_barrier(
        (packed, expert_gate[0], expert_up[0], expert_down[0])
    )
    (own_weights,) = run(
        weights_body,
        (jax.ShapeDtypeStruct((3 * width, units), BF16),),
        gate,
        up,
        lower,
        hbm_in=3,
        sems=2 + width // units,
    )
    swap = [(i, cores - 1 - i) for i in range(cores)]
    other_weights = lax.ppermute(own_weights, CORE, swap)
    arrived = lax.all_to_all(packed, CHIPS, 0, 0, tiled=True)
    (sums,) = run(
        experts_body,
        (jax.ShapeDtypeStruct((chips, tp_count, GROUP_CAP, quarter_cols), BF16),),
        expert_here,
        arrived,
        own_weights,
        other_weights,
        flops=100_000_000,
        scalars=1,
    )
    returned = lax.all_to_all(
        sums.reshape(chips * tp_count, GROUP_CAP, quarter_cols), (*CHIPS, "tp"), 0, 0, tiled=True
    ).reshape(parts, chips_in_group, planes, tp_count, GROUP_CAP, quarter_cols)
    (mixed_out,) = run(
        mix_body,
        (jax.ShapeDtypeStruct((seq_count, quarter_cols), BF16),),
        index,
        returned,
        placing_t,
        attn_resid,
        scalars=1,
        hbm_out=1,
        sems=1,
        scratch=(pltpu.VMEM((seq_count, quarter_cols), BF16),),
    )
    return (mixed_out, new_latent, new_rope)


def solution(mesh):
    torus = Mesh(mesh.devices.reshape(8, 8, 2, mesh.shape["tp"]), ("ep_0", "ep_1", "ep_2", "tp"))
    placed = (
        P(EP, None),
        P(),
        P(None, "tp"),
        P(None, "tp"),
        P(),
        P(),
        P(),
        P(None, "tp"),
        P("tp", None),
        P(None, "tp"),
        P(None, "tp"),
        P("tp", None),
        P(EP_TP, None, None),
        P(EP_TP, None, None),
        P(EP),
        P(),
        P(EP, None),
        P(EP, None),
        P(EP, None, "tp"),
        P(EP, None, "tp"),
        P(EP, "tp", None),
    )

    return jax.shard_map(
        shards,
        mesh=torus,
        in_specs=placed,
        out_specs=(P(EP, "tp"), P(EP, "tp"), P(EP, None)),
        check_vma=False,
    )
```
